256 devices in a mesh: sp: 16 (over y, x), tp: 16 (over z, core).
Axes of the slice: x: 4, y: 4, z: 8, core: 2. Of those that a mesh axis runs over, the one named last changes fastest.
Arguments:
- ask_preactivation_left: bfloat16 [8192, 2048], P('sp', 'tp'), may hold values from -6 to 6
- keep_preactivation_left: bfloat16 [8192, 2048], P('sp', 'tp'), may hold values from -6 to 6
- keep_bound_complement_left: float32 [2048], P('tp'), may hold values from 0 to 0.1
- ask_preactivation_right: bfloat16 [8192, 4096], P('sp', 'tp'), may hold values from -6 to 6
- keep_preactivation_right: bfloat16 [8192, 4096], P('sp', 'tp'), may hold values from -6 to 6
- keep_bound_complement_right: float32 [4096], P('tp'), may hold values from 0 to 0.1
- payload_entries: bfloat16 [8192, 2048], P('sp', 'tp'), may hold values from -6 to 6
- emission_switch_logits: bfloat16 [8192, 2048], P('sp', 'tp'), may hold values from -6 to 6
- added_log_keep_bias: float32 [8192, 32], P('sp', 'tp'), may hold values from -2.1 to 0
- lanewise_rescale: float32 [64], replicated, may hold values from 0.1 to 1.9
- emission_matrix_alpha: bfloat16 [1024, 2048], P('tp'), may hold values from -0.125 to 0.125
- emission_matrix_beta: bfloat16 [1024, 2048], P('tp'), may hold values from -0.125 to 0.125
- skip_stream: bfloat16 [8192, 2048], P(('sp', 'tp')), may hold values from -6 to 6
- postrecurrence_rescale: float32 [2048], replicated, may hold values from 0.1 to 1.9
- premixture_rescale: float32 [2048], replicated, may hold values from 0.1 to 1.9
- postmixture_rescale: float32 [2048], replicated, may hold values from 0.1 to 1.9
- dispatcher_columns: bfloat16 [2048, 32], P(None, 'sp'), may hold values from -0.125 to 0.125
- switch_matrix: bfloat16 [16, 2048, 4096], P('sp', None, 'tp'), may hold values from -0.125 to 0.125
- expansion_matrix: bfloat16 [16, 2048, 4096], P('sp', None, 'tp'), may hold values from -0.125 to 0.125
- contraction_matrix: bfloat16 [16, 4096, 2048], P('sp', 'tp'), may hold values from -0.125 to 0.125
- item_specialist_cluster: int32 [8192], P(('sp', 'tp')), may hold values from 0 to 15, as said below
Outputs:
- result: bfloat16 [8192, 2048], P(('sp', 'tp'))
The draws below stay inside these ranges and needn't reach their ends.
Inputs may be any that keep to these rules, and one draw needn't show every extreme that they name: `item_specialist_cluster`: in every aligned block of 32 tokens (the rows of one device) no group is named more than 3 times, and some group exactly 3 times.
All inputs are finite; a program needn't handle non-finite values.
Results may differ from the reference program's by a relative error of at most 0.023.
Values may be sent and summed in bfloat16 or wider, within the bound.
A program may use at most 64 MiB of HBM per device.

```python
import jax
import jax.numpy as jnp
from jax import lax

D = 2048
HEADS_IN_SET = 16
DKA = 128
DKB = 256
DV = 64
FF = 2048
EXP_GROUP = 2
TOK_DEV = 512
BLOCK_LENGTH = 512
SEQ_STEPS = 8192
ROWS_DEV = 32
GROUPS = 16
EXPERTS = 32
CAP = 3
N_TP = 16


def forget_draw(key, columns):
    noise_part = jnp.clip(jax.random.normal(jax.random.fold_in(key, 1), (SEQ_STEPS, columns), jnp.float32), -5.0, 5.0)
    block_shift = jax.random.uniform(jax.random.fold_in(key, 2), (SEQ_STEPS // TOK_DEV, 1, 1), jnp.float32, -1.0, 1.0)
    shifted = noise_part.reshape(SEQ_STEPS // TOK_DEV, TOK_DEV, columns) + block_shift
    return shifted.reshape(SEQ_STEPS, columns).astype(jnp.bfloat16)


def draw_keep_preactivation_left(key, part):
    return forget_draw(key, HEADS_IN_SET * DKA)


def draw_keep_preactivation_right(key, part):
    return forget_draw(key, HEADS_IN_SET * DKB)


def gap_draw(key, recurrent_state_width):
    fast_share = 0.5
    fast_head = jax.random.uniform(jax.random.fold_in(key, 21), (HEADS_IN_SET, 1), jnp.float32) < fast_share
    quick_gap = jnp.exp(jax.random.uniform(jax.random.fold_in(key, 22), (HEADS_IN_SET, recurrent_state_width), jnp.float32, jnp.log(0.04), jnp.log(0.1)))
    slow_gap = jnp.exp(jax.random.uniform(jax.random.fold_in(key, 23), (HEADS_IN_SET, recurrent_state_width), jnp.float32, jnp.log(0.3 / SEQ_STEPS), jnp.log(1.5 / SEQ_STEPS)))
    return jnp.where(fast_head, quick_gap, slow_gap).reshape(HEADS_IN_SET * recurrent_state_width)


def draw_keep_bound_complement_left(key, part):
    return gap_draw(key, DKA)


def draw_keep_bound_complement_right(key, part):
    return gap_draw(key, DKB)


def draw_added_log_keep_bias(key, part):
    spike_position = jax.random.randint(jax.random.fold_in(key, 31), (3, 2 * HEADS_IN_SET), 0, SEQ_STEPS)
    spike_strength = jax.random.uniform(jax.random.fold_in(key, 32), (3, 2 * HEADS_IN_SET), jnp.float32, jnp.log(0.5), jnp.log(0.8))
    sequence_positions = jnp.arange(SEQ_STEPS, dtype=jnp.int32)[:, None]
    spike_sum = jnp.zeros((SEQ_STEPS, 2 * HEADS_IN_SET), jnp.float32)
    for selected_group in range(3):
        spike_sum = spike_sum + jnp.where(sequence_positions == spike_position[selected_group][None, :], spike_strength[selected_group][None, :], 0.0)
    return spike_sum


def draw_item_specialist_cluster(key, part):
    block_total_count = SEQ_STEPS // ROWS_DEV
    others = GROUPS - 1
    spare_rows = ROWS_DEV - CAP
    base_load = spare_rows // others
    extra_rows = spare_rows - base_load * others
    move_limit = max(0, min(CAP - base_load - 1, base_load))
    hot_group = jax.random.randint(jax.random.fold_in(key, 11), (block_total_count, 1), 0, GROUPS)
    other_index = jnp.arange(others, dtype=jnp.int32)[None, :]
    shuffled = jnp.argsort(jax.random.randint(jax.random.fold_in(key, 12), (block_total_count, others), 0, 1 << 16) * others + other_index, axis=1)
    loads = base_load + (shuffled < extra_rows).astype(jnp.int32)
    pairs = others // 2
    if pairs > 0:
        moved = jax.random.randint(jax.random.fold_in(key, 13), (block_total_count, pairs), -move_limit, move_limit + 1)
        load_shift = jnp.stack([moved, -moved], axis=2).reshape(block_total_count, 2 * pairs)
        if others > 2 * pairs:
            load_shift = jnp.concatenate([load_shift, jnp.zeros((block_total_count, 1), jnp.int32)], axis=1)
        loads = loads + load_shift
    group_index = jnp.arange(GROUPS, dtype=jnp.int32)[None, :]
    source = jnp.clip(jnp.where(group_index < hot_group, group_index, group_index - 1), 0, others - 1)
    source = jnp.broadcast_to(source, (block_total_count, GROUPS))
    all_loads = jnp.where(group_index == hot_group, CAP, jnp.take_along_axis(loads, source, axis=1))
    load_ends = jnp.cumsum(all_loads, axis=1)
    sequence_positions = jnp.arange(ROWS_DEV, dtype=jnp.int32)[None, :, None]
    group_of = jnp.sum((load_ends[:, None, :] <= sequence_positions).astype(jnp.int32), axis=2)
    row_index = jnp.arange(ROWS_DEV, dtype=jnp.int32)[None, :]
    row_order = jnp.argsort(jax.random.randint(jax.random.fold_in(key, 14), (block_total_count, ROWS_DEV), 0, 1 << 16) * ROWS_DEV + row_index, axis=1)
    group_of = jnp.take_along_axis(group_of, row_order, axis=1)
    return group_of.reshape(SEQ_STEPS).astype(jnp.int32)


def steps_of(own_key, extent, split, smallest, high):
    loudness, own = 1.0, jax.random.fold_in(own_key, 6)
    for dim, shards_of in split:
        steps = jnp.exp(jax.random.uniform(jax.random.fold_in(own, dim), (shards_of,), jnp.float32, smallest / len(split), high / len(split)))
        loudness = loudness * jnp.repeat(steps, extent[dim] // shards_of).reshape([-1 if axis == dim else 1 for axis in range(len(extent))])
    return loudness


def gaussian(rng, extent, width, bound, split=(), kind=jnp.bfloat16):
    level = steps_of(rng, extent, split, -0.22, 0.18) if split else 1.0
    drawn = jax.random.normal(rng, extent, jnp.float32) * width * level
    return jnp.minimum(jnp.maximum(drawn, -bound), bound).astype(kind)


def setup_inputs(seed: int = 0) -> dict:
    key_list = jax.random.split(jax.random.key(seed), 22)
    return {
        "ask_preactivation_left": gaussian(key_list[0], (SEQ_STEPS, HEADS_IN_SET * DKA), 1.0, 6.0, ((0, 16), (1, 16))),
        "keep_preactivation_left": draw_keep_preactivation_left(jax.random.fold_in(key_list[21], 71), 0),
        "keep_bound_complement_left": draw_keep_bound_complement_left(jax.random.fold_in(key_list[21], 71), 0),
        "ask_preactivation_right": gaussian(key_list[3], (SEQ_STEPS, HEADS_IN_SET * DKB), 1.0, 6.0, ((0, 16), (1, 16))),
        "keep_preactivation_right": draw_keep_preactivation_right(jax.random.fold_in(key_list[21], 71), 0),
        "keep_bound_complement_right": draw_keep_bound_complement_right(jax.random.fold_in(key_list[21], 71), 0),
        "payload_entries": gaussian(key_list[6], (SEQ_STEPS, 2 * HEADS_IN_SET * DV), 1.0, 6.0, ((0, 16), (1, 16))),
        "emission_switch_logits": gaussian(key_list[7], (SEQ_STEPS, 2 * HEADS_IN_SET * DV), 1.0, 6.0, ((0, 16), (1, 16))),
        "added_log_keep_bias": draw_added_log_keep_bias(jax.random.fold_in(key_list[21], 71), 0),
        "lanewise_rescale": jnp.clip(1.0 + 0.18 * jax.random.normal(key_list[9], (DV,), jnp.float32), 0.1, 1.9),
        "emission_matrix_alpha": gaussian(key_list[10], (HEADS_IN_SET * DV, D), (2 * HEADS_IN_SET * DV) ** -0.5, 0.125, ((0, 16),)),
        "emission_matrix_beta": gaussian(key_list[11], (HEADS_IN_SET * DV, D), (2 * HEADS_IN_SET * DV) ** -0.5, 0.125, ((0, 16),)),
        "skip_stream": gaussian(key_list[12], (SEQ_STEPS, D), 1.0, 6.0, ((0, 256),)),
        "postrecurrence_rescale": jnp.clip(1.0 + 0.18 * jax.random.normal(key_list[13], (D,), jnp.float32), 0.1, 1.9),
        "premixture_rescale": jnp.clip(1.0 + 0.18 * jax.random.normal(key_list[14], (D,), jnp.float32), 0.1, 1.9),
        "postmixture_rescale": jnp.clip(1.0 + 0.18 * jax.random.normal(key_list[15], (D,), jnp.float32), 0.1, 1.9),
        "dispatcher_columns": gaussian(key_list[16], (D, EXPERTS), D ** -0.5, 0.125, ((1, 16),)),
        "switch_matrix": gaussian(key_list[17], (GROUPS, D, EXP_GROUP * FF), D ** -0.5, 0.125, ((0, 16), (2, 16))),
        "expansion_matrix": gaussian(key_list[18], (GROUPS, D, EXP_GROUP * FF), D ** -0.5, 0.125, ((0, 16), (2, 16))),
        "contraction_matrix": gaussian(key_list[19], (GROUPS, EXP_GROUP * FF, D), FF ** -0.5, 0.125, ((0, 16), (1, 16))),
        "item_specialist_cluster": draw_item_specialist_cluster(jax.random.fold_in(key_list[21], 71), 0),
    }


EPSILON = 1e-06
PRECISE = lax.Precision.HIGHEST

def rms_scale(features, gain):
    return features * lax.rsqrt(lax.optimization_barrier(jnp.mean(features * features, axis=-1, keepdims=True)) + EPSILON) * gain

def block_step(carry_state, inputs):
    queries, incoming_key_rows, value_row_block, inside = inputs
    length = queries.shape[0]
    causal = lax.broadcasted_iota(jnp.int32, (length, length), 0) >= lax.broadcasted_iota(jnp.int32, (length, length), 1)
    q_decayed = queries * jnp.exp(inside)
    k_grown = incoming_key_rows * jnp.exp(-inside)
    scores = jnp.einsum('thd,shd->hts', q_decayed, k_grown, precision=PRECISE)
    scores = jnp.where(causal[None], scores, jnp.zeros_like(scores))
    outputs = jnp.einsum('hts,shv->thv', scores, value_row_block, precision=PRECISE)
    outputs = outputs + jnp.einsum('thd,hdv->thv', q_decayed, carry_state, precision=PRECISE)
    last_decay = inside[-1]
    fresh_state = jnp.einsum('shd,shv->hdv', incoming_key_rows * jnp.exp(last_decay[None] - inside), value_row_block, precision=PRECISE)
    return (jnp.exp(last_decay)[:, :, None] * carry_state + fresh_state, outputs)

def head_outputs(call_arguments):
    query_vector, forget_gate, lower_margin, spike_value, value_row_block = call_arguments
    recurrent_state_width = query_vector.shape[1]
    block_total_count = SEQ_STEPS // BLOCK_LENGTH
    block_shape = (block_total_count, BLOCK_LENGTH, 1, recurrent_state_width)
    queries = jax.nn.silu(query_vector.astype(jnp.float32)).reshape(block_shape)
    incoming_key_rows = lower_margin * jax.nn.sigmoid(-forget_gate.astype(jnp.float32)).reshape(block_shape)
    logarithm_decay = jnp.log1p(-incoming_key_rows) + spike_value.reshape(block_total_count, BLOCK_LENGTH, 1, 1)
    inside = jnp.cumsum(logarithm_decay, axis=1)
    start_state = jnp.zeros((1, recurrent_state_width, DV), jnp.float32)
    final_state, outputs = lax.scan(block_step, start_state, (queries, incoming_key_rows, value_row_block.reshape(block_total_count, BLOCK_LENGTH, 1, DV), inside))
    return outputs.reshape(SEQ_STEPS, DV)

def partitioned_result_array(query_vector, forget_gate, lower_margin, spike_value, value_row_block):
    recurrent_state_width = query_vector.shape[1] // HEADS_IN_SET
    per_head_split = (query_vector.reshape(SEQ_STEPS, HEADS_IN_SET, recurrent_state_width).transpose(1, 0, 2), forget_gate.reshape(SEQ_STEPS, HEADS_IN_SET, recurrent_state_width).transpose(1, 0, 2), lower_margin.reshape(HEADS_IN_SET, recurrent_state_width), spike_value.T, value_row_block.transpose(1, 0, 2))
    outputs = lax.map(head_outputs, per_head_split)
    return outputs.transpose(1, 0, 2)

def head_rows(outputs, gate_rows, lanewise_rescale):
    scaled = rms_scale(outputs, lanewise_rescale) * jax.nn.sigmoid(gate_rows.astype(jnp.float32))
    return scaled.astype(jnp.bfloat16).reshape(SEQ_STEPS, HEADS_IN_SET * DV)

def project(head_a, head_b, emission_matrix_alpha, emission_matrix_beta):
    slice_rows = HEADS_IN_SET * DV // N_TP
    pieces_a = head_a.reshape(SEQ_STEPS, N_TP, slice_rows)
    pieces_b = head_b.reshape(SEQ_STEPS, N_TP, slice_rows)
    weights_a = emission_matrix_alpha.reshape(N_TP, slice_rows, D)
    weights_b = emission_matrix_beta.reshape(N_TP, slice_rows, D)

    def add_slice(slice_index, running_sum):
        slice_sum = jnp.dot(pieces_a[:, slice_index], weights_a[slice_index], preferred_element_type=jnp.float32)
        slice_sum = slice_sum + jnp.dot(pieces_b[:, slice_index], weights_b[slice_index], preferred_element_type=jnp.float32)
        return running_sum + lax.optimization_barrier(slice_sum.astype(jnp.bfloat16)).astype(jnp.float32)
    return lax.fori_loop(0, N_TP, add_slice, jnp.zeros((SEQ_STEPS, D), jnp.float32))

def expert_mixture(normed, dispatcher_columns, switch_matrix, expansion_matrix, contraction_matrix, item_specialist_cluster):
    sorted_order = jnp.argsort(item_specialist_cluster, stable=True).astype(jnp.int32)
    members = item_specialist_cluster[None, :] == jnp.arange(GROUPS, dtype=jnp.int32)[:, None]
    counts = lax.optimization_barrier(jnp.sum(members.astype(jnp.int32), axis=1))
    starts = jnp.cumsum(counts) - counts
    group_slots = SEQ_STEPS // ROWS_DEV * CAP
    slice_width = EXP_GROUP * FF // N_TP

    def one_group(group):
        slot_index = jnp.arange(group_slots, dtype=jnp.int32)
        filled = slot_index < counts[group]
        token_index = sorted_order[jnp.minimum(starts[group] + slot_index, SEQ_STEPS - 1)]
        group_rows = jnp.where(filled[:, None], normed[token_index], jnp.zeros((), jnp.bfloat16))
        columns = lax.dynamic_slice_in_dim(dispatcher_columns, group * EXP_GROUP, EXP_GROUP, 1)
        scores = jax.nn.sigmoid(jnp.dot(group_rows, columns, preferred_element_type=jnp.float32))
        weights = scores / lax.optimization_barrier(jnp.sum(scores, axis=1, keepdims=True))
        gate_proj = jnp.dot(group_rows, switch_matrix[group], preferred_element_type=jnp.float32)
        up_proj = jnp.dot(group_rows, expansion_matrix[group], preferred_element_type=jnp.float32)
        hidden = (jax.nn.silu(gate_proj) * up_proj).astype(jnp.bfloat16)
        down_rows = contraction_matrix[group]

        def add_slice(slice_index, running_sum):
            first_unit = (slice_index * slice_width).astype(jnp.int32)
            hidden_part = lax.dynamic_slice_in_dim(hidden, first_unit, slice_width, 1)
            down_part = lax.dynamic_slice_in_dim(down_rows, first_unit, slice_width, 0)
            product = jnp.dot(hidden_part, down_part, preferred_element_type=jnp.float32)
            member = (first_unit // FF).astype(jnp.int32)
            member_weight = lax.dynamic_slice_in_dim(weights, member, 1, 1)
            slice_sum = member_weight * product
            return running_sum + lax.optimization_barrier(slice_sum.astype(jnp.bfloat16)).astype(jnp.float32)
        running_sum = lax.fori_loop(0, N_TP, add_slice, jnp.zeros((group_slots, D), jnp.float32))
        return (running_sum.astype(jnp.bfloat16), jnp.where(filled, token_index, SEQ_STEPS))
    routed_rows, targets = lax.map(one_group, jnp.arange(GROUPS, dtype=jnp.int32))
    empty = jnp.zeros((SEQ_STEPS, D), jnp.bfloat16)
    return empty.at[targets.reshape(-1)].set(routed_rows.reshape(-1, D), mode='drop')

def reference(ask_preactivation_left, keep_preactivation_left, keep_bound_complement_left, ask_preactivation_right, keep_preactivation_right, keep_bound_complement_right, payload_entries, emission_switch_logits, added_log_keep_bias, lanewise_rescale, emission_matrix_alpha, emission_matrix_beta, skip_stream, postrecurrence_rescale, premixture_rescale, postmixture_rescale, dispatcher_columns, switch_matrix, expansion_matrix, contraction_matrix, item_specialist_cluster):
    routing_assignment = added_log_keep_bias.reshape(SEQ_STEPS, HEADS_IN_SET, 2)
    content_coupling = payload_entries.astype(jnp.float32).reshape(SEQ_STEPS, HEADS_IN_SET, 2, DV)
    gate_pair = emission_switch_logits.reshape(SEQ_STEPS, HEADS_IN_SET, 2, DV)
    raw_leading_factor = partitioned_result_array(ask_preactivation_left, keep_preactivation_left, keep_bound_complement_left, routing_assignment[:, :, 0], content_coupling[:, :, 0])
    raw_trailing_factor = partitioned_result_array(ask_preactivation_right, keep_preactivation_right, keep_bound_complement_right, routing_assignment[:, :, 1], content_coupling[:, :, 1])
    head_a = head_rows(raw_leading_factor, gate_pair[:, :, 0], lanewise_rescale)
    head_b = head_rows(raw_trailing_factor, gate_pair[:, :, 1], lanewise_rescale)
    mixed = project(head_a, head_b, emission_matrix_alpha, emission_matrix_beta)
    h_mid = (skip_stream.astype(jnp.float32) + rms_scale(mixed, postrecurrence_rescale)).astype(jnp.bfloat16)
    normed = rms_scale(h_mid.astype(jnp.float32), premixture_rescale).astype(jnp.bfloat16)
    routed = expert_mixture(normed, dispatcher_columns, switch_matrix, expansion_matrix, contraction_matrix, item_specialist_cluster)
    return (h_mid.astype(jnp.float32) + rms_scale(routed.astype(jnp.float32), postmixture_rescale)).astype(jnp.bfloat16)
```

```python
import functools

import jax
import jax.numpy as jnp
from jax import lax
from jax.experimental import pallas as pl
from jax.experimental.pallas import tpu as pltpu
from jax.sharding import PartitionSpec as P

EPSILON = 1e-06
NX, NY, NZ = 4, 4, 8
NS = NX * NY
D = 2048
KT = 384
TOK = 512
ROWS = 32
CAP = 3
SLOTS = NS * CAP
LINES = D // 128
HID = 256
FAR, NEAR = NZ // 2, NZ // 2 - 1
PLACE = {0: 0, 7: 1, 1: 2, 6: 3, 2: 4, 5: 5, 3: 6, 4: 7}
DCH, GCH = 2, 3
MESH = pl.DeviceIdType.MESH
F32, BF16 = jnp.float32, jnp.bfloat16


def dot(a, b):
    return jnp.dot(a, b, preferred_element_type=F32)


def dot_nt(a, b):
    return lax.dot_general(a, b, (((1,), (1,)), ((), ())), preferred_element_type=F32)


def dot_tn(a, b):
    return lax.dot_general(a, b, (((0,), (0,)), ((), ())), preferred_element_type=F32)


def sigmoid(v):
    return 1.0 / (1.0 + jnp.exp(-v))


def rms(v, gain):
    return v * lax.rsqrt(jnp.mean(v * v, axis=-1, keepdims=True) + EPSILON) * gain


def split3(v):
    high = v.astype(BF16)
    rest = v - high.astype(F32)
    mid = rest.astype(BF16)
    low = (rest - mid.astype(F32)).astype(BF16)
    return high, mid, low


def iota(shape, dim):
    return lax.broadcasted_iota(jnp.int32, shape, dim)


def kernel(
    qa_ref, fa_ref, ga_ref, qb_ref, fb_ref, gb_ref, v_ref, gate_ref, bias_ref, lane_ref,
    skip_ref, post_ref, pre_ref, postmix_ref, router_ref, cluster_ref,
    alpha_ref, beta_ref, sw_ref, ex_ref, co_ref,
    out_ref,
    key_s, ins_s, qd_s, kg_s, wk_s, intra_s, buf1, buf2, row_s, hd_s, hrecv, wproj, p_s,
    dsend, drecv, hmid_s, out_rt, x_rt, conv_s, x_s, part_s, swv, exv, cov, gsend, grecv, ret_rt, fin_rt,
    wsem, wssem, wrsem, s1s, s1r, s2s, s2r, hs, hr, dss, drs, dps, dpr, ags, agr, gss, grs, rts, rtr,
):
    s = lax.axis_index("sp")
    t = lax.axis_index("tp")
    y, x = s // NX, lax.rem(s, NX)
    z, c = t // 2, lax.rem(t, 2)
    way = 1 - 2 * c
    ahead = lax.rem(z + way + NZ, NZ) * 2 + c
    behind = lax.rem(z - way + NZ, NZ) * 2 + c
    sibling = z * 2 + 1 - c

    def remote(src, dst, ssem, rsem, sp, tp):
        return pltpu.make_async_remote_copy(
            src_ref=src, dst_ref=dst, send_sem=ssem, recv_sem=rsem,
            device_id=(sp, tp), device_id_type=MESH,
        )

    barrier = pltpu.get_barrier_semaphore()

    def greet(d, carry):
        pl.semaphore_signal(barrier, inc=1, device_id=(lax.rem(s + d, NS), t), device_id_type=MESH)
        return carry

    lax.fori_loop(1, NS, greet, 0)
    for peer in (ahead, behind, sibling):
        pl.semaphore_signal(barrier, inc=1, device_id=(s, peer), device_id_type=MESH)

    own_weights = [
        pltpu.make_async_copy(alpha_ref, wproj.at[0, pl.ds(0, 64)], wsem.at[0]),
        pltpu.make_async_copy(beta_ref, wproj.at[0, pl.ds(64, 64)], wsem.at[1]),
        pltpu.make_async_copy(sw_ref.at[0], swv.at[0], wsem.at[2]),
        pltpu.make_async_copy(ex_ref.at[0], exv.at[0], wsem.at[3]),
        pltpu.make_async_copy(co_ref.at[0], cov.at[0], wsem.at[4]),
    ]
    for copy in own_weights:
        copy.start()

    gap = jnp.concatenate([ga_ref[...], gb_ref[...]], axis=1)
    lower = jnp.where(iota((128, 128), 0) >= iota((128, 128), 1), 1.0, 0.0).astype(BF16)

    def decays(r, carry):
        rows = pl.ds(pl.multiple_of(r * 128, 128), 128)
        forget = jnp.concatenate([fa_ref[rows, :].astype(F32), fb_ref[rows, :].astype(F32)], axis=1)
        key = gap * sigmoid(-forget)
        left = jnp.broadcast_to(bias_ref[0:1, rows], (128, 128)).T
        right = jnp.broadcast_to(bias_ref[1:2, rows], (128, 128)).T
        logf = jnp.log1p(-key) + jnp.concatenate([left, right, right], axis=1)
        high, mid, low = split3(logf)
        inside = dot(lower, high) + dot(lower, mid) + dot(lower, low) + carry
        key_s[rows, :] = key
        ins_s[rows, :] = inside
        return inside[127:128, :]

    last = lax.fori_loop(0, TOK // 128, decays, jnp.zeros((1, KT), F32))

    def scaled(r, carry):
        rows = pl.ds(pl.multiple_of(r * 128, 128), 128)
        ask = jnp.concatenate([qa_ref[rows, :].astype(F32), qb_ref[rows, :].astype(F32)], axis=1)
        key = key_s[rows, :]
        inside = ins_s[rows, :]
        qd_s[rows, :] = (ask * sigmoid(ask) * jnp.exp(inside)).astype(BF16)
        kg_s[rows, :] = (key * jnp.exp(-inside)).astype(BF16)
        wk_s[rows, :] = (key * jnp.exp(last - inside)).astype(BF16)
        return carry

    lax.fori_loop(0, TOK // 128, scaled, 0)
    summed = dot_tn(v_ref[...], wk_s[...])
    state = jnp.concatenate([summed[0:64, 0:128], summed[64:128, 128:KT]], axis=1)

    def packed(buf, place, state, total):
        rows3 = iota((16, KT), 0)
        high, mid, low = (part.astype(F32) for part in split3(total))
        lines = jnp.where(rows3 == 0, high, jnp.where(rows3 == 1, mid, jnp.where(rows3 == 2, low, 0.0)))
        buf[place, 0:64, :] = state.astype(BF16)
        buf[place, 64:80, :] = lines.astype(BF16)

    def unpacked(buf, place):
        lines = buf[place, 64:80, :].astype(F32)
        return buf[place, 0:64, :].astype(F32), lines[0:1] + lines[1:2] + lines[2:3]

    packed(buf1, x, state, last)
    pl.semaphore_wait(barrier, NS + 2)

    def along_x(d):
        return remote(buf1.at[x], buf1.at[x], s1s.at[d], s1r.at[x], y * NX + lax.rem(x + d, NX), t)

    def from_x(d):
        there = lax.rem(x + d, NX)
        return remote(buf1.at[there], buf1.at[there], s1s.at[d], s1r.at[there], y * NX + there, t)

    for d in range(1, NX):
        along_x(d).start()

    shared = [
        (alpha_ref, wproj.at[1, pl.ds(0, 64)]), (beta_ref, wproj.at[1, pl.ds(64, 64)]),
        (sw_ref.at[0], swv.at[1]), (ex_ref.at[0], exv.at[1]), (co_ref.at[0], cov.at[1]),
    ]
    shared = [remote(a, b, wssem.at[k], wrsem.at[k], s, sibling) for k, (a, b) in enumerate(shared)]
    for copy in shared:
        copy.start()

    left_half = iota((256, 128), 1) < 64

    def intra(columns, first):
        for block in range(2):
            rows, width = slice(block * 256, block * 256 + 256), 256 * (block + 1)
            scores = dot_nt(qd_s[rows, columns], kg_s[0:width, columns])
            causal = iota((256, width), 0) + 256 * block >= iota((256, width), 1)
            scores = jnp.where(causal, scores, 0.0).astype(BF16)
            found = dot(scores, v_ref[0:width, :])
            intra_s[rows, :] = found if first else jnp.where(left_half, intra_s[rows, :], found)

    intra(slice(0, 128), True)

    for d in range(1, NX):
        from_x(d).wait_recv()
    sofar, gone = jnp.zeros((64, KT), F32), jnp.zeros((1, KT), F32)
    before, before_gone = sofar, gone
    for k in range(NX):
        before = jnp.where(x == k, sofar, before)
        before_gone = jnp.where(x == k, gone, before_gone)
        piece, total = unpacked(buf1, k)
        sofar = jnp.exp(total) * sofar + piece
        gone = gone + total
    packed(buf2, y, sofar, gone)
    row_s[...] = jnp.zeros_like(row_s)

    def along_y(d):
        return remote(buf2.at[y], buf2.at[y], s2s.at[d], s2r.at[y], (y + d) * NX + x, t)

    def from_y(k):
        return remote(buf2.at[k], buf2.at[k], s2s.at[0], s2r.at[k], k * NX + x, t)

    for d in range(1, NY):
        @pl.when(y + d < NY)
        def _():
            along_y(d).start()

    intra(slice(128, KT), False)

    for k in range(NY - 1):
        @pl.when(k < y)
        def _():
            from_y(k).wait_recv()
            piece, total = unpacked(buf2, k)
            row_s[...] = jnp.exp(total) * row_s[...] + piece

    carried = jnp.exp(before_gone) * row_s[...] + before
    is_left = iota((64, KT), 1) < 128
    carried = jnp.concatenate(
        [jnp.where(is_left, carried, 0.0), jnp.where(is_left, 0.0, carried)], axis=0
    ).astype(BF16)
    lane_gain = jnp.concatenate([lane_ref[...], lane_ref[...]], axis=1)
    left = iota((128, 128), 1) < 64
    for r in range(TOK // 128):
        rows = slice(r * 128, r * 128 + 128)
        raw = intra_s[rows, :] + dot_nt(qd_s[rows, :], carried)
        squares = raw * raw
        mean_a = jnp.sum(jnp.where(left, squares, 0.0), axis=1, keepdims=True) * (1.0 / 64)
        mean_b = jnp.sum(jnp.where(left, 0.0, squares), axis=1, keepdims=True) * (1.0 / 64)
        mean = jnp.where(left, mean_a, mean_b)
        head = raw * lax.rsqrt(mean + EPSILON) * lane_gain * sigmoid(gate_ref[rows, :].astype(F32))
        head = head.astype(BF16)
        for q in range(4):
            at = (2 * r + q // 2) * 32
            hd_s[q % 2, at : at + 32, :] = head[q * 32 : q * 32 + 32, :]

    swap = remote(hd_s.at[1 - c], hrecv, hs, hr, s, sibling)
    swap.start()
    for copy in own_weights[:2]:
        copy.wait()
    p_s[...] = dot(hd_s[c], wproj[0])
    for copy in shared[:2]:
        copy.wait_recv()
    swap.wait_recv()
    p_s[...] = p_s[...] + dot(hrecv[...], wproj[1])

    HALF = ROWS // DCH

    def ring_d(k, j):
        part = pl.ds(j * HALF, HALF)
        return remote(
            dsend.at[k, part], drecv.at[k, part], dss.at[k, j], drs.at[k, j], s,
            ahead if k < FAR else behind,
        )

    def send_d(k, j, first):
        place = FAR - k if k < FAR else -(NEAR - (k - FAR))
        target = lax.rem(z + way * place + NZ, NZ)
        rows = pl.ds(pl.multiple_of(target * ROWS + j * HALF, HALF), HALF)
        value = p_s[rows, :]
        if not first:
            ring_d(k - 1, j).wait_recv()
            value = value + drecv[k - 1, j * HALF : (j + 1) * HALF, :].astype(F32)
        dsend[k, j * HALF : (j + 1) * HALF, :] = value.astype(BF16)
        ring_d(k, j).start()

    for step in range(FAR):
        for j in range(DCH):
            send_d(step, j, step == 0)
            if step < NEAR:
                send_d(FAR + step, j, step == 0)
    mixed = p_s[pl.ds(pl.multiple_of(z * ROWS, ROWS), ROWS), :]
    for k in (FAR + NEAR - 1, FAR - 1):
        for j in range(DCH):
            ring_d(k, j).wait_recv()
        mixed = mixed + drecv[k].astype(F32)

    h_mid = (skip_ref[...].astype(F32) + rms(mixed, post_ref[...])).astype(BF16).astype(F32)
    hmid_s[...] = h_mid
    normed = rms(h_mid, pre_ref[...]).astype(BF16)

    group_row = jnp.broadcast_to(cluster_ref[...], (ROWS, ROWS))
    group_row = group_row.astype(F32)
    diagonal = iota((ROWS, ROWS), 0) == iota((ROWS, ROWS), 1)
    group_column = jnp.sum(jnp.where(diagonal, group_row, 0.0), axis=1, keepdims=True)
    same = jnp.where(group_row == group_column, 1.0, 0.0)
    earlier_row = iota((ROWS, ROWS), 0) < iota((ROWS, ROWS), 1)
    rank_row = jnp.sum(jnp.where(earlier_row, same, 0.0), axis=0, keepdims=True)
    earlier_column = iota((ROWS, ROWS), 1) < iota((ROWS, ROWS), 0)
    rank_column = jnp.sum(jnp.where(earlier_column, same, 0.0), axis=1, keepdims=True)
    slot_row = group_row[0:1, :] * CAP + rank_row
    slot_column = group_column * CAP + rank_column
    placing = jnp.where(
        iota((SLOTS, ROWS), 0).astype(F32) == slot_row, 1.0, 0.0
    ).astype(BF16)
    placed_back = jnp.where(
        iota((ROWS, SLOTS), 1).astype(F32) == slot_column, 1.0, 0.0
    ).astype(BF16)

    def to_lines(value):
        for i in range(LINES):
            conv_s[pl.ds(i, SLOTS, stride=LINES), :] = value[:, i * 128 : i * 128 + 128]
        return conv_s[...].astype(BF16)

    out_rt[...] = to_lines(dot(placing, normed))
    own = pl.ds(pl.multiple_of(s * (CAP * LINES), CAP * LINES), CAP * LINES)

    def lines_of(k):
        return pl.ds(pl.multiple_of(k * (CAP * LINES), CAP * LINES), CAP * LINES)

    def dispatch(d):
        there = lax.rem(s + d, NS)
        return remote(out_rt.at[lines_of(there)], x_rt.at[0, own], dps.at[d], dpr.at[s], there, t)

    def dispatched(d):
        there = lax.rem(s + d, NS)
        return remote(out_rt.at[own], x_rt.at[0, lines_of(there)], dps.at[d], dpr.at[there], there, t)

    def each(action):
        def body(d, carry):
            action(d)
            return carry

        lax.fori_loop(1, NS, body, 0)

    each(lambda d: dispatch(d).start())
    x_rt[0, own, :] = out_rt[own, :]

    for copy in own_weights[2:]:
        copy.wait()
    router = router_ref[...].astype(F32)
    router_rows = iota((16, D), 0)
    router = jnp.where(
        router_rows == 0, router[0:1], jnp.where(router_rows == 1, router[1:2], 0.0)
    ).astype(BF16)
    member = z // (NZ // 2)

    def ring_g(k, j):
        source = (NZ - k) % NZ if k < FAR else k - FAR
        target = (source + NZ - 1) % NZ if k < FAR else source + 1
        part = pl.ds(j * (SLOTS // GCH * LINES), SLOTS // GCH * LINES)
        return remote(
            x_rt.at[source, part], x_rt.at[target, part], ags.at[k, j], agr.at[k, j], s,
            ahead if k < FAR else behind,
        )

    def to_rows(place):
        conv_s[...] = x_rt[place].astype(F32)
        at = PLACE[place] * SLOTS
        for i in range(LINES):
            x_s[at : at + SLOTS, i * 128 : i * 128 + 128] = conv_s[
                pl.ds(i, SLOTS, stride=LINES), :
            ].astype(BF16)

    def compute(places):
        for place in places:
            to_rows(place)
        at, size = PLACE[places[0]] * SLOTS, SLOTS * len(places)
        rows = x_s[at : at + size, :]
        scores = sigmoid(dot_nt(rows, router))
        first, second = scores[:, 0:1], scores[:, 1:2]
        weight = jnp.where(member == 0, first, second) / (first + second)
        total = None
        for u in range(2):
            gate = dot(rows, swv[u])
            hidden = (gate * sigmoid(gate) * dot(rows, exv[u])).astype(BF16)
            term = dot(hidden, cov[u])
            total = term if total is None else total + term
        part_s[at : at + size, :] = total * weight

    each(lambda d: dispatched(d).wait_recv())
    for j in range(GCH):
        ring_g(0, j).start()
        ring_g(FAR, j).start()
    for copy in shared[2:]:
        copy.wait_recv()
    compute((0,))
    for k in range(FAR):
        for j in range(GCH):
            ring_g(k, j).wait_recv()
            if k + 1 < FAR:
                ring_g(k + 1, j).start()
            if k < NEAR:
                ring_g(FAR + k, j).wait_recv()
                if k + 1 < NEAR:
                    ring_g(FAR + k + 1, j).start()
        compute((NZ - 1 - k, k + 1) if k < NEAR else (NZ - 1 - k,))

    PART = SLOTS // GCH

    def ring_p(k, j):
        part = pl.ds(j * PART, PART)
        return remote(
            gsend.at[k, part], grecv.at[k, part], gss.at[k, j], grs.at[k, j], s,
            ahead if k < FAR else behind,
        )

    def send_p(k, j, first):
        place = PLACE[FAR - k if k < FAR else NZ - (NEAR - (k - FAR))]
        value = part_s[place * SLOTS + j * PART : place * SLOTS + (j + 1) * PART, :]
        if not first:
            ring_p(k - 1, j).wait_recv()
            value = value + grecv[k - 1, j * PART : (j + 1) * PART, :].astype(F32)
        gsend[k, j * PART : (j + 1) * PART, :] = value.astype(BF16)
        ring_p(k, j).start()

    for step in range(FAR):
        for j in range(GCH):
            send_p(step, j, step == 0)
            if step < NEAR:
                send_p(FAR + step, j, step == 0)
    final = part_s[0:SLOTS, :]
    for k in (FAR + NEAR - 1, FAR - 1):
        for j in range(GCH):
            ring_p(k, j).wait_recv()
        final = final + grecv[k].astype(F32)

    fin_rt[...] = to_lines(final)

    def give(d):
        there = lax.rem(s + d, NS)
        return remote(fin_rt.at[lines_of(there)], ret_rt.at[own], rts.at[d], rtr.at[s], there, t)

    def given(d):
        there = lax.rem(s + d, NS)
        return remote(fin_rt.at[own], ret_rt.at[lines_of(there)], rts.at[d], rtr.at[there], there, t)

    each(lambda d: give(d).start())
    ret_rt[own, :] = fin_rt[own, :]

    for d in range(1, NX):
        along_x(d).wait_send()
    for d in range(1, NY):
        @pl.when(y + d < NY)
        def _():
            along_y(d).wait_send()
    for copy in shared:
        copy.wait_send()
    swap.wait_send()
    for k in range(FAR + NEAR):
        for j in range(DCH):
            ring_d(k, j).wait_send()
        for j in range(GCH):
            ring_g(k, j).wait_send()
            ring_p(k, j).wait_send()
    each(lambda d: dispatch(d).wait_send())

    each(lambda d: given(d).wait_recv())
    conv_s[...] = ret_rt[...].astype(F32)
    for i in range(LINES):
        x_s[0:SLOTS, i * 128 : i * 128 + 128] = conv_s[pl.ds(i, SLOTS, stride=LINES), :].astype(BF16)
    routed = dot(placed_back, x_s[0:SLOTS, :])
    out_ref[...] = (hmid_s[...] + rms(routed, postmix_ref[...])).astype(BF16)
    each(lambda d: give(d).wait_send())


def shards(
    ask_left, keep_left, gap_left, ask_right, keep_right, gap_right, payload, switch_logits,
    keep_bias, lanewise, alpha, beta, skip, post, pre, postmix, router, switch, expansion,
    contraction, cluster,
):
    vmem = pl.BlockSpec(memory_space=pltpu.VMEM)
    hbm = pl.BlockSpec(memory_space=pl.ANY)
    ring = FAR + NEAR
    dma, lines = pltpu.SemaphoreType.DMA, SLOTS * LINES
    return pl.pallas_call(
        kernel,
        out_shape=jax.ShapeDtypeStruct((ROWS, D), BF16),
        in_specs=[vmem] * 16 + [hbm] * 5,
        out_specs=vmem,
        scratch_shapes=[
            pltpu.VMEM((TOK, KT), F32),
            pltpu.VMEM((TOK, KT), F32),
            pltpu.VMEM((TOK, KT), BF16),
            pltpu.VMEM((TOK, KT), BF16),
            pltpu.VMEM((TOK, KT), BF16),
            pltpu.VMEM((TOK, 128), F32),
            pltpu.VMEM((NX, 80, KT), BF16),
            pltpu.VMEM((NY, 80, KT), BF16),
            pltpu.VMEM((64, KT), F32),
            pltpu.VMEM((2, TOK // 2, 128), BF16),
            pltpu.VMEM((TOK // 2, 128), BF16),
            pltpu.VMEM((2, 128, D), BF16),
            pltpu.VMEM((TOK // 2, D), F32),
            pltpu.VMEM((ring, ROWS, D), BF16),
            pltpu.VMEM((ring, ROWS, D), BF16),
            pltpu.VMEM((ROWS, D), F32),
            pltpu.VMEM((lines, 128), BF16),
            pltpu.VMEM((NZ, lines, 128), BF16),
            pltpu.VMEM((lines, 128), F32),
            pltpu.VMEM((NZ * SLOTS, D), BF16),
            pltpu.VMEM((NZ * SLOTS, D), F32),
            pltpu.VMEM((2, D, HID), BF16),
            pltpu.VMEM((2, D, HID), BF16),
            pltpu.VMEM((2, HID, D), BF16),
            pltpu.VMEM((ring, SLOTS, D), BF16),
            pltpu.VMEM((ring, SLOTS, D), BF16),
            pltpu.VMEM((lines, 128), BF16),
            pltpu.VMEM((lines, 128), BF16),
            dma((5,)), dma((5,)), dma((5,)),
            dma((NX,)), dma((NX,)), dma((NY,)), dma((NY,)),
            dma, dma,
            dma((ring, DCH)), dma((ring, DCH)),
            dma((NS,)), dma((NS,)),
            dma((ring, GCH)), dma((ring, GCH)),
            dma((ring, GCH)), dma((ring, GCH)),
            dma((NS,)), dma((NS,)),
        ],
        compiler_params=pltpu.CompilerParams(
            collective_id=0, has_side_effects=True, vmem_limit_bytes=56 * 1024 * 1024
        ),
    )(
        ask_left, keep_left, gap_left.reshape(1, -1), ask_right, keep_right,
        gap_right.reshape(1, -1), payload, switch_logits, keep_bias.T, lanewise.reshape(1, -1),
        skip, post.reshape(1, -1), pre.reshape(1, -1), postmix.reshape(1, -1), router.T,
        cluster.reshape(1, -1), alpha, beta, switch, expansion, contraction,
    )


def solution(mesh):
    placed = (
        P("sp", "tp"),
        P("sp", "tp"),
        P("tp"),
        P("sp", "tp"),
        P("sp", "tp"),
        P("tp"),
        P("sp", "tp"),
        P("sp", "tp"),
        P("sp", "tp"),
        P(),
        P("tp", None),
        P("tp", None),
        P(("sp", "tp"), None),
        P(),
        P(),
        P(),
        P(None, "sp"),
        P("sp", None, "tp"),
        P("sp", None, "tp"),
        P("sp", "tp", None),
        P(("sp", "tp")),
    )
    return jax.shard_map(
        shards, mesh=mesh, in_specs=placed, out_specs=P(("sp", "tp"), None), check_vma=False
    )
```

```python
import functools

import jax
import jax.numpy as jnp
from jax import lax
from jax.experimental import pallas as pl
from jax.experimental.pallas import tpu as pltpu
from jax.sharding import PartitionSpec as P

EPSILON = 1e-06
NX, NY, NZ = 4, 4, 8
NS = NX * NY
D = 2048
KT = 384
TOK = 512
ROWS = 32
CAP = 3
SLOTS = NS * CAP
LINES = D // 128
HID = 256
FAR, NEAR = NZ // 2, NZ // 2 - 1
PLACE = {0: 0, 7: 1, 1: 2, 6: 3, 2: 4, 5: 5, 3: 6, 4: 7}
PITCH = 24
OFFSETS = sorted(
    ((dy, dx) for dy in range(NY) for dx in range(NX)),
    key=lambda o: min(o[0], NY - o[0]) + min(o[1], NX - o[1]),
)
DCH, GCH, ZCH, ACH = 4, 6, 4, 4
MESH = pl.DeviceIdType.MESH
F32, BF16 = jnp.float32, jnp.bfloat16


def dot(a, b):
    return jnp.dot(a, b, preferred_element_type=F32)


def dot_nt(a, b):
    return lax.dot_general(a, b, (((1,), (1,)), ((), ())), preferred_element_type=F32)


def dot_tn(a, b):
    return lax.dot_general(a, b, (((0,), (0,)), ((), ())), preferred_element_type=F32)


def sigmoid(v):
    return 1.0 / (1.0 + jnp.exp(-v))


def rms(v, gain):
    return v * lax.rsqrt(jnp.mean(v * v, axis=-1, keepdims=True) + EPSILON) * gain


def split3(v):
    high = v.astype(BF16)
    rest = v - high.astype(F32)
    mid = rest.astype(BF16)
    low = (rest - mid.astype(F32)).astype(BF16)
    return high, mid, low


def iota(shape, dim):
    return lax.broadcasted_iota(jnp.int32, shape, dim)


def kernel(
    fa_hbm, fb_hbm, ga_hbm, gb_hbm, bias_hbm, cluster_hbm, qa_hbm, qb_hbm, v_hbm,
    gate_hbm, lane_hbm, skip_hbm, post_hbm, pre_hbm, postmix_hbm, router_hbm,
    alpha_ref, beta_ref, sw_ref, ex_ref, co_ref,
    out_ref,
    fa_ref, fb_ref, ga_ref, gb_ref, bias_ref, cluster_ref, qa_ref, qb_ref, v_ref,
    gate_ref, lane_ref, skip_ref, post_ref, pre_ref, postmix_ref, router_ref, insem,
    key_s, ins_s, qd_s, kg_s, wk_s, intra_s, buf1, buf2, row_s, hd_s, hrecv, wproj, p_s,
    dsend, drecv, hmid_s, out_rt, x_rt, conv_s, x_s, part_s, swv, exv, cov, gsend, grecv, ret_rt, fin_rt,
    clus_s, place_s, unplace_s, nz_s, qz_s,
    cls, clr, zos, zor, zis, zir, xir,
    wsem, wssem, wrsem, s1s, s1r, s2s, s2r, hs, hr, dss, drs, ags, agr, gss, grs,
):
    s = lax.axis_index("sp")
    t = lax.axis_index("tp")
    y, x = s // NX, lax.rem(s, NX)
    z, c = t // 2, lax.rem(t, 2)
    way = 1 - 2 * c
    ahead = lax.rem(z + way + NZ, NZ) * 2 + c
    behind = lax.rem(z - way + NZ, NZ) * 2 + c
    sibling = z * 2 + 1 - c

    def remote(src, dst, ssem, rsem, sp, tp):
        return pltpu.make_async_remote_copy(
            src_ref=src, dst_ref=dst, send_sem=ssem, recv_sem=rsem,
            device_id=(sp, tp), device_id_type=MESH,
        )

    barrier = pltpu.get_barrier_semaphore()

    def greet(d, carry):
        pl.semaphore_signal(barrier, inc=1, device_id=(lax.rem(s + d, NS), t), device_id_type=MESH)
        return carry

    lax.fori_loop(1, NS, greet, 0)

    def greet_z(d, carry):
        peer = lax.rem(z + d, NZ) * 2 + c
        pl.semaphore_signal(barrier, inc=1, device_id=(s, peer), device_id_type=MESH)
        return carry

    lax.fori_loop(1, NZ, greet_z, 0)
    pl.semaphore_signal(barrier, inc=1, device_id=(s, sibling), device_id_type=MESH)

    inputs = [
        pltpu.make_async_copy(a, b, insem.at[k])
        for k, (a, b) in enumerate(
            [
                (fa_hbm, fa_ref), (fb_hbm, fb_ref), (ga_hbm, ga_ref), (gb_hbm, gb_ref),
                (bias_hbm, bias_ref), (cluster_hbm, cluster_ref), (qa_hbm, qa_ref),
                (qb_hbm, qb_ref), (v_hbm, v_ref), (gate_hbm, gate_ref), (lane_hbm, lane_ref),
                (skip_hbm, skip_ref), (post_hbm, post_ref), (pre_hbm, pre_ref),
                (postmix_hbm, postmix_ref), (router_hbm, router_ref),
            ]
        )
    ]
    for copy in inputs:
        copy.start()
    own_weights = [
        pltpu.make_async_copy(alpha_ref, wproj.at[0, pl.ds(0, 64)], wsem.at[0]),
        pltpu.make_async_copy(beta_ref, wproj.at[0, pl.ds(64, 64)], wsem.at[1]),
        pltpu.make_async_copy(sw_ref.at[0], swv.at[0], wsem.at[2]),
        pltpu.make_async_copy(ex_ref.at[0], exv.at[0], wsem.at[3]),
        pltpu.make_async_copy(co_ref.at[0], cov.at[0], wsem.at[4]),
    ]
    for copy in own_weights:
        copy.start()

    for copy in inputs[:6]:
        copy.wait()
    gap = jnp.concatenate([ga_ref[...], gb_ref[...]], axis=1)
    lower = jnp.where(iota((128, 128), 0) >= iota((128, 128), 1), 1.0, 0.0).astype(BF16)

    def decays(r, carry):
        rows = pl.ds(pl.multiple_of(r * 128, 128), 128)
        forget = jnp.concatenate([fa_ref[rows, :].astype(F32), fb_ref[rows, :].astype(F32)], axis=1)
        key = gap * sigmoid(-forget)
        left = jnp.broadcast_to(bias_ref[0:1, rows], (128, 128)).T
        right = jnp.broadcast_to(bias_ref[1:2, rows], (128, 128)).T
        logf = jnp.log1p(-key) + jnp.concatenate([left, right, right], axis=1)
        high, mid, low = split3(logf)
        inside = dot(lower, high) + dot(lower, mid) + dot(lower, low) + carry
        key_s[rows, :] = key
        ins_s[rows, :] = inside
        return inside[127:128, :]

    last = lax.fori_loop(0, TOK // 128, decays, jnp.zeros((1, KT), F32))

    def scaled(r, carry):
        rows = pl.ds(pl.multiple_of(r * 128, 128), 128)
        ask = jnp.concatenate([qa_ref[rows, :].astype(F32), qb_ref[rows, :].astype(F32)], axis=1)
        key = key_s[rows, :]
        inside = ins_s[rows, :]
        qd_s[rows, :] = (ask * sigmoid(ask) * jnp.exp(inside)).astype(BF16)
        kg_s[rows, :] = (key * jnp.exp(-inside)).astype(BF16)
        wk_s[rows, :] = (key * jnp.exp(last - inside)).astype(BF16)
        return carry

    for copy in inputs[6:9]:
        copy.wait()
    lax.fori_loop(0, TOK // 128, scaled, 0)
    summed = dot_tn(v_ref[...], wk_s[...])
    state = jnp.concatenate([summed[0:64, 0:128], summed[64:128, 128:KT]], axis=1)

    def packed(buf, place, state, total):
        rows3 = iota((8, KT), 0)
        high, mid, low = (part.astype(F32) for part in split3(total))
        lines = jnp.where(rows3 == 0, high, jnp.where(rows3 == 1, mid, jnp.where(rows3 == 2, low, 0.0)))
        buf[place, 0:64, :] = state.astype(BF16)
        buf[place, 64:72, :] = lines.astype(BF16)

    def unpacked(buf, place):
        lines = buf[place, 64:72, :].astype(F32)
        return buf[place, 0:64, :].astype(F32), lines[0:1] + lines[1:2] + lines[2:3]

    packed(buf1, x, state, last)
    clus_s[z] = jnp.zeros((8, 128), F32)
    clus_s[z, :, 0:ROWS] = jnp.broadcast_to(cluster_ref[...].astype(F32), (8, ROWS))
    pl.semaphore_wait(barrier, NS - 1 + NZ)

    def along_x(d):
        return remote(buf1.at[x], buf1.at[x], s1s, s1r.at[x], y * NX + lax.rem(x + d, NX), t)

    def from_x(d):
        there = lax.rem(x + d, NX)
        return remote(buf1.at[there], buf1.at[there], s1s, s1r.at[there], y * NX + there, t)

    for d in (2, 1, 3):
        along_x(d).start()

    shared = [
        (alpha_ref, wproj.at[1, pl.ds(0, 64)]), (beta_ref, wproj.at[1, pl.ds(64, 64)]),
        (sw_ref.at[0], swv.at[1]), (ex_ref.at[0], exv.at[1]), (co_ref.at[0], cov.at[1]),
    ]
    shared = [remote(a, b, wssem.at[k], wrsem.at[k], s, sibling) for k, (a, b) in enumerate(shared)]
    for copy in shared[:4]:
        copy.start()

    def share_groups(d):
        return remote(
            clus_s.at[z], clus_s.at[z], cls, clr, s, lax.rem(z + d, NZ) * 2 + c
        )

    def shared_groups():
        most = pl.ds(0, NZ - 1)
        return remote(clus_s.at[most], clus_s.at[most], cls, clr, s, ahead)

    def each(action, count=NS):
        def body(d, carry):
            action(d)
            return carry

        lax.fori_loop(1, count, body, 0)

    each(lambda d: share_groups(d).start(), NZ)
    left_half = iota((256, 128), 1) < 64

    def intra(columns, first):
        for block in range(2):
            rows, width = slice(block * 256, block * 256 + 256), 256 * (block + 1)
            scores = dot_nt(qd_s[rows, columns], kg_s[0:width, columns])
            causal = iota((256, width), 0) + 256 * block >= iota((256, width), 1)
            scores = jnp.where(causal, scores, 0.0).astype(BF16)
            found = dot(scores, v_ref[0:width, :])
            intra_s[rows, :] = found if first else jnp.where(left_half, intra_s[rows, :], found)

    for copy in inputs[9:]:
        copy.wait()
    intra(slice(0, 128), True)

    for d in range(1, NX):
        from_x(d).wait_recv()
    sofar, gone = jnp.zeros((64, KT), F32), jnp.zeros((1, KT), F32)
    before, before_gone = sofar, gone
    for k in range(NX):
        before = jnp.where(x == k, sofar, before)
        before_gone = jnp.where(x == k, gone, before_gone)
        piece, total = unpacked(buf1, k)
        sofar = jnp.exp(total) * sofar + piece
        gone = gone + total
    packed(buf2, y, sofar, gone)
    row_s[...] = jnp.zeros_like(row_s)

    def along_y(d):
        return remote(buf2.at[y], buf2.at[y], s2s.at[d], s2r.at[y], (y + d) * NX + x, t)

    def from_y(k):
        return remote(buf2.at[k], buf2.at[k], s2s.at[0], s2r.at[k], k * NX + x, t)

    for d in range(1, NY):
        @pl.when(y + d < NY)
        def _():
            along_y(d).start()

    intra(slice(128, KT), False)

    for k in range(NY - 1):
        @pl.when(k < y)
        def _():
            from_y(k).wait_recv()
            piece, total = unpacked(buf2, k)
            row_s[...] = jnp.exp(total) * row_s[...] + piece

    carried = jnp.exp(before_gone) * row_s[...] + before
    is_left = iota((64, KT), 1) < 128
    carried = jnp.concatenate(
        [jnp.where(is_left, carried, 0.0), jnp.where(is_left, 0.0, carried)], axis=0
    ).astype(BF16)
    lane_gain = jnp.concatenate([lane_ref[...], lane_ref[...]], axis=1)
    left = iota((128, 128), 1) < 64
    for r in range(TOK // 128):
        rows = slice(r * 128, r * 128 + 128)
        raw = intra_s[rows, :] + dot_nt(qd_s[rows, :], carried)
        squares = raw * raw
        mean_a = jnp.sum(jnp.where(left, squares, 0.0), axis=1, keepdims=True) * (1.0 / 64)
        mean_b = jnp.sum(jnp.where(left, 0.0, squares), axis=1, keepdims=True) * (1.0 / 64)
        mean = jnp.where(left, mean_a, mean_b)
        head = raw * lax.rsqrt(mean + EPSILON) * lane_gain * sigmoid(gate_ref[rows, :].astype(F32))
        head = head.astype(BF16)
        for q in range(4):
            at = (2 * r + q // 2) * 32
            hd_s[q % 2, at : at + 32, :] = head[q * 32 : q * 32 + 32, :]

    swap = remote(hd_s.at[1 - c], hrecv, hs, hr, s, sibling)
    swap.start()
    for copy in own_weights[:2]:
        copy.wait()
    p_s[...] = dot(hd_s[c], wproj[0])
    for copy in shared[:2]:
        copy.wait_recv()
    swap.wait_recv()
    p_s[...] = p_s[...] + dot(hrecv[...], wproj[1])

    HALF = ROWS // DCH

    def ring_d(k, j):
        part = pl.ds(j * HALF, HALF)
        return remote(
            dsend.at[k, part], drecv.at[k, part], dss, drs.at[k, j], s,
            ahead if k < FAR else behind,
        )

    def send_d(k, j, first):
        place = FAR - k if k < FAR else -(NEAR - (k - FAR))
        target = lax.rem(z + way * place + NZ, NZ)
        rows = pl.ds(pl.multiple_of(target * ROWS + j * HALF, HALF), HALF)
        value = p_s[rows, :]
        if not first:
            ring_d(k - 1, j).wait_recv()
            value = value + drecv[k - 1, j * HALF : (j + 1) * HALF, :].astype(F32)
        dsend[k, j * HALF : (j + 1) * HALF, :] = value.astype(BF16)
        ring_d(k, j).start()

    def slots_of(r, carry):
        there = lax.rem(z + way * r + NZ, NZ)
        group_row = jnp.broadcast_to(clus_s[there, 0:1, 0:ROWS], (ROWS, ROWS))
        diagonal = iota((ROWS, ROWS), 0) == iota((ROWS, ROWS), 1)
        group_column = jnp.sum(jnp.where(diagonal, group_row, 0.0), axis=1, keepdims=True)
        same = jnp.where(group_row == group_column, 1.0, 0.0)
        earlier_row = iota((ROWS, ROWS), 0) < iota((ROWS, ROWS), 1)
        rank_row = jnp.sum(jnp.where(earlier_row, same, 0.0), axis=0, keepdims=True)
        earlier_column = iota((ROWS, ROWS), 1) < iota((ROWS, ROWS), 0)
        rank_column = jnp.sum(jnp.where(earlier_column, same, 0.0), axis=1, keepdims=True)
        slot_row = group_row[0:1, :] * CAP + rank_row
        slot_column = group_column * CAP + rank_column
        place_s[r] = jnp.where(
            iota((SLOTS, ROWS), 0).astype(F32) == slot_row, 1.0, 0.0
        ).astype(BF16)
        unplace_s[r] = jnp.where(
            iota((ROWS, SLOTS), 1).astype(F32) == slot_column, 1.0, 0.0
        ).astype(BF16)
        return carry

    for step in range(FAR):
        for j in range(DCH):
            send_d(step, j, step == 0)
            if step < NEAR:
                send_d(FAR + step, j, step == 0)
        if step == 0:
            shared[4].start()
            shared_groups().wait_recv()
            lax.fori_loop(0, NZ, slots_of, 0)
    mixed = p_s[pl.ds(pl.multiple_of(z * ROWS, ROWS), ROWS), :]
    for k in (FAR + NEAR - 1, FAR - 1):
        for j in range(DCH):
            ring_d(k, j).wait_recv()
        mixed = mixed + drecv[k].astype(F32)

    h_mid = (skip_ref[...].astype(F32) + rms(mixed, post_ref[...])).astype(BF16).astype(F32)
    hmid_s[...] = h_mid
    nz_s[0] = rms(h_mid, pre_ref[...]).astype(BF16)

    lines3 = conv_s.reshape(SLOTS, PITCH, 128)
    own = pl.ds(s * CAP, CAP)

    def slots_for(k):
        return pl.ds(k * CAP, CAP)

    def to_lines(value):
        for i in range(LINES):
            conv_s[pl.ds(i, SLOTS, stride=PITCH), :] = value[:, i * 128 : i * 128 + 128]
        return lines3[:, 0:LINES, :].astype(BF16)

    def from_lines(value, at):
        lines3[:, 0:LINES, :] = value.astype(F32)
        for i in range(LINES):
            x_s[at : at + SLOTS, i * 128 : i * 128 + 128] = conv_s[
                pl.ds(i, SLOTS, stride=PITCH), :
            ].astype(BF16)

    def at_offset(dy, dx):
        return lax.rem(y + dy, NY) * NX + lax.rem(x + dx, NX)

    def far_first(action):
        middle = 2 * NX + 2

        def body(i, carry):
            i = i + jnp.where(i >= middle, 1, 0)
            action(at_offset(lax.rem(2 + i // NX, NY), lax.rem(2 + lax.rem(i, NX), NX)))
            return carry

        lax.fori_loop(0, NS - 1, body, 0)

    def all_but_own(src, dst, r, ssem, rsem):
        most = pl.ds(0, SLOTS - CAP)
        return remote(src.at[r, most], dst.at[r, most], ssem, rsem, lax.rem(s + 1, NS), t)

    def scatter(src, dst, r, ssem, rsem):
        far_first(
            lambda there: remote(
                src.at[r, slots_for(there)], dst.at[r, own], ssem, rsem, there, t
            ).start()
        )
        dst[r, own] = src[r, own]

    def near_slots(p):
        return pl.ds(p * CAP, CAP)

    def scatter_in(src, dst):
        for dy, dx in reversed(OFFSETS[1:]):
            there = at_offset(dy, dx)
            p = OFFSETS.index(((-dy) % NY, (-dx) % NX))
            remote(
                src.at[0, slots_for(there)], dst.at[0, near_slots(p)], zos, xir.at[p // (NS // ACH)],
                there, t,
            ).start()
        dst[0, 0:CAP] = src[0, own]

    def scattered_in(src, dst, q):
        first = 1 if q == 0 else q * (NS // ACH)
        part = pl.ds(first * CAP, ((q + 1) * (NS // ACH) - first) * CAP)
        return remote(src.at[0, part], dst.at[0, part], zos, xir.at[q], lax.rem(s + 1, NS), t)

    def scatter_back(src, dst, r, ssem, rsem):
        for p in range(NS - 1, 0, -1):
            there = at_offset(*OFFSETS[p])
            remote(src.at[r, near_slots(p)], dst.at[r, own], ssem, rsem, there, t).start()
        dst[r, own] = src[r, 0:CAP]

    def returned(r):
        all_but_own(fin_rt, ret_rt, r, zis, zir.at[r]).wait_recv()
        at = PLACE[r] * SLOTS
        from_lines(ret_rt[r], at)
        return dot(unplace_s[r], x_s[at : at + SLOTS, :])

    for copy in own_weights[2:]:
        copy.wait()
    router = router_ref[...].astype(F32)
    router_rows = iota((16, D), 0)
    router = jnp.where(
        router_rows == 0, router[0:1], jnp.where(router_rows == 1, router[1:2], 0.0)
    ).astype(BF16)
    member = z // (NZ // 2)

    def part_of(r):
        return part_s[PLACE[r] * SLOTS : PLACE[r] * SLOTS + SLOTS, :]

    def compute(places):
        for place in places:
            from_lines(x_rt[place], PLACE[place] * SLOTS)
        at, size = PLACE[places[0]] * SLOTS, SLOTS * len(places)
        rows = x_s[at : at + size, :]
        scores = sigmoid(dot_nt(rows, router))
        first, second = scores[:, 0:1], scores[:, 1:2]
        weight = jnp.where(member == 0, first, second) / (first + second)
        total = None
        for u in range(2):
            gate = dot(rows, swv[u])
            hidden = (gate * sigmoid(gate) * dot(rows, exv[u])).astype(BF16)
            term = dot(hidden, cov[u])
            total = term if total is None else total + term
        part_s[at : at + size, :] = total * weight

    def gather(buf, chunk):
        def copy(k, j):
            source = (NZ - k) % NZ if k < FAR else k - FAR
            target = (source + NZ - 1) % NZ if k < FAR else source + 1
            part = pl.ds(j * chunk, chunk)
            return remote(
                buf.at[source, part], buf.at[target, part], ags, agr.at[k, j], s,
                ahead if k < FAR else behind,
            )

        return copy

    def gather_step(ring, k, chunks):
        for j in range(chunks):
            ring(k, j).wait_recv()
            if k + 1 < FAR:
                ring(k + 1, j).start()
            if k < NEAR:
                ring(FAR + k, j).wait_recv()
                if k + 1 < NEAR:
                    ring(FAR + k + 1, j).start()

    def reduce(values, chunk):
        def copy(k, j):
            part = pl.ds(j * chunk, chunk)
            return remote(
                gsend.at[k, part], grecv.at[k, part], gss, grs.at[k, j], s,
                ahead if k < FAR else behind,
            )

        def send(k, j, first):
            place = FAR - k if k < FAR else NZ - (NEAR - (k - FAR))
            rows = slice(j * chunk, (j + 1) * chunk)
            value = values(place, rows)
            if not first:
                copy(k - 1, j).wait_recv()
                value = value + grecv[k - 1, rows, :].astype(F32)
            gsend[k, rows, :] = value.astype(BF16)
            copy(k, j).start()

        return copy, send

    def reduce_rest(copy, send, chunks, start):
        for step in range(1, FAR):
            for j in range(chunks):
                if step < NEAR:
                    send(FAR + step, j, False)
                send(step, j, False)
        total = start()
        size = total.shape[0]
        for k in (FAR + NEAR - 1, FAR - 1):
            for j in range(chunks):
                copy(k, j).wait_recv()
            total = total + grecv[k, 0:size, :].astype(F32)
        return total

    sides = [(NZ - 1 - k, k + 1) if k < NEAR else (NZ - 1 - k,) for k in range(FAR)]

    @pl.when(c == 0)
    def _():
        ring = gather(x_rt, SLOTS // ACH)
        out_rt[0] = to_lines(dot(place_s[0], nz_s[0]))
        scatter_in(out_rt, x_rt)
        for copy in shared[2:]:
            copy.wait_recv()
        for j in range(ACH):
            scattered_in(out_rt, x_rt, j).wait_recv()
            ring(0, j).start()
            ring(FAR, j).start()

        def back(places):
            compute(places)
            for r in places:
                fin_rt[r] = to_lines(part_of(r))
                scatter_back(fin_rt, ret_rt, r, zis, zir.at[r])

        back((0,))
        for k in range(FAR):
            gather_step(ring, k, ACH)
            back(sides[k])
        copy, send = reduce(lambda place, rows: qz_s[place, rows, :], ROWS // ZCH)
        for r in (0, 7, 1, 6, 2, 5):
            qz_s[r] = returned(r)
        for j in range(ZCH):
            send(FAR, j, True)
        for r in (3, 4):
            qz_s[r] = returned(r)
        for j in range(ZCH):
            send(0, j, True)
        routed = reduce_rest(copy, send, ZCH, lambda: qz_s[0])
        out_ref[...] = (hmid_s[...] + rms(routed, postmix_ref[...])).astype(BF16)
        all_but_own(out_rt, x_rt, 0, zos, xir.at[0]).wait_send()
        most = pl.ds(0, SLOTS - CAP)
        remote(
            fin_rt.at[:, most], ret_rt.at[:, most], zis, zir.at[0], lax.rem(s + 1, NS), t
        ).wait_send()
        around = pl.ds(0, FAR + NEAR)
        remote(x_rt.at[around], x_rt.at[around], ags, agr.at[0, 0], s, ahead).wait_send()
        rows = pl.ds(0, ROWS)
        remote(gsend.at[:, rows], grecv.at[:, rows], gss, grs.at[0, 0], s, ahead).wait_send()

    @pl.when(c == 1)
    def _():
        ring = gather(nz_s, ROWS // ZCH)
        for j in range(ZCH):
            ring(0, j).start()
            ring(FAR, j).start()

        def dispatch(r):
            out_rt[r] = to_lines(dot(place_s[r], nz_s[r]))
            scatter(out_rt, x_rt, r, zos, zor.at[r])

        def work(places):
            for r in places:
                all_but_own(out_rt, x_rt, r, zos, zor.at[r]).wait_recv()
            compute(places)

        dispatch(0)
        for copy in shared[2:]:
            copy.wait_recv()
        for k in range(FAR):
            gather_step(ring, k, ZCH)
            for r in sides[k]:
                dispatch(r)
            if k == 1:
                work((0,))
            elif k == 2:
                work(sides[0])
        copy, send = reduce(
            lambda place, rows: part_s[
                PLACE[place] * SLOTS + rows.start : PLACE[place] * SLOTS + rows.stop, :
            ],
            SLOTS // GCH,
        )
        work(sides[1])
        work(sides[2])
        for j in range(GCH):
            send(FAR, j, True)
        work(sides[3])
        for j in range(GCH):
            send(0, j, True)
        final = reduce_rest(copy, send, GCH, lambda: part_of(0))
        fin_rt[0] = to_lines(final)
        scatter(fin_rt, ret_rt, 0, zis, zir.at[0])
        routed = returned(0)
        out_ref[...] = (hmid_s[...] + rms(routed, postmix_ref[...])).astype(BF16)
        most = pl.ds(0, SLOTS - CAP)
        remote(
            out_rt.at[:, most], x_rt.at[:, most], zos, zor.at[0], lax.rem(s + 1, NS), t
        ).wait_send()
        all_but_own(fin_rt, ret_rt, 0, zis, zir.at[0]).wait_send()
        around = pl.ds(0, FAR + NEAR)
        remote(nz_s.at[around], nz_s.at[around], ags, agr.at[0, 0], s, ahead).wait_send()
        remote(gsend, grecv, gss, grs.at[0, 0], s, ahead).wait_send()

    remote(
        buf1.at[pl.ds(0, NX - 1)], buf1.at[pl.ds(0, NX - 1)], s1s, s1r.at[0], s, sibling
    ).wait_send()
    for d in range(1, NY):
        @pl.when(y + d < NY)
        def _():
            along_y(d).wait_send()
    shared_groups().wait_send()
    for copy in shared:
        copy.wait_send()
    swap.wait_send()
    remote(dsend, drecv, dss, drs.at[0, 0], s, ahead).wait_send()


def shards(
    ask_left, keep_left, gap_left, ask_right, keep_right, gap_right, payload, switch_logits,
    keep_bias, lanewise, alpha, beta, skip, post, pre, postmix, router, switch, expansion,
    contraction, cluster,
):
    inputs = (
        keep_left, keep_right, gap_left.reshape(1, -1), gap_right.reshape(1, -1), keep_bias.T,
        cluster.reshape(1, -1), ask_left, ask_right, payload, switch_logits,
        lanewise.reshape(1, -1), skip, post.reshape(1, -1), pre.reshape(1, -1),
        postmix.reshape(1, -1), router.T,
    )
    vmem = pl.BlockSpec(memory_space=pltpu.VMEM)
    hbm = pl.BlockSpec(memory_space=pl.ANY)
    ring = FAR + NEAR
    dma = pltpu.SemaphoreType.DMA
    return pl.pallas_call(
        kernel,
        out_shape=pltpu.VMEM((ROWS, D), BF16),
        in_specs=[hbm] * 21,
        out_specs=vmem,
        scratch_shapes=[
            *(pltpu.VMEM(a.shape, a.dtype) for a in inputs),
            dma((16,)),
            pltpu.VMEM((TOK, KT), F32),
            pltpu.VMEM((TOK, KT), F32),
            pltpu.VMEM((TOK, KT), BF16),
            pltpu.VMEM((TOK, KT), BF16),
            pltpu.VMEM((TOK, KT), BF16),
            pltpu.VMEM((TOK, 128), F32),
            pltpu.VMEM((NX, 72, KT), BF16),
            pltpu.VMEM((NY, 72, KT), BF16),
            pltpu.VMEM((64, KT), F32),
            pltpu.VMEM((2, TOK // 2, 128), BF16),
            pltpu.VMEM((TOK // 2, 128), BF16),
            pltpu.VMEM((2, 128, D), BF16),
            pltpu.VMEM((TOK // 2, D), F32),
            pltpu.VMEM((ring, ROWS, D), BF16),
            pltpu.VMEM((ring, ROWS, D), BF16),
            pltpu.VMEM((ROWS, D), F32),
            pltpu.VMEM((NZ, SLOTS, LINES, 128), BF16),
            pltpu.VMEM((NZ, SLOTS, LINES, 128), BF16),
            pltpu.VMEM((SLOTS * PITCH, 128), F32),
            pltpu.VMEM((NZ * SLOTS, D), BF16),
            pltpu.VMEM((NZ * SLOTS, D), F32),
            pltpu.VMEM((2, D, HID), BF16),
            pltpu.VMEM((2, D, HID), BF16),
            pltpu.VMEM((2, HID, D), BF16),
            pltpu.VMEM((ring, SLOTS, D), BF16),
            pltpu.VMEM((ring, SLOTS, D), BF16),
            pltpu.VMEM((NZ, SLOTS, LINES, 128), BF16),
            pltpu.VMEM((NZ, SLOTS, LINES, 128), BF16),
            pltpu.VMEM((NZ, 8, 128), F32),
            pltpu.VMEM((NZ, SLOTS, ROWS), BF16),
            pltpu.VMEM((NZ, ROWS, SLOTS), BF16),
            pltpu.VMEM((NZ, ROWS, D), BF16),
            pltpu.VMEM((NZ, ROWS, D), F32),
            dma, dma,
            dma, dma((NZ,)), dma, dma((NZ,)), dma((ACH,)),
            dma((5,)), dma((5,)), dma((5,)),
            dma, dma((NX,)), dma((NY,)), dma((NY,)),
            dma, dma,
            dma, dma((ring, DCH)),
            dma, dma((ring, max(ACH, ZCH))),
            dma, dma((ring, GCH)),
        ],
        compiler_params=pltpu.CompilerParams(
            collective_id=0, has_side_effects=True, vmem_limit_bytes=56 * 1024 * 1024
        ),
    )(
        *inputs, alpha, beta, switch, expansion, contraction,
    )


def solution(mesh):
    placed = (
        P("sp", "tp"),
        P("sp", "tp"),
        P("tp"),
        P("sp", "tp"),
        P("sp", "tp"),
        P("tp"),
        P("sp", "tp"),
        P("sp", "tp"),
        P("sp", "tp"),
        P(),
        P("tp", None),
        P("tp", None),
        P(("sp", "tp"), None),
        P(),
        P(),
        P(),
        P(None, "sp"),
        P("sp", None, "tp"),
        P("sp", None, "tp"),
        P("sp", "tp", None),
        P(("sp", "tp")),
    )
    return jax.shard_map(
        shards, mesh=mesh, in_specs=placed, out_specs=P(("sp", "tp"), None), check_vma=False
    )
```

```python
import functools

import jax
import jax.numpy as jnp
from jax import lax
from jax.experimental import pallas as pl
from jax.experimental.pallas import tpu as pltpu
from jax.sharding import PartitionSpec as P

EPSILON = 1e-06
NX, NY, NZ = 4, 4, 8
NS = NX * NY
D = 2048
KT = 384
TOK = 512
ROWS = 32
CAP = 3
SLOTS = NS * CAP
LINES = D // 128
HID = 256
FAR, NEAR = NZ // 2, NZ // 2 - 1
PLACE = {0: 0, 7: 1, 1: 2, 6: 3, 2: 4, 5: 5, 3: 6, 4: 7}
PITCH = 24
OFFSETS = sorted(
    ((dy, dx) for dy in range(NY) for dx in range(NX)),
    key=lambda o: min(o[0], NY - o[0]) + min(o[1], NX - o[1]),
)
DCH, GCH, ZCH, ACH = 8, 6, 4, 8
MESH = pl.DeviceIdType.MESH
F32, BF16 = jnp.float32, jnp.bfloat16


def dot(a, b):
    return jnp.dot(a, b, preferred_element_type=F32)


def dot_nt(a, b):
    return lax.dot_general(a, b, (((1,), (1,)), ((), ())), preferred_element_type=F32)


def dot_tn(a, b):
    return lax.dot_general(a, b, (((0,), (0,)), ((), ())), preferred_element_type=F32)


def sigmoid(v):
    return 1.0 / (1.0 + jnp.exp(-v))


def rms(v, gain):
    return v * lax.rsqrt(jnp.mean(v * v, axis=-1, keepdims=True) + EPSILON) * gain


def split3(v):
    high = v.astype(BF16)
    rest = v - high.astype(F32)
    mid = rest.astype(BF16)
    low = (rest - mid.astype(F32)).astype(BF16)
    return high, mid, low


def iota(shape, dim):
    return lax.broadcasted_iota(jnp.int32, shape, dim)


def kernel(
    fa_hbm, fb_hbm, ga_hbm, gb_hbm, bias_hbm, cluster_hbm, qa_hbm, qb_hbm, v_hbm,
    gate_hbm, lane_hbm, skip_hbm, post_hbm, pre_hbm, postmix_hbm, router_hbm,
    alpha_ref, beta_ref, sw_ref, ex_ref, co_ref,
    out_ref,
    fa_ref, fb_ref, ga_ref, gb_ref, bias_ref, cluster_ref, qa_ref, qb_ref, v_ref,
    gate_ref, lane_ref, skip_ref, post_ref, pre_ref, postmix_ref, router_ref, insem,
    key_s, ins_s, qd_s, kg_s, wk_s, intra_s, buf1, buf2, row_s, hd_s, hrecv, wproj, p_s,
    dsend, drecv, hmid_s, out_rt, x_rt, conv_s, x_s, part_s, swv, exv, cov, gsend, grecv, ret_rt, fin_rt,
    clus_s, place_s, unplace_s, nz_s, qz_s,
    cls, clr, zos, zor, zis, zir, xir,
    wsem, wssem, wrsem, s1s, s1r, s2s, s2r, hs, hr, dss, drs, ags, agr, gss, grs,
):
    s = lax.axis_index("sp")
    t = lax.axis_index("tp")
    y, x = s // NX, lax.rem(s, NX)
    z, c = t // 2, lax.rem(t, 2)
    way = 1 - 2 * c
    ahead = lax.rem(z + way + NZ, NZ) * 2 + c
    behind = lax.rem(z - way + NZ, NZ) * 2 + c
    sibling = z * 2 + 1 - c

    def remote(src, dst, ssem, rsem, sp, tp):
        return pltpu.make_async_remote_copy(
            src_ref=src, dst_ref=dst, send_sem=ssem, recv_sem=rsem,
            device_id=(sp, tp), device_id_type=MESH,
        )

    barrier = pltpu.get_barrier_semaphore()

    def greet(d, carry):
        pl.semaphore_signal(barrier, inc=1, device_id=(lax.rem(s + d, NS), t), device_id_type=MESH)
        return carry

    lax.fori_loop(1, NS, greet, 0)

    def greet_z(d, carry):
        peer = lax.rem(z + d, NZ) * 2 + c
        pl.semaphore_signal(barrier, inc=1, device_id=(s, peer), device_id_type=MESH)
        return carry

    lax.fori_loop(1, NZ, greet_z, 0)
    pl.semaphore_signal(barrier, inc=1, device_id=(s, sibling), device_id_type=MESH)

    inputs = [
        pltpu.make_async_copy(a, b, insem.at[k])
        for k, (a, b) in enumerate(
            [
                (fa_hbm, fa_ref), (fb_hbm, fb_ref), (ga_hbm, ga_ref), (gb_hbm, gb_ref),
                (bias_hbm, bias_ref), (cluster_hbm, cluster_ref), (qa_hbm, qa_ref),
                (qb_hbm, qb_ref), (v_hbm, v_ref), (gate_hbm, gate_ref), (lane_hbm, lane_ref),
                (skip_hbm, skip_ref), (post_hbm, post_ref), (pre_hbm, pre_ref),
                (postmix_hbm, postmix_ref), (router_hbm, router_ref),
            ]
        )
    ]
    for copy in inputs:
        copy.start()
    own_weights = [
        pltpu.make_async_copy(alpha_ref, wproj.at[0, pl.ds(0, 64)], wsem.at[0]),
        pltpu.make_async_copy(beta_ref, wproj.at[0, pl.ds(64, 64)], wsem.at[1]),
        pltpu.make_async_copy(sw_ref.at[0], swv.at[0], wsem.at[2]),
        pltpu.make_async_copy(ex_ref.at[0], exv.at[0], wsem.at[3]),
        pltpu.make_async_copy(co_ref.at[0], cov.at[0], wsem.at[4]),
    ]
    for copy in own_weights:
        copy.start()

    for copy in inputs[:6]:
        copy.wait()
    gap = jnp.concatenate([ga_ref[...], gb_ref[...]], axis=1)
    lower = jnp.where(iota((128, 128), 0) >= iota((128, 128), 1), 1.0, 0.0).astype(BF16)

    def decays(r, carry):
        rows = slice(r * 128, r * 128 + 128)
        forget = jnp.concatenate([fa_ref[rows, :].astype(F32), fb_ref[rows, :].astype(F32)], axis=1)
        key = gap * sigmoid(-forget)
        left = jnp.broadcast_to(bias_ref[0:1, rows], (128, 128)).T
        right = jnp.broadcast_to(bias_ref[1:2, rows], (128, 128)).T
        logf = jnp.log1p(-key) + jnp.concatenate([left, right, right], axis=1)
        high, mid, _ = split3(logf)
        inside = dot(lower, high) + dot(lower, mid) + carry
        key_s[rows, :] = key
        ins_s[rows, :] = inside
        return inside[127:128, :]

    last = jnp.zeros((1, KT), F32)
    for r in range(TOK // 128):
        last = decays(r, last)

    def scaled(r, carry):
        rows = slice(r * 128, r * 128 + 128)
        ask = jnp.concatenate([qa_ref[rows, :].astype(F32), qb_ref[rows, :].astype(F32)], axis=1)
        key = key_s[rows, :]
        inside = ins_s[rows, :]
        qd_s[rows, :] = (ask * sigmoid(ask) * jnp.exp(inside)).astype(BF16)
        kg_s[rows, :] = (key * jnp.exp(-inside)).astype(BF16)
        wk_s[rows, :] = (key * jnp.exp(last - inside)).astype(BF16)
        return carry

    for copy in inputs[6:9]:
        copy.wait()
    for r in range(TOK // 128):
        scaled(r, 0)
    summed = dot_tn(v_ref[...], wk_s[...])
    state = jnp.concatenate([summed[0:64, 0:128], summed[64:128, 128:KT]], axis=1)

    def packed(buf, place, state, total):
        rows3 = iota((8, KT), 0)
        high, mid, low = (part.astype(F32) for part in split3(total))
        lines = jnp.where(rows3 == 0, high, jnp.where(rows3 == 1, mid, jnp.where(rows3 == 2, low, 0.0)))
        buf[place, 0:64, :] = state.astype(BF16)
        buf[place, 64:72, :] = lines.astype(BF16)

    def unpacked(buf, place):
        lines = buf[place, 64:72, :].astype(F32)
        return buf[place, 0:64, :].astype(F32), lines[0:1] + lines[1:2] + lines[2:3]

    packed(buf1, x, state, last)
    clus_s[z] = jnp.zeros((8, 128), F32)
    clus_s[z, :, 0:ROWS] = jnp.broadcast_to(cluster_ref[...].astype(F32), (8, ROWS))
    pl.semaphore_wait(barrier, NS - 1 + NZ)

    def along_x(d):
        return remote(buf1.at[x], buf1.at[x], s1s, s1r.at[x], y * NX + lax.rem(x + d, NX), t)

    def from_x(d):
        there = lax.rem(x + d, NX)
        return remote(buf1.at[there], buf1.at[there], s1s, s1r.at[there], y * NX + there, t)

    for d in (2, 1, 3):
        along_x(d).start()

    shared = [
        (alpha_ref, wproj.at[1, pl.ds(0, 64)]), (beta_ref, wproj.at[1, pl.ds(64, 64)]),
        (sw_ref.at[0], swv.at[1]), (ex_ref.at[0], exv.at[1]), (co_ref.at[0], cov.at[1]),
    ]
    shared = [remote(a, b, wssem.at[k], wrsem.at[k], s, sibling) for k, (a, b) in enumerate(shared)]
    for copy in shared[:4]:
        copy.start()

    def share_groups(d):
        return remote(
            clus_s.at[z], clus_s.at[z], cls, clr, s, lax.rem(z + d, NZ) * 2 + c
        )

    def shared_groups():
        most = pl.ds(0, NZ - 1)
        return remote(clus_s.at[most], clus_s.at[most], cls, clr, s, ahead)

    def each(action, count=NS):
        def body(d, carry):
            action(d)
            return carry

        lax.fori_loop(1, count, body, 0)

    each(lambda d: share_groups(d).start(), NZ)
    left_half = iota((256, 128), 1) < 64

    def intra(columns, first):
        for block in range(2):
            rows, width = slice(block * 256, block * 256 + 256), 256 * (block + 1)
            scores = dot_nt(qd_s[rows, columns], kg_s[0:width, columns])
            causal = iota((256, width), 0) + 256 * block >= iota((256, width), 1)
            scores = jnp.where(causal, scores, 0.0).astype(BF16)
            found = dot(scores, v_ref[0:width, :])
            intra_s[rows, :] = found if first else jnp.where(left_half, intra_s[rows, :], found)

    for copy in inputs[9:]:
        copy.wait()
    intra(slice(0, 128), True)

    for d in range(1, NX):
        from_x(d).wait_recv()
    sofar, gone = jnp.zeros((64, KT), F32), jnp.zeros((1, KT), F32)
    before, before_gone = sofar, gone
    for k in range(NX):
        before = jnp.where(x == k, sofar, before)
        before_gone = jnp.where(x == k, gone, before_gone)
        piece, total = unpacked(buf1, k)
        sofar = jnp.exp(total) * sofar + piece
        gone = gone + total
    packed(buf2, y, sofar, gone)
    row_s[...] = jnp.zeros_like(row_s)

    def along_y(d):
        return remote(buf2.at[y], buf2.at[y], s2s.at[d], s2r.at[y], (y + d) * NX + x, t)

    def from_y(k):
        return remote(buf2.at[k], buf2.at[k], s2s.at[0], s2r.at[k], k * NX + x, t)

    for d in (2, 3, 1):
        @pl.when(y + d < NY)
        def _():
            along_y(d).start()

    intra(slice(128, KT), False)

    for k in range(NY - 1):
        @pl.when(k < y)
        def _():
            from_y(k).wait_recv()
            piece, total = unpacked(buf2, k)
            row_s[...] = jnp.exp(total) * row_s[...] + piece

    carried = jnp.exp(before_gone) * row_s[...] + before
    is_left = iota((64, KT), 1) < 128
    carried = jnp.concatenate(
        [jnp.where(is_left, carried, 0.0), jnp.where(is_left, 0.0, carried)], axis=0
    ).astype(BF16)
    lane_gain = jnp.concatenate([lane_ref[...], lane_ref[...]], axis=1)
    left = iota((128, 128), 1) < 64
    for r in range(TOK // 128):
        rows = slice(r * 128, r * 128 + 128)
        raw = intra_s[rows, :] + dot_nt(qd_s[rows, :], carried)
        squares = raw * raw
        mean_a = jnp.sum(jnp.where(left, squares, 0.0), axis=1, keepdims=True) * (1.0 / 64)
        mean_b = jnp.sum(jnp.where(left, 0.0, squares), axis=1, keepdims=True) * (1.0 / 64)
        mean = jnp.where(left, mean_a, mean_b)
        head = raw * lax.rsqrt(mean + EPSILON) * lane_gain * sigmoid(gate_ref[rows, :].astype(F32))
        head = head.astype(BF16)
        for q in range(4):
            at = (2 * r + q // 2) * 32
            hd_s[q % 2, at : at + 32, :] = head[q * 32 : q * 32 + 32, :]

    swap = remote(hd_s.at[1 - c], hrecv, hs, hr, s, sibling)
    swap.start()
    for copy in own_weights[:2]:
        copy.wait()
    p_s[...] = dot(hd_s[c], wproj[0])
    for copy in shared[:2]:
        copy.wait_recv()
    swap.wait_recv()
    p_s[...] = p_s[...] + dot(hrecv[...], wproj[1])

    PIECE = 8

    def piece_d(j):
        return j // 2 * PIECE, slice(j % 2 * (D // 2), (j % 2 + 1) * (D // 2))

    def ring_d(k, j):
        first, columns = piece_d(j)
        part = (k, pl.ds(first, PIECE), pl.ds(columns.start, D // 2))
        return remote(
            dsend.at[part], drecv.at[part], dss, drs.at[k, j], s,
            ahead if k < FAR else behind,
        )

    def send_d(k, j, starts):
        place = FAR - k if k < FAR else -(NEAR - (k - FAR))
        target = lax.rem(z + way * place + NZ, NZ)
        first, columns = piece_d(j)
        rows = pl.ds(pl.multiple_of(target * ROWS + first, PIECE), PIECE)
        value = p_s[rows, columns]
        if not starts:
            ring_d(k - 1, j).wait_recv()
            value = value + drecv[k - 1, first : first + PIECE, columns].astype(F32)
        dsend[k, first : first + PIECE, columns] = value.astype(BF16)
        ring_d(k, j).start()

    def slots_of(r, carry):
        there = lax.rem(z + way * r + NZ, NZ)
        group_row = jnp.broadcast_to(clus_s[there, 0:1, 0:ROWS], (ROWS, ROWS))
        diagonal = iota((ROWS, ROWS), 0) == iota((ROWS, ROWS), 1)
        group_column = jnp.sum(jnp.where(diagonal, group_row, 0.0), axis=1, keepdims=True)
        same = jnp.where(group_row == group_column, 1.0, 0.0)
        earlier_row = iota((ROWS, ROWS), 0) < iota((ROWS, ROWS), 1)
        rank_row = jnp.sum(jnp.where(earlier_row, same, 0.0), axis=0, keepdims=True)
        earlier_column = iota((ROWS, ROWS), 1) < iota((ROWS, ROWS), 0)
        rank_column = jnp.sum(jnp.where(earlier_column, same, 0.0), axis=1, keepdims=True)
        slot_row = group_row[0:1, :] * CAP + rank_row
        slot_column = group_column * CAP + rank_column
        place_s[r] = jnp.where(
            iota((SLOTS, ROWS), 0).astype(F32) == slot_row, 1.0, 0.0
        ).astype(BF16)
        unplace_s[r] = jnp.where(
            iota((ROWS, SLOTS), 1).astype(F32) == slot_column, 1.0, 0.0
        ).astype(BF16)
        return carry

    for step in range(FAR):
        for j in range(DCH):
            send_d(step, j, step == 0)
            if step < NEAR:
                send_d(FAR + step, j, step == 0)
        if step == 0:
            shared[4].start()
            shared_groups().wait_recv()
            lax.fori_loop(0, NZ, slots_of, 0)
    mixed = p_s[pl.ds(pl.multiple_of(z * ROWS, ROWS), ROWS), :]
    for k in (FAR + NEAR - 1, FAR - 1):
        for j in range(DCH):
            ring_d(k, j).wait_recv()
        mixed = mixed + drecv[k].astype(F32)

    h_mid = (skip_ref[...].astype(F32) + rms(mixed, post_ref[...])).astype(BF16).astype(F32)
    hmid_s[...] = h_mid
    nz_s[0] = rms(h_mid, pre_ref[...]).astype(BF16)

    lines3 = conv_s.reshape(SLOTS, PITCH, 128)
    own = pl.ds(s * CAP, CAP)

    def slots_for(k):
        return pl.ds(k * CAP, CAP)

    def to_lines(value):
        for i in range(LINES):
            conv_s[pl.ds(i, SLOTS, stride=PITCH), :] = value[:, i * 128 : i * 128 + 128]
        return lines3[:, 0:LINES, :].astype(BF16)

    def from_lines(value, at):
        lines3[:, 0:LINES, :] = value.astype(F32)
        for i in range(LINES):
            x_s[at : at + SLOTS, i * 128 : i * 128 + 128] = conv_s[
                pl.ds(i, SLOTS, stride=PITCH), :
            ].astype(BF16)

    def at_offset(dy, dx):
        return lax.rem(y + dy, NY) * NX + lax.rem(x + dx, NX)

    def far_first(action):
        middle = 2 * NX + 2

        def body(i, carry):
            i = i + jnp.where(i >= middle, 1, 0)
            action(at_offset(lax.rem(2 + i // NX, NY), lax.rem(2 + lax.rem(i, NX), NX)))
            return carry

        lax.fori_loop(0, NS - 1, body, 0)

    def all_but_own(src, dst, r, ssem, rsem):
        most = pl.ds(0, SLOTS - CAP)
        return remote(src.at[r, most], dst.at[r, most], ssem, rsem, lax.rem(s + 1, NS), t)

    def scatter(src, dst, r, ssem, rsem):
        far_first(
            lambda there: remote(
                src.at[r, slots_for(there)], dst.at[r, own], ssem, rsem, there, t
            ).start()
        )
        dst[r, own] = src[r, own]

    def near_slots(p):
        return pl.ds(p * CAP, CAP)

    def scatter_in(src, dst):
        for dy, dx in reversed(OFFSETS[1:]):
            there = at_offset(dy, dx)
            p = OFFSETS.index(((-dy) % NY, (-dx) % NX))
            remote(
                src.at[0, slots_for(there)], dst.at[0, near_slots(p)], zos, xir.at[p // (NS // ACH)],
                there, t,
            ).start()
        dst[0, 0:CAP] = src[0, own]

    def scattered_in(src, dst, q):
        first = 1 if q == 0 else q * (NS // ACH)
        part = pl.ds(first * CAP, ((q + 1) * (NS // ACH) - first) * CAP)
        return remote(src.at[0, part], dst.at[0, part], zos, xir.at[q], lax.rem(s + 1, NS), t)

    def scatter_back(src, dst, r, ssem, rsem):
        for p in range(NS - 1, 0, -1):
            there = at_offset(*OFFSETS[p])
            remote(src.at[r, near_slots(p)], dst.at[r, own], ssem, rsem, there, t).start()
        dst[r, own] = src[r, 0:CAP]

    def returned(r):
        all_but_own(fin_rt, ret_rt, r, zis, zir.at[r]).wait_recv()
        at = PLACE[r] * SLOTS
        from_lines(ret_rt[r], at)
        return dot(unplace_s[r], x_s[at : at + SLOTS, :])

    for copy in own_weights[2:]:
        copy.wait()
    router = router_ref[...].astype(F32)
    router_rows = iota((16, D), 0)
    router = jnp.where(
        router_rows == 0, router[0:1], jnp.where(router_rows == 1, router[1:2], 0.0)
    ).astype(BF16)
    member = z // (NZ // 2)

    def part_of(r):
        return part_s[PLACE[r] * SLOTS : PLACE[r] * SLOTS + SLOTS, :]

    def hidden_of(places):
        for place in places:
            from_lines(x_rt[place], PLACE[place] * SLOTS)
        at = PLACE[places[0]] * SLOTS
        rows = x_s[at : at + SLOTS * len(places), :]
        scores = sigmoid(dot_nt(rows, router))
        first, second = scores[:, 0:1], scores[:, 1:2]
        weight = jnp.where(member == 0, first, second) / (first + second)
        hidden = []
        for u in range(2):
            gate = dot(rows, swv[u])
            hidden.append((gate * sigmoid(gate) * dot(rows, exv[u])).astype(BF16))
        return places, weight, hidden

    def contract(found):
        places, weight, hidden = found
        at = PLACE[places[0]] * SLOTS
        total = dot(hidden[0], cov[0]) + dot(hidden[1], cov[1])
        part_s[at : at + SLOTS * len(places), :] = total * weight

    def compute(places):
        contract(hidden_of(places))

    def gather(buf, chunk):
        def copy(k, j):
            source = (NZ - k) % NZ if k < FAR else k - FAR
            target = (source + NZ - 1) % NZ if k < FAR else source + 1
            part = pl.ds(j * chunk, chunk)
            return remote(
                buf.at[source, part], buf.at[target, part], ags, agr.at[k, j], s,
                ahead if k < FAR else behind,
            )

        return copy

    def gather_step(ring, k, chunks, meanwhile=()):
        for j in range(chunks):
            ring(k, j).wait_recv()
            if k + 1 < FAR:
                ring(k + 1, j).start()
            if k < NEAR:
                ring(FAR + k, j).wait_recv()
                if k + 1 < NEAR:
                    ring(FAR + k + 1, j).start()
            if j < len(meanwhile):
                meanwhile[j]()

    def reduce(values, chunk):
        def copy(k, j):
            part = pl.ds(j * chunk, chunk)
            return remote(
                gsend.at[k, part], grecv.at[k, part], gss, grs.at[k, j], s,
                ahead if k < FAR else behind,
            )

        def send(k, j, first):
            place = FAR - k if k < FAR else NZ - (NEAR - (k - FAR))
            rows = slice(j * chunk, (j + 1) * chunk)
            value = values(place, rows)
            if not first:
                copy(k - 1, j).wait_recv()
                value = value + grecv[k - 1, rows, :].astype(F32)
            gsend[k, rows, :] = value.astype(BF16)
            copy(k, j).start()

        return copy, send

    def reduce_rest(copy, send, chunks, start):
        for step in range(1, FAR):
            for j in range(chunks):
                if step < NEAR:
                    send(FAR + step, j, False)
                send(step, j, False)
        total = start()
        size = total.shape[0]
        for k in (FAR + NEAR - 1, FAR - 1):
            for j in range(chunks):
                copy(k, j).wait_recv()
            total = total + grecv[k, 0:size, :].astype(F32)
        return total

    sides = [(NZ - 1 - k, k + 1) if k < NEAR else (NZ - 1 - k,) for k in range(FAR)]

    @pl.when(c == 0)
    def _():
        ring = gather(x_rt, SLOTS // ACH)
        out_rt[0] = to_lines(dot(place_s[0], nz_s[0]))
        scatter_in(out_rt, x_rt)
        for copy in shared[2:]:
            copy.wait_recv()
        for j in range(ACH):
            scattered_in(out_rt, x_rt, j).wait_recv()
            ring(0, j).start()
            ring(FAR, j).start()

        def back(places):
            for r in places:
                fin_rt[r] = to_lines(part_of(r))
                scatter_back(fin_rt, ret_rt, r, zis, zir.at[r])

        compute((0,))
        back((0,))
        gather_step(ring, 0, ACH)
        for k in range(1, FAR):
            found = []
            gather_step(
                ring, k, ACH,
                (
                    lambda: found.append(hidden_of(sides[k - 1])),
                    lambda: contract(found[0]),
                    lambda: back(sides[k - 1]),
                ),
            )
        compute(sides[FAR - 1])
        back(sides[FAR - 1])
        copy, send = reduce(lambda place, rows: qz_s[place, rows, :], ROWS // ZCH)
        for r in (0, 7, 1, 6, 2, 5):
            qz_s[r] = returned(r)
        for j in range(ZCH):
            send(FAR, j, True)
        for r in (3, 4):
            qz_s[r] = returned(r)
        for j in range(ZCH):
            send(0, j, True)
        routed = reduce_rest(copy, send, ZCH, lambda: qz_s[0])
        out_ref[...] = (hmid_s[...] + rms(routed, postmix_ref[...])).astype(BF16)
        all_but_own(out_rt, x_rt, 0, zos, xir.at[0]).wait_send()
        most = pl.ds(0, SLOTS - CAP)
        remote(
            fin_rt.at[:, most], ret_rt.at[:, most], zis, zir.at[0], lax.rem(s + 1, NS), t
        ).wait_send()
        around = pl.ds(0, FAR + NEAR)
        remote(x_rt.at[around], x_rt.at[around], ags, agr.at[0, 0], s, ahead).wait_send()
        rows = pl.ds(0, ROWS)
        remote(gsend.at[:, rows], grecv.at[:, rows], gss, grs.at[0, 0], s, ahead).wait_send()

    @pl.when(c == 1)
    def _():
        ring = gather(nz_s, ROWS // ZCH)
        for j in range(ZCH):
            ring(0, j).start()
            ring(FAR, j).start()

        def dispatch(r):
            out_rt[r] = to_lines(dot(place_s[r], nz_s[r]))
            scatter(out_rt, x_rt, r, zos, zor.at[r])

        def work(places):
            for r in places:
                all_but_own(out_rt, x_rt, r, zos, zor.at[r]).wait_recv()
            compute(places)

        dispatch(0)
        for copy in shared[2:]:
            copy.wait_recv()
        for k in range(FAR):
            gather_step(ring, k, ZCH)
            for r in sides[k]:
                dispatch(r)
            if k == 1:
                work((0,))
        copy, send = reduce(
            lambda place, rows: part_s[
                PLACE[place] * SLOTS + rows.start : PLACE[place] * SLOTS + rows.stop, :
            ],
            SLOTS // GCH,
        )
        work(sides[0] + sides[1])
        work(sides[2])
        for j in range(GCH):
            send(FAR, j, True)
        work(sides[3])
        for j in range(GCH):
            send(0, j, True)
        final = reduce_rest(copy, send, GCH, lambda: part_of(0))
        fin_rt[0] = to_lines(final)
        scatter(fin_rt, ret_rt, 0, zis, zir.at[0])
        routed = returned(0)
        out_ref[...] = (hmid_s[...] + rms(routed, postmix_ref[...])).astype(BF16)
        most = pl.ds(0, SLOTS - CAP)
        remote(
            out_rt.at[:, most], x_rt.at[:, most], zos, zor.at[0], lax.rem(s + 1, NS), t
        ).wait_send()
        all_but_own(fin_rt, ret_rt, 0, zis, zir.at[0]).wait_send()
        around = pl.ds(0, FAR + NEAR)
        remote(nz_s.at[around], nz_s.at[around], ags, agr.at[0, 0], s, ahead).wait_send()
        remote(gsend, grecv, gss, grs.at[0, 0], s, ahead).wait_send()

    remote(
        buf1.at[pl.ds(0, NX - 1)], buf1.at[pl.ds(0, NX - 1)], s1s, s1r.at[0], s, sibling
    ).wait_send()
    for d in range(1, NY):
        @pl.when(y + d < NY)
        def _():
            along_y(d).wait_send()
    shared_groups().wait_send()
    for copy in shared:
        copy.wait_send()
    swap.wait_send()
    remote(dsend, drecv, dss, drs.at[0, 0], s, ahead).wait_send()


def shards(
    ask_left, keep_left, gap_left, ask_right, keep_right, gap_right, payload, switch_logits,
    keep_bias, lanewise, alpha, beta, skip, post, pre, postmix, router, switch, expansion,
    contraction, cluster,
):
    inputs = (
        keep_left, keep_right, gap_left.reshape(1, -1), gap_right.reshape(1, -1), keep_bias.T,
        cluster.reshape(1, -1), ask_left, ask_right, payload, switch_logits,
        lanewise.reshape(1, -1), skip, post.reshape(1, -1), pre.reshape(1, -1),
        postmix.reshape(1, -1), router.T,
    )
    vmem = pl.BlockSpec(memory_space=pltpu.VMEM)
    hbm = pl.BlockSpec(memory_space=pl.ANY)
    ring = FAR + NEAR
    dma = pltpu.SemaphoreType.DMA
    return pl.pallas_call(
        kernel,
        out_shape=pltpu.VMEM((ROWS, D), BF16),
        in_specs=[hbm] * 21,
        out_specs=vmem,
        scratch_shapes=[
            *(pltpu.VMEM(a.shape, a.dtype) for a in inputs),
            dma((16,)),
            pltpu.VMEM((TOK, KT), F32),
            pltpu.VMEM((TOK, KT), F32),
            pltpu.VMEM((TOK, KT), BF16),
            pltpu.VMEM((TOK, KT), BF16),
            pltpu.VMEM((TOK, KT), BF16),
            pltpu.VMEM((TOK, 128), F32),
            pltpu.VMEM((NX, 72, KT), BF16),
            pltpu.VMEM((NY, 72, KT), BF16),
            pltpu.VMEM((64, KT), F32),
            pltpu.VMEM((2, TOK // 2, 128), BF16),
            pltpu.VMEM((TOK // 2, 128), BF16),
            pltpu.VMEM((2, 128, D), BF16),
            pltpu.VMEM((TOK // 2, D), F32),
            pltpu.VMEM((ring, ROWS, D), BF16),
            pltpu.VMEM((ring, ROWS, D), BF16),
            pltpu.VMEM((ROWS, D), F32),
            pltpu.VMEM((NZ, SLOTS, LINES, 128), BF16),
            pltpu.VMEM((NZ, SLOTS, LINES, 128), BF16),
            pltpu.VMEM((SLOTS * PITCH, 128), F32),
            pltpu.VMEM((NZ * SLOTS, D), BF16),
            pltpu.VMEM((NZ * SLOTS, D), F32),
            pltpu.VMEM((2, D, HID), BF16),
            pltpu.VMEM((2, D, HID), BF16),
            pltpu.VMEM((2, HID, D), BF16),
            pltpu.VMEM((ring, SLOTS, D), BF16),
            pltpu.VMEM((ring, SLOTS, D), BF16),
            pltpu.VMEM((NZ, SLOTS, LINES, 128), BF16),
            pltpu.VMEM((NZ, SLOTS, LINES, 128), BF16),
            pltpu.VMEM((NZ, 8, 128), F32),
            pltpu.VMEM((NZ, SLOTS, ROWS), BF16),
            pltpu.VMEM((NZ, ROWS, SLOTS), BF16),
            pltpu.VMEM((NZ, ROWS, D), BF16),
            pltpu.VMEM((NZ, ROWS, D), F32),
            dma, dma,
            dma, dma((NZ,)), dma, dma((NZ,)), dma((ACH,)),
            dma((5,)), dma((5,)), dma((5,)),
            dma, dma((NX,)), dma((NY,)), dma((NY,)),
            dma, dma,
            dma, dma((ring, DCH)),
            dma, dma((ring, max(ACH, ZCH))),
            dma, dma((ring, GCH)),
        ],
        compiler_params=pltpu.CompilerParams(
            collective_id=0, has_side_effects=True, vmem_limit_bytes=56 * 1024 * 1024
        ),
    )(
        *inputs, alpha, beta, switch, expansion, contraction,
    )


def solution(mesh):
    placed = (
        P("sp", "tp"),
        P("sp", "tp"),
        P("tp"),
        P("sp", "tp"),
        P("sp", "tp"),
        P("tp"),
        P("sp", "tp"),
        P("sp", "tp"),
        P("sp", "tp"),
        P(),
        P("tp", None),
        P("tp", None),
        P(("sp", "tp"), None),
        P(),
        P(),
        P(),
        P(None, "sp"),
        P("sp", None, "tp"),
        P("sp", None, "tp"),
        P("sp", "tp", None),
        P(("sp", "tp")),
    )
    return jax.shard_map(
        shards, mesh=mesh, in_specs=placed, out_specs=P(("sp", "tp"), None), check_vma=False
    )
```

```python
import functools

import jax
import jax.numpy as jnp
from jax import lax
from jax.experimental import pallas as pl
from jax.experimental.pallas import tpu as pltpu
from jax.sharding import PartitionSpec as P

EPSILON = 1e-06
NX, NY, NZ = 4, 4, 8
NS = NX * NY
D = 2048
KT = 384
TOK = 512
ROWS = 32
CAP = 3
SLOTS = NS * CAP
LINES = D // 128
HID = 256
FAR, NEAR = NZ // 2, NZ // 2 - 1
PLACE = {0: 0, 7: 1, 1: 2, 6: 3, 2: 4, 5: 5, 3: 6, 4: 7}
PITCH = 24
OFFSETS = sorted(
    ((dy, dx) for dy in range(NY) for dx in range(NX)),
    key=lambda o: min(o[0], NY - o[0]) + min(o[1], NX - o[1]),
)
PIECE = 8
DCH, GCH, ZCH, ACH = 8, 6, 8, 8
MESH = pl.DeviceIdType.MESH
F32, BF16 = jnp.float32, jnp.bfloat16


def dot(a, b):
    return jnp.dot(a, b, preferred_element_type=F32)


def dot_nt(a, b):
    return lax.dot_general(a, b, (((1,), (1,)), ((), ())), preferred_element_type=F32)


def dot_tn(a, b):
    return lax.dot_general(a, b, (((0,), (0,)), ((), ())), preferred_element_type=F32)


def sigmoid(v):
    return 1.0 / (1.0 + jnp.exp(-v))


def rms(v, gain):
    return v * lax.rsqrt(jnp.mean(v * v, axis=-1, keepdims=True) + EPSILON) * gain


def split3(v):
    high = v.astype(BF16)
    rest = v - high.astype(F32)
    mid = rest.astype(BF16)
    low = (rest - mid.astype(F32)).astype(BF16)
    return high, mid, low


def iota(shape, dim):
    return lax.broadcasted_iota(jnp.int32, shape, dim)


def kernel(
    fa_hbm, fb_hbm, ga_hbm, gb_hbm, bias_hbm, cluster_hbm, qa_hbm, qb_hbm, v_hbm,
    gate_hbm, lane_hbm, skip_hbm, post_hbm, pre_hbm, postmix_hbm, router_hbm,
    alpha_ref, beta_ref, sw_ref, ex_ref, co_ref,
    out_ref,
    fa_ref, fb_ref, ga_ref, gb_ref, bias_ref, cluster_ref, qa_ref, qb_ref, v_ref,
    gate_ref, lane_ref, skip_ref, post_ref, pre_ref, postmix_ref, router_ref, insem,
    key_s, ins_s, qd_s, kg_s, wk_s, intra_s, buf1, buf2, row_s, hd_s, hrecv, wproj, p_s,
    dsend, drecv, hmid_s, out_rt, x_rt, conv_s, x_s, part_s, swv, exv, cov, gsend, grecv, ret_rt, fin_rt,
    clus_s, place_s, unplace_s, nz_s, qz_s,
    plane_sem, cls, clr, zos, zor, zis, xir,
    wsem, wssem, wrsem, s1s, s1r, s2s, s2r, hs, hr, dss, drs, ags, agr, gss,
):
    s = lax.axis_index("sp")
    t = lax.axis_index("tp")
    y, x = s // NX, lax.rem(s, NX)
    z, c = t // 2, lax.rem(t, 2)
    way = 1 - 2 * c
    ahead = lax.rem(z + way + NZ, NZ) * 2 + c
    behind = lax.rem(z - way + NZ, NZ) * 2 + c
    sibling = z * 2 + 1 - c

    def remote(src, dst, ssem, rsem, sp, tp):
        return pltpu.make_async_remote_copy(
            src_ref=src, dst_ref=dst, send_sem=ssem, recv_sem=rsem,
            device_id=(sp, tp), device_id_type=MESH,
        )

    barrier = pltpu.get_barrier_semaphore()
    row = [(y * NX + lax.rem(x + d, NX), t) for d in range(1, NX)]
    column = [(lax.rem(y + d, NY) * NX + x, t) for d in range(1, NY)]
    near = [*row, *column, (s, ahead), (s, behind), (s, sibling)]
    for peer in near:
        pl.semaphore_signal(barrier, inc=1, device_id=peer, device_id_type=MESH)

    inputs = [
        pltpu.make_async_copy(a, b, insem.at[k])
        for k, (a, b) in enumerate(
            [
                (fa_hbm, fa_ref), (fb_hbm, fb_ref), (ga_hbm, ga_ref), (gb_hbm, gb_ref),
                (bias_hbm, bias_ref), (cluster_hbm, cluster_ref), (qa_hbm, qa_ref),
                (qb_hbm, qb_ref), (v_hbm, v_ref), (gate_hbm, gate_ref), (lane_hbm, lane_ref),
                (skip_hbm, skip_ref), (post_hbm, post_ref), (pre_hbm, pre_ref),
                (postmix_hbm, postmix_ref), (router_hbm, router_ref),
            ]
        )
    ]
    for copy in inputs:
        copy.start()
    own_weights = [
        pltpu.make_async_copy(alpha_ref, wproj.at[0, pl.ds(0, 64)], wsem.at[0]),
        pltpu.make_async_copy(beta_ref, wproj.at[0, pl.ds(64, 64)], wsem.at[1]),
        pltpu.make_async_copy(sw_ref.at[0], swv.at[0], wsem.at[2]),
        pltpu.make_async_copy(ex_ref.at[0], exv.at[0], wsem.at[3]),
        pltpu.make_async_copy(co_ref.at[0], cov.at[0], wsem.at[4]),
    ]
    for copy in own_weights:
        copy.start()

    for copy in inputs[:6]:
        copy.wait()
    gap = jnp.concatenate([ga_ref[...], gb_ref[...]], axis=1)
    lower = jnp.where(iota((128, 128), 0) >= iota((128, 128), 1), 1.0, 0.0).astype(BF16)

    def decays(r, carry):
        rows = slice(r * 128, r * 128 + 128)
        forget = jnp.concatenate([fa_ref[rows, :].astype(F32), fb_ref[rows, :].astype(F32)], axis=1)
        key = gap * sigmoid(-forget)
        left = jnp.broadcast_to(bias_ref[0:1, rows], (128, 128)).T
        right = jnp.broadcast_to(bias_ref[1:2, rows], (128, 128)).T
        logf = jnp.log1p(-key) + jnp.concatenate([left, right, right], axis=1)
        high, mid, _ = split3(logf)
        inside = dot(lower, high) + dot(lower, mid) + carry
        key_s[rows, :] = key
        ins_s[rows, :] = inside
        return inside[127:128, :]

    last = jnp.zeros((1, KT), F32)
    for r in range(TOK // 128):
        last = decays(r, last)

    def weighted(r):
        rows = slice(r * 128, r * 128 + 128)
        wk_s[rows, :] = (key_s[rows, :] * jnp.exp(last - ins_s[rows, :])).astype(BF16)

    def scaled(r):
        rows = slice(r * 128, r * 128 + 128)
        ask = jnp.concatenate([qa_ref[rows, :].astype(F32), qb_ref[rows, :].astype(F32)], axis=1)
        inside = ins_s[rows, :]
        qd_s[rows, :] = (ask * sigmoid(ask) * jnp.exp(inside)).astype(BF16)
        kg_s[rows, :] = (key_s[rows, :] * jnp.exp(-inside)).astype(BF16)

    for r in range(TOK // 128):
        weighted(r)
    inputs[8].wait()
    summed = dot_tn(v_ref[...], wk_s[...])
    state = jnp.concatenate([summed[0:64, 0:128], summed[64:128, 128:KT]], axis=1)

    def packed(buf, place, state, total):
        rows3 = iota((8, KT), 0)
        high, mid, low = (part.astype(F32) for part in split3(total))
        lines = jnp.where(rows3 == 0, high, jnp.where(rows3 == 1, mid, jnp.where(rows3 == 2, low, 0.0)))
        buf[place, 0:64, :] = state.astype(BF16)
        buf[place, 64:72, :] = lines.astype(BF16)

    def unpacked(buf, place):
        lines = buf[place, 64:72, :].astype(F32)
        return buf[place, 0:64, :].astype(F32), lines[0:1] + lines[1:2] + lines[2:3]

    packed(buf1, x, state, last)
    clus_s[0] = jnp.zeros((8, 128), F32)
    clus_s[0, :, 0:ROWS] = jnp.broadcast_to(cluster_ref[...].astype(F32), (8, ROWS))
    pl.semaphore_wait(barrier, len(near))
    for peer in row:
        pl.semaphore_signal(plane_sem, inc=1, device_id=peer, device_id_type=MESH)

    def along_x(d):
        return remote(buf1.at[x], buf1.at[x], s1s, s1r.at[x], y * NX + lax.rem(x + d, NX), t)

    def from_x(d):
        there = lax.rem(x + d, NX)
        return remote(buf1.at[there], buf1.at[there], s1s, s1r.at[there], y * NX + there, t)

    for d in (2, 1, 3):
        along_x(d).start()

    shared = [
        (alpha_ref, wproj.at[1, pl.ds(0, 64)]), (beta_ref, wproj.at[1, pl.ds(64, 64)]),
        (sw_ref.at[0], swv.at[1]), (ex_ref.at[0], exv.at[1]), (co_ref.at[0], cov.at[1]),
    ]
    shared = [remote(a, b, wssem.at[k], wrsem.at[k], s, sibling) for k, (a, b) in enumerate(shared)]
    for copy in shared[:4]:
        copy.start()

    left_half = iota((256, 128), 1) < 64

    def intra(columns, first):
        for block in range(2):
            rows, width = slice(block * 256, block * 256 + 256), 256 * (block + 1)
            scores = dot_nt(qd_s[rows, columns], kg_s[0:width, columns])
            causal = iota((256, width), 0) + 256 * block >= iota((256, width), 1)
            scores = jnp.where(causal, scores, 0.0).astype(BF16)
            found = dot(scores, v_ref[0:width, :])
            intra_s[rows, :] = found if first else jnp.where(left_half, intra_s[rows, :], found)

    for copy in inputs[6:8] + inputs[9:]:
        copy.wait()
    for r in range(TOK // 128):
        scaled(r)
    intra(slice(0, 128), True)

    for d in range(1, NX):
        from_x(d).wait_recv()
    sofar, gone = jnp.zeros((64, KT), F32), jnp.zeros((1, KT), F32)
    before, before_gone = sofar, gone
    for k in range(NX):
        before = jnp.where(x == k, sofar, before)
        before_gone = jnp.where(x == k, gone, before_gone)
        piece, total = unpacked(buf1, k)
        sofar = jnp.exp(total) * sofar + piece
        gone = gone + total
    packed(buf2, y, sofar, gone)
    row_s[...] = jnp.zeros_like(row_s)

    def along_y(d):
        return remote(buf2.at[y], buf2.at[y], s2s.at[d], s2r.at[y], (y + d) * NX + x, t)

    def from_y(k):
        return remote(buf2.at[k], buf2.at[k], s2s.at[0], s2r.at[k], k * NX + x, t)

    for d in (2, 3, 1):
        @pl.when(y + d < NY)
        def _():
            along_y(d).start()

    intra(slice(128, KT), False)

    for k in range(NY - 1):
        @pl.when(k < y)
        def _():
            from_y(k).wait_recv()
            piece, total = unpacked(buf2, k)
            row_s[...] = jnp.exp(total) * row_s[...] + piece

    carried = jnp.exp(before_gone) * row_s[...] + before
    is_left = iota((64, KT), 1) < 128
    carried = jnp.concatenate(
        [jnp.where(is_left, carried, 0.0), jnp.where(is_left, 0.0, carried)], axis=0
    ).astype(BF16)
    lane_gain = jnp.concatenate([lane_ref[...], lane_ref[...]], axis=1)
    left = iota((128, 128), 1) < 64
    for r in range(TOK // 128):
        rows = slice(r * 128, r * 128 + 128)
        raw = intra_s[rows, :] + dot_nt(qd_s[rows, :], carried)
        squares = raw * raw
        mean_a = jnp.sum(jnp.where(left, squares, 0.0), axis=1, keepdims=True) * (1.0 / 64)
        mean_b = jnp.sum(jnp.where(left, 0.0, squares), axis=1, keepdims=True) * (1.0 / 64)
        mean = jnp.where(left, mean_a, mean_b)
        head = raw * lax.rsqrt(mean + EPSILON) * lane_gain * sigmoid(gate_ref[rows, :].astype(F32))
        head = head.astype(BF16)
        for q in range(4):
            at = (2 * r + q // 2) * 32
            hd_s[q % 2, at : at + 32, :] = head[q * 32 : q * 32 + 32, :]

    swap = remote(hd_s.at[1 - c], hrecv, hs, hr, s, sibling)
    swap.start()
    for copy in own_weights[:2]:
        copy.wait()
    p_s[...] = dot(hd_s[c], wproj[0])
    for copy in shared[:2]:
        copy.wait_recv()
    swap.wait_recv()
    p_s[...] = p_s[...] + dot(hrecv[...], wproj[1])

    def piece_d(j):
        return j // 2 * PIECE, slice(j % 2 * (D // 2), (j % 2 + 1) * (D // 2))

    def ring_d(k, j):
        first, columns = piece_d(j)
        part = (k, pl.ds(first, PIECE), pl.ds(columns.start, D // 2))
        return remote(
            dsend.at[part], drecv.at[part], dss, drs.at[k, j], s,
            ahead if k < FAR else behind,
        )

    def send_d(k, j, starts):
        place = FAR - k if k < FAR else -(NEAR - (k - FAR))
        target = lax.rem(z + way * place + NZ, NZ)
        first, columns = piece_d(j)
        rows = pl.ds(pl.multiple_of(target * ROWS + first, PIECE), PIECE)
        value = p_s[rows, columns]
        if not starts:
            ring_d(k - 1, j).wait_recv()
            value = value + drecv[k - 1, first : first + PIECE, columns].astype(F32)
        dsend[k, first : first + PIECE, columns] = value.astype(BF16)
        ring_d(k, j).start()

    def gather(buf, part, ssem, rsem):
        def copy(k, j):
            source = (NZ - k) % NZ if k < FAR else k - FAR
            target = (source + NZ - 1) % NZ if k < FAR else source + 1
            return remote(
                buf.at[(source, *part(j))], buf.at[(target, *part(j))], ssem, rsem.at[k, j], s,
                ahead if k < FAR else behind,
            )

        return copy

    def gather_step(ring, k, chunks, meanwhile=()):
        for j in range(chunks):
            ring(k, j).wait_recv()
            if k + 1 < FAR:
                ring(k + 1, j).start()
            if k < NEAR:
                ring(FAR + k, j).wait_recv()
                if k + 1 < NEAR:
                    ring(FAR + k + 1, j).start()
            if j < len(meanwhile):
                meanwhile[j]()

    def slots_of(r):
        group_row = jnp.broadcast_to(clus_s[r, 0:1, 0:ROWS], (ROWS, ROWS))
        diagonal = iota((ROWS, ROWS), 0) == iota((ROWS, ROWS), 1)
        group_column = jnp.sum(jnp.where(diagonal, group_row, 0.0), axis=1, keepdims=True)
        same = jnp.where(group_row == group_column, 1.0, 0.0)
        earlier_row = iota((ROWS, ROWS), 0) < iota((ROWS, ROWS), 1)
        rank_row = jnp.sum(jnp.where(earlier_row, same, 0.0), axis=0, keepdims=True)
        earlier_column = iota((ROWS, ROWS), 1) < iota((ROWS, ROWS), 0)
        rank_column = jnp.sum(jnp.where(earlier_column, same, 0.0), axis=1, keepdims=True)
        slot_row = group_row[0:1, :] * CAP + rank_row
        slot_column = group_column * CAP + rank_column
        place_s[r] = jnp.where(
            iota((SLOTS, ROWS), 0).astype(F32) == slot_row, 1.0, 0.0
        ).astype(BF16)
        unplace_s[r] = jnp.where(
            iota((ROWS, SLOTS), 1).astype(F32) == slot_column, 1.0, 0.0
        ).astype(BF16)

    groups = gather(clus_s, lambda j: (), cls, clr)
    groups(0, 0).start()
    groups(FAR, 0).start()
    for step in range(FAR):
        if step:
            gather_step(groups, step - 1, 1)
        for j in range(DCH):
            send_d(step, j, step == 0)
            if step < NEAR:
                send_d(FAR + step, j, step == 0)
        if step == 0:
            shared[4].start()
            slots_of(0)
        else:
            slots_of(NZ - step)
            slots_of(step)
    gather_step(groups, FAR - 1, 1)
    slots_of(FAR)
    mixed = p_s[pl.ds(pl.multiple_of(z * ROWS, ROWS), ROWS), :]
    for k in (FAR + NEAR - 1, FAR - 1):
        for j in range(DCH):
            ring_d(k, j).wait_recv()
        mixed = mixed + drecv[k].astype(F32)

    h_mid = (skip_ref[...].astype(F32) + rms(mixed, post_ref[...])).astype(BF16).astype(F32)
    hmid_s[...] = h_mid
    nz_s[0] = rms(h_mid, pre_ref[...]).astype(BF16)

    lines3 = conv_s.reshape(SLOTS, PITCH, 128)
    own = pl.ds(s * CAP, CAP)

    def slots_for(k):
        return pl.ds(k * CAP, CAP)

    def to_lines(value):
        for i in range(LINES):
            conv_s[pl.ds(i, SLOTS, stride=PITCH), :] = value[:, i * 128 : i * 128 + 128]
        return lines3[:, 0:LINES, :].astype(BF16)

    def from_lines(value, at):
        lines3[:, 0:LINES, :] = value.astype(F32)
        for i in range(LINES):
            x_s[at : at + SLOTS, i * 128 : i * 128 + 128] = conv_s[
                pl.ds(i, SLOTS, stride=PITCH), :
            ].astype(BF16)

    def at_offset(dy, dx):
        return lax.rem(y + dy, NY) * NX + lax.rem(x + dx, NX)

    def far_first(action):
        middle = 2 * NX + 2

        def body(i, carry):
            i = i + jnp.where(i >= middle, 1, 0)
            action(at_offset(lax.rem(2 + i // NX, NY), lax.rem(2 + lax.rem(i, NX), NX)))
            return carry

        lax.fori_loop(0, NS - 1, body, 0)

    def all_but_own(src, dst, r, ssem, rsem):
        most = pl.ds(0, SLOTS - CAP)
        return remote(src.at[r, most], dst.at[r, most], ssem, rsem, lax.rem(s + 1, NS), t)

    def scatter(src, dst, r, ssem, rsem):
        far_first(
            lambda there: remote(
                src.at[r, slots_for(there)], dst.at[r, own], ssem, rsem, there, t
            ).start()
        )
        dst[r, own] = src[r, own]

    def near_slots(p):
        return pl.ds(p * CAP, CAP)

    def scatter_in(src, dst):
        for dy, dx in reversed(OFFSETS[1:]):
            there = at_offset(dy, dx)
            p = OFFSETS.index(((-dy) % NY, (-dx) % NX))
            remote(
                src.at[0, slots_for(there)], dst.at[0, near_slots(p)], zos, xir.at[p // (NS // ACH)],
                there, t,
            ).start()
        dst[0, 0:CAP] = src[0, own]

    def scattered_in(src, dst, q):
        first = 1 if q == 0 else q * (NS // ACH)
        part = pl.ds(first * CAP, ((q + 1) * (NS // ACH) - first) * CAP)
        return remote(src.at[0, part], dst.at[0, part], zos, xir.at[q], lax.rem(s + 1, NS), t)

    def scatter_back(src, dst, r, ssem, rsem):
        for p in range(NS - 1, 0, -1):
            there = at_offset(*OFFSETS[p])
            remote(src.at[r, near_slots(p)], dst.at[r, own], ssem, rsem, there, t).start()
        dst[r, own] = src[r, 0:CAP]

    def returned(r, rsem):
        all_but_own(fin_rt, ret_rt, r, zis, rsem).wait_recv()
        at = PLACE[r] * SLOTS
        from_lines(ret_rt[r], at)
        return dot(unplace_s[r], x_s[at : at + SLOTS, :])

    for copy in own_weights[2:]:
        copy.wait()
    router = router_ref[...].astype(F32)
    router_rows = iota((16, D), 0)
    router = jnp.where(
        router_rows == 0, router[0:1], jnp.where(router_rows == 1, router[1:2], 0.0)
    ).astype(BF16)
    member = z // (NZ // 2)

    def part_of(r):
        return part_s[PLACE[r] * SLOTS : PLACE[r] * SLOTS + SLOTS, :]

    def hidden_of(places):
        for place in places:
            from_lines(x_rt[place], PLACE[place] * SLOTS)
        at = PLACE[places[0]] * SLOTS
        rows = x_s[at : at + SLOTS * len(places), :]
        scores = sigmoid(dot_nt(rows, router))
        first, second = scores[:, 0:1], scores[:, 1:2]
        weight = jnp.where(member == 0, first, second) / (first + second)
        hidden = []
        for u in range(2):
            gate = dot(rows, swv[u])
            hidden.append((gate * sigmoid(gate) * dot(rows, exv[u])).astype(BF16))
        return places, weight, hidden

    def contract(found):
        places, weight, hidden = found
        at = PLACE[places[0]] * SLOTS
        total = dot(hidden[0], cov[0]) + dot(hidden[1], cov[1])
        part_s[at : at + SLOTS * len(places), :] = total * weight

    def compute(places):
        contract(hidden_of(places))

    def part_z(j):
        first, columns = piece_d(j)
        return pl.ds(first, PIECE), pl.ds(columns.start, D // 2)

    def part_g(j):
        return pl.ds(j * PIECE, PIECE), pl.ds(0, D)

    def reduce(values, part):
        def copy(k, j):
            return remote(
                gsend.at[(k, *part(j))], grecv.at[(k, *part(j))], gss, drs.at[k, j], s,
                ahead if k < FAR else behind,
            )

        def send(k, j, first):
            place = FAR - k if k < FAR else NZ - (NEAR - (k - FAR))
            rows, columns = (slice(d.start, d.start + d.size) for d in part(j))
            value = values(place, rows, columns)
            if not first:
                copy(k - 1, j).wait_recv()
                value = value + grecv[k - 1, rows, columns].astype(F32)
            gsend[k, rows, columns] = value.astype(BF16)
            copy(k, j).start()

        return copy, send

    def reduce_rest(copy, send, chunks, start):
        for step in range(1, FAR):
            for j in range(chunks):
                if step < NEAR:
                    send(FAR + step, j, False)
                send(step, j, False)
        total = start()
        size = total.shape[0]
        for k in (FAR + NEAR - 1, FAR - 1):
            for j in range(chunks):
                copy(k, j).wait_recv()
            total = total + grecv[k, 0:size, :].astype(F32)
        return total

    sides = [(NZ - 1 - k, k + 1) if k < NEAR else (NZ - 1 - k,) for k in range(FAR)]

    pl.semaphore_wait(plane_sem, NX - 1)

    @pl.when(c == 0)
    def _():
        ring = gather(x_rt, lambda j: (pl.ds(j * (SLOTS // ACH), SLOTS // ACH),), ags, agr)
        out_rt[0] = to_lines(dot(place_s[0], nz_s[0]))
        scatter_in(out_rt, x_rt)
        for copy in shared[2:]:
            copy.wait_recv()
        for j in range(ACH):
            scattered_in(out_rt, x_rt, j).wait_recv()
            ring(0, j).start()
            ring(FAR, j).start()

        def back(places):
            for r in places:
                fin_rt[r] = to_lines(part_of(r))
                scatter_back(fin_rt, ret_rt, r, zis, zor.at[r])

        compute((0,))
        back((0,))
        gather_step(ring, 0, ACH)
        for k in range(1, FAR):
            found = []
            gather_step(
                ring, k, ACH,
                (
                    lambda: found.append(hidden_of(sides[k - 1])),
                    lambda: contract(found[0]),
                    lambda: back(sides[k - 1]),
                ),
            )
        compute(sides[FAR - 1])
        back(sides[FAR - 1])
        copy, send = reduce(lambda place, rows, columns: qz_s[place, rows, columns], part_z)
        for r in (0, 7, 1, 6, 2, 5):
            qz_s[r] = returned(r, zor.at[r])
        for j in range(ZCH):
            send(FAR, j, True)
        for r in (3, 4):
            qz_s[r] = returned(r, zor.at[r])
        for j in range(ZCH):
            send(0, j, True)
        routed = reduce_rest(copy, send, ZCH, lambda: qz_s[0])
        out_ref[...] = (hmid_s[...] + rms(routed, postmix_ref[...])).astype(BF16)
        all_but_own(out_rt, x_rt, 0, zos, xir.at[0]).wait_send()
        most = pl.ds(0, SLOTS - CAP)
        remote(
            fin_rt.at[:, most], ret_rt.at[:, most], zis, zor.at[0], lax.rem(s + 1, NS), t
        ).wait_send()
        around = pl.ds(0, FAR + NEAR)
        remote(x_rt.at[around], x_rt.at[around], ags, agr.at[0, 0], s, ahead).wait_send()
        rows = pl.ds(0, ROWS)
        remote(gsend.at[:, rows], grecv.at[:, rows], gss, drs.at[0, 0], s, ahead).wait_send()

    @pl.when(c == 1)
    def _():
        ring = gather(nz_s, part_z, ags, agr)
        for j in range(ZCH):
            ring(0, j).start()
            ring(FAR, j).start()

        def dispatch(r):
            out_rt[r] = to_lines(dot(place_s[r], nz_s[r]))
            scatter(out_rt, x_rt, r, zos, zor.at[r])

        def work(places):
            for r in places:
                all_but_own(out_rt, x_rt, r, zos, zor.at[r]).wait_recv()
            compute(places)

        dispatch(0)
        for copy in shared[2:]:
            copy.wait_recv()
        for k in range(FAR):
            gather_step(ring, k, ZCH)
            for r in sides[k]:
                dispatch(r)
            if k == 1:
                work((0,))
        copy, send = reduce(
            lambda place, rows, columns: part_s[
                PLACE[place] * SLOTS + rows.start : PLACE[place] * SLOTS + rows.stop, columns
            ],
            part_g,
        )
        work(sides[0] + sides[1])
        work(sides[2])
        for j in range(GCH):
            send(FAR, j, True)
        work(sides[3])
        for j in range(GCH):
            send(0, j, True)
        final = reduce_rest(copy, send, GCH, lambda: part_of(0))
        fin_rt[0] = to_lines(final)
        scatter(fin_rt, ret_rt, 0, zis, xir.at[0])
        routed = returned(0, xir.at[0])
        out_ref[...] = (hmid_s[...] + rms(routed, postmix_ref[...])).astype(BF16)
        most = pl.ds(0, SLOTS - CAP)
        remote(
            out_rt.at[:, most], x_rt.at[:, most], zos, zor.at[0], lax.rem(s + 1, NS), t
        ).wait_send()
        all_but_own(fin_rt, ret_rt, 0, zis, xir.at[0]).wait_send()
        around = pl.ds(0, FAR + NEAR)
        remote(nz_s.at[around], nz_s.at[around], ags, agr.at[0, 0], s, ahead).wait_send()
        remote(gsend, grecv, gss, drs.at[0, 0], s, ahead).wait_send()

    remote(
        buf1.at[pl.ds(0, NX - 1)], buf1.at[pl.ds(0, NX - 1)], s1s, s1r.at[0], s, sibling
    ).wait_send()
    for d in range(1, NY):
        @pl.when(y + d < NY)
        def _():
            along_y(d).wait_send()
    around = pl.ds(0, FAR + NEAR)
    remote(clus_s.at[around], clus_s.at[around], cls, clr.at[0, 0], s, ahead).wait_send()
    for copy in shared:
        copy.wait_send()
    swap.wait_send()
    remote(dsend, drecv, dss, drs.at[0, 0], s, ahead).wait_send()


def shards(
    ask_left, keep_left, gap_left, ask_right, keep_right, gap_right, payload, switch_logits,
    keep_bias, lanewise, alpha, beta, skip, post, pre, postmix, router, switch, expansion,
    contraction, cluster,
):
    inputs = (
        keep_left, keep_right, gap_left.reshape(1, -1), gap_right.reshape(1, -1), keep_bias.T,
        cluster.reshape(1, -1), ask_left, ask_right, payload, switch_logits,
        lanewise.reshape(1, -1), skip, post.reshape(1, -1), pre.reshape(1, -1),
        postmix.reshape(1, -1), router.T,
    )
    vmem = pl.BlockSpec(memory_space=pltpu.VMEM)
    hbm = pl.BlockSpec(memory_space=pl.ANY)
    ring = FAR + NEAR
    dma = pltpu.SemaphoreType.DMA
    return pl.pallas_call(
        kernel,
        out_shape=pltpu.VMEM((ROWS, D), BF16),
        in_specs=[hbm] * 21,
        out_specs=vmem,
        scratch_shapes=[
            *(pltpu.VMEM(a.shape, a.dtype) for a in inputs),
            dma((16,)),
            pltpu.VMEM((TOK, KT), F32),
            pltpu.VMEM((TOK, KT), F32),
            pltpu.VMEM((TOK, KT), BF16),
            pltpu.VMEM((TOK, KT), BF16),
            pltpu.VMEM((TOK, KT), BF16),
            pltpu.VMEM((TOK, 128), F32),
            pltpu.VMEM((NX, 72, KT), BF16),
            pltpu.VMEM((NY, 72, KT), BF16),
            pltpu.VMEM((64, KT), F32),
            pltpu.VMEM((2, TOK // 2, 128), BF16),
            pltpu.VMEM((TOK // 2, 128), BF16),
            pltpu.VMEM((2, 128, D), BF16),
            pltpu.VMEM((TOK // 2, D), F32),
            pltpu.VMEM((ring, ROWS, D), BF16),
            pltpu.VMEM((ring, ROWS, D), BF16),
            pltpu.VMEM((ROWS, D), F32),
            pltpu.VMEM((NZ, SLOTS, LINES, 128), BF16),
            pltpu.VMEM((NZ, SLOTS, LINES, 128), BF16),
            pltpu.VMEM((SLOTS * PITCH, 128), F32),
            pltpu.VMEM((NZ * SLOTS, D), BF16),
            pltpu.VMEM((NZ * SLOTS, D), F32),
            pltpu.VMEM((2, D, HID), BF16),
            pltpu.VMEM((2, D, HID), BF16),
            pltpu.VMEM((2, HID, D), BF16),
            pltpu.VMEM((ring, SLOTS, D), BF16),
            pltpu.VMEM((ring, SLOTS, D), BF16),
            pltpu.VMEM((NZ, SLOTS, LINES, 128), BF16),
            pltpu.VMEM((NZ, SLOTS, LINES, 128), BF16),
            pltpu.VMEM((NZ, 8, 128), F32),
            pltpu.VMEM((NZ, SLOTS, ROWS), BF16),
            pltpu.VMEM((NZ, ROWS, SLOTS), BF16),
            pltpu.VMEM((NZ, ROWS, D), BF16),
            pltpu.VMEM((NZ, ROWS, D), F32),
            pltpu.SemaphoreType.REGULAR, dma, dma((ring, 1)),
            dma, dma((NZ,)), dma, dma((ACH,)),
            dma((5,)), dma((5,)), dma((5,)),
            dma, dma((NX,)), dma((NY,)), dma((NY,)),
            dma, dma,
            dma, dma((ring, DCH)),
            dma, dma((ring, max(ACH, ZCH))),
            dma,
        ],
        compiler_params=pltpu.CompilerParams(
            collective_id=0, has_side_effects=True, vmem_limit_bytes=56 * 1024 * 1024
        ),
    )(
        *inputs, alpha, beta, switch, expansion, contraction,
    )


def solution(mesh):
    placed = (
        P("sp", "tp"),
        P("sp", "tp"),
        P("tp"),
        P("sp", "tp"),
        P("sp", "tp"),
        P("tp"),
        P("sp", "tp"),
        P("sp", "tp"),
        P("sp", "tp"),
        P(),
        P("tp", None),
        P("tp", None),
        P(("sp", "tp"), None),
        P(),
        P(),
        P(),
        P(None, "sp"),
        P("sp", None, "tp"),
        P("sp", None, "tp"),
        P("sp", "tp", None),
        P(("sp", "tp")),
    )
    return jax.shard_map(
        shards, mesh=mesh, in_specs=placed, out_specs=P(("sp", "tp"), None), check_vma=False
    )
```

```python
import functools

import jax
import jax.numpy as jnp
from jax import lax
from jax.experimental import pallas as pl
from jax.experimental.pallas import tpu as pltpu
from jax.sharding import PartitionSpec as P

EPSILON = 1e-06
NX, NY, NZ = 4, 4, 8
NS = NX * NY
D = 2048
KT = 384
TOK = 512
ROWS = 32
CAP = 3
SLOTS = NS * CAP
LINES = D // 128
HID = 256
FAR, NEAR = NZ // 2, NZ // 2 - 1
PLACE = {0: 0, 7: 1, 1: 2, 6: 3, 2: 4, 5: 5, 3: 6, 4: 7}
PITCH = 24
OFFSETS = sorted(
    ((dy, dx) for dy in range(NY) for dx in range(NX)),
    key=lambda o: min(o[0], NY - o[0]) + min(o[1], NX - o[1]),
)
PIECE = 8
DCH, GCH, ZCH, ACH = 8, 6, 8, 8
MESH = pl.DeviceIdType.MESH
F32, BF16 = jnp.float32, jnp.bfloat16


def dot(a, b):
    return jnp.dot(a, b, preferred_element_type=F32)


def dot_nt(a, b):
    return lax.dot_general(a, b, (((1,), (1,)), ((), ())), preferred_element_type=F32)


def dot_tn(a, b):
    return lax.dot_general(a, b, (((0,), (0,)), ((), ())), preferred_element_type=F32)


def sigmoid(v):
    return 1.0 / (1.0 + jnp.exp(-v))


def rms(v, gain):
    return v * lax.rsqrt(jnp.mean(v * v, axis=-1, keepdims=True) + EPSILON) * gain


def split3(v):
    high = v.astype(BF16)
    rest = v - high.astype(F32)
    mid = rest.astype(BF16)
    low = (rest - mid.astype(F32)).astype(BF16)
    return high, mid, low


def iota(shape, dim):
    return lax.broadcasted_iota(jnp.int32, shape, dim)


def kernel(
    fa_hbm, fb_hbm, ga_hbm, gb_hbm, bias_hbm, cluster_hbm, qa_hbm, qb_hbm, v_hbm,
    gate_hbm, lane_hbm, skip_hbm, post_hbm, pre_hbm, postmix_hbm, router_hbm,
    alpha_ref, beta_ref, sw_ref, ex_ref, co_ref,
    out_ref,
    fa_ref, fb_ref, ga_ref, gb_ref, bias_ref, cluster_ref, qa_ref, qb_ref, v_ref,
    gate_ref, lane_ref, skip_ref, post_ref, pre_ref, postmix_ref, router_ref, insem,
    key_s, ins_s, qd_s, kg_s, wk_s, intra_s, buf1, buf2, row_s, hd_s, hrecv, wproj, p_s,
    dsend, drecv, hmid_s, out_rt, x_rt, conv_s, x_s, part_s, swv, exv, cov, gsend, grecv, ret_rt, fin_rt,
    clus_s, place_s, unplace_s, nz_s, qz_s,
    rets_rt, sends_s, recvs_s, unp_s, routs_s, routr_s, oss, rrs, us, ur, qs, qr, pair_sem,
    plane_sem, cls, clr, zos, zor, zis, xir,
    wsem, wssem, wrsem, s1s, s1r, s2s, s2r, hs, hr, dss, drs, ags, agr, gss,
):
    s = lax.axis_index("sp")
    t = lax.axis_index("tp")
    y, x = s // NX, lax.rem(s, NX)
    z, c = t // 2, lax.rem(t, 2)
    way = 1 - 2 * c
    ahead = lax.rem(z + way + NZ, NZ) * 2 + c
    behind = lax.rem(z - way + NZ, NZ) * 2 + c
    sibling = z * 2 + 1 - c

    def remote(src, dst, ssem, rsem, sp, tp):
        return pltpu.make_async_remote_copy(
            src_ref=src, dst_ref=dst, send_sem=ssem, recv_sem=rsem,
            device_id=(sp, tp), device_id_type=MESH,
        )

    barrier = pltpu.get_barrier_semaphore()
    row = [(y * NX + lax.rem(x + d, NX), t) for d in range(1, NX)]
    column = [(lax.rem(y + d, NY) * NX + x, t) for d in range(1, NY)]
    near = [*row, *column, (s, ahead), (s, behind), (s, sibling)]
    for peer in near:
        pl.semaphore_signal(barrier, inc=1, device_id=peer, device_id_type=MESH)

    inputs = [
        pltpu.make_async_copy(a, b, insem.at[k])
        for k, (a, b) in enumerate(
            [
                (fa_hbm, fa_ref), (fb_hbm, fb_ref), (ga_hbm, ga_ref), (gb_hbm, gb_ref),
                (bias_hbm, bias_ref), (cluster_hbm, cluster_ref), (qa_hbm, qa_ref),
                (qb_hbm, qb_ref), (v_hbm, v_ref), (gate_hbm, gate_ref), (lane_hbm, lane_ref),
                (skip_hbm, skip_ref), (post_hbm, post_ref), (pre_hbm, pre_ref),
                (postmix_hbm, postmix_ref), (router_hbm, router_ref),
            ]
        )
    ]
    for copy in inputs:
        copy.start()
    own_weights = [
        pltpu.make_async_copy(alpha_ref, wproj.at[0, pl.ds(0, 64)], wsem.at[0]),
        pltpu.make_async_copy(beta_ref, wproj.at[0, pl.ds(64, 64)], wsem.at[1]),
        pltpu.make_async_copy(sw_ref.at[0], swv.at[0], wsem.at[2]),
        pltpu.make_async_copy(ex_ref.at[0], exv.at[0], wsem.at[3]),
        pltpu.make_async_copy(co_ref.at[0], cov.at[0], wsem.at[4]),
    ]
    for copy in own_weights:
        copy.start()

    for copy in inputs[:6]:
        copy.wait()
    gap = jnp.concatenate([ga_ref[...], gb_ref[...]], axis=1)
    lower = jnp.where(iota((128, 128), 0) >= iota((128, 128), 1), 1.0, 0.0).astype(BF16)

    def decays(r, carry):
        rows = slice(r * 128, r * 128 + 128)
        forget = jnp.concatenate([fa_ref[rows, :].astype(F32), fb_ref[rows, :].astype(F32)], axis=1)
        key = gap * sigmoid(-forget)
        left = jnp.broadcast_to(bias_ref[0:1, rows], (128, 128)).T
        right = jnp.broadcast_to(bias_ref[1:2, rows], (128, 128)).T
        logf = jnp.log1p(-key) + jnp.concatenate([left, right, right], axis=1)
        high, mid, _ = split3(logf)
        inside = dot(lower, high) + dot(lower, mid) + carry
        key_s[rows, :] = key
        ins_s[rows, :] = inside
        return inside[127:128, :]

    last = jnp.zeros((1, KT), F32)
    for r in range(TOK // 128):
        last = decays(r, last)

    def weighted(r):
        rows = slice(r * 128, r * 128 + 128)
        wk_s[rows, :] = (key_s[rows, :] * jnp.exp(last - ins_s[rows, :])).astype(BF16)

    def scaled(r):
        rows = slice(r * 128, r * 128 + 128)
        ask = jnp.concatenate([qa_ref[rows, :].astype(F32), qb_ref[rows, :].astype(F32)], axis=1)
        inside = ins_s[rows, :]
        qd_s[rows, :] = (ask * sigmoid(ask) * jnp.exp(inside)).astype(BF16)
        kg_s[rows, :] = (key_s[rows, :] * jnp.exp(-inside)).astype(BF16)

    for r in range(TOK // 128):
        weighted(r)
    inputs[8].wait()
    summed = dot_tn(v_ref[...], wk_s[...])
    state = jnp.concatenate([summed[0:64, 0:128], summed[64:128, 128:KT]], axis=1)

    def packed(buf, place, state, total):
        rows3 = iota((8, KT), 0)
        high, mid, low = (part.astype(F32) for part in split3(total))
        lines = jnp.where(rows3 == 0, high, jnp.where(rows3 == 1, mid, jnp.where(rows3 == 2, low, 0.0)))
        buf[place, 0:64, :] = state.astype(BF16)
        buf[place, 64:72, :] = lines.astype(BF16)

    def unpacked(buf, place):
        lines = buf[place, 64:72, :].astype(F32)
        return buf[place, 0:64, :].astype(F32), lines[0:1] + lines[1:2] + lines[2:3]

    packed(buf1, x, state, last)
    clus_s[0] = jnp.zeros((8, 128), F32)
    clus_s[0, :, 0:ROWS] = jnp.broadcast_to(cluster_ref[...].astype(F32), (8, ROWS))
    pl.semaphore_wait(barrier, len(near))
    for peer in row:
        pl.semaphore_signal(plane_sem, inc=1, device_id=peer, device_id_type=MESH)

    def along_x(d):
        return remote(buf1.at[x], buf1.at[x], s1s, s1r.at[x], y * NX + lax.rem(x + d, NX), t)

    def from_x(d):
        there = lax.rem(x + d, NX)
        return remote(buf1.at[there], buf1.at[there], s1s, s1r.at[there], y * NX + there, t)

    for d in (2, 1, 3):
        along_x(d).start()

    shared = [
        (alpha_ref, wproj.at[1, pl.ds(0, 64)]), (beta_ref, wproj.at[1, pl.ds(64, 64)]),
        (sw_ref.at[0], swv.at[1]), (ex_ref.at[0], exv.at[1]), (co_ref.at[0], cov.at[1]),
    ]
    shared = [remote(a, b, wssem.at[k], wrsem.at[k], s, sibling) for k, (a, b) in enumerate(shared)]
    for copy in shared[:4]:
        copy.start()

    left_half = iota((256, 128), 1) < 64

    def intra(columns, first):
        for block in range(2):
            rows, width = slice(block * 256, block * 256 + 256), 256 * (block + 1)
            scores = dot_nt(qd_s[rows, columns], kg_s[0:width, columns])
            causal = iota((256, width), 0) + 256 * block >= iota((256, width), 1)
            scores = jnp.where(causal, scores, 0.0).astype(BF16)
            found = dot(scores, v_ref[0:width, :])
            intra_s[rows, :] = found if first else jnp.where(left_half, intra_s[rows, :], found)

    for copy in inputs[6:8] + inputs[9:]:
        copy.wait()
    for r in range(TOK // 128):
        scaled(r)
    intra(slice(0, 128), True)

    for d in range(1, NX):
        from_x(d).wait_recv()
    sofar, gone = jnp.zeros((64, KT), F32), jnp.zeros((1, KT), F32)
    before, before_gone = sofar, gone
    for k in range(NX):
        before = jnp.where(x == k, sofar, before)
        before_gone = jnp.where(x == k, gone, before_gone)
        piece, total = unpacked(buf1, k)
        sofar = jnp.exp(total) * sofar + piece
        gone = gone + total
    packed(buf2, y, sofar, gone)
    row_s[...] = jnp.zeros_like(row_s)

    def along_y(d):
        return remote(buf2.at[y], buf2.at[y], s2s.at[d], s2r.at[y], (y + d) * NX + x, t)

    def from_y(k):
        return remote(buf2.at[k], buf2.at[k], s2s.at[0], s2r.at[k], k * NX + x, t)

    for d in (2, 3, 1):
        @pl.when(y + d < NY)
        def _():
            along_y(d).start()

    intra(slice(128, KT), False)

    for k in range(NY - 1):
        @pl.when(k < y)
        def _():
            from_y(k).wait_recv()
            piece, total = unpacked(buf2, k)
            row_s[...] = jnp.exp(total) * row_s[...] + piece

    carried = jnp.exp(before_gone) * row_s[...] + before
    is_left = iota((64, KT), 1) < 128
    carried = jnp.concatenate(
        [jnp.where(is_left, carried, 0.0), jnp.where(is_left, 0.0, carried)], axis=0
    ).astype(BF16)
    lane_gain = jnp.concatenate([lane_ref[...], lane_ref[...]], axis=1)
    left = iota((128, 128), 1) < 64
    for r in range(TOK // 128):
        rows = slice(r * 128, r * 128 + 128)
        raw = intra_s[rows, :] + dot_nt(qd_s[rows, :], carried)
        squares = raw * raw
        mean_a = jnp.sum(jnp.where(left, squares, 0.0), axis=1, keepdims=True) * (1.0 / 64)
        mean_b = jnp.sum(jnp.where(left, 0.0, squares), axis=1, keepdims=True) * (1.0 / 64)
        mean = jnp.where(left, mean_a, mean_b)
        head = raw * lax.rsqrt(mean + EPSILON) * lane_gain * sigmoid(gate_ref[rows, :].astype(F32))
        head = head.astype(BF16)
        for q in range(4):
            at = (2 * r + q // 2) * 32
            hd_s[q % 2, at : at + 32, :] = head[q * 32 : q * 32 + 32, :]

    swap = remote(hd_s.at[1 - c], hrecv, hs, hr, s, sibling)
    swap.start()
    for copy in own_weights[:2]:
        copy.wait()
    p_s[...] = dot(hd_s[c], wproj[0])
    for copy in shared[:2]:
        copy.wait_recv()
    swap.wait_recv()
    p_s[...] = p_s[...] + dot(hrecv[...], wproj[1])

    def piece_d(j):
        return j // 2 * PIECE, slice(j % 2 * (D // 2), (j % 2 + 1) * (D // 2))

    def ring_d(k, j):
        first, columns = piece_d(j)
        part = (k, pl.ds(first, PIECE), pl.ds(columns.start, D // 2))
        return remote(
            dsend.at[part], drecv.at[part], dss, drs.at[k, j], s,
            ahead if k < FAR else behind,
        )

    def send_d(k, j, starts):
        place = FAR - k if k < FAR else -(NEAR - (k - FAR))
        target = lax.rem(z + way * place + NZ, NZ)
        first, columns = piece_d(j)
        rows = pl.ds(pl.multiple_of(target * ROWS + first, PIECE), PIECE)
        value = p_s[rows, columns]
        if not starts:
            ring_d(k - 1, j).wait_recv()
            value = value + drecv[k - 1, first : first + PIECE, columns].astype(F32)
        dsend[k, first : first + PIECE, columns] = value.astype(BF16)
        ring_d(k, j).start()

    def gather(buf, part, ssem, rsem):
        def copy(k, j):
            source = (NZ - k) % NZ if k < FAR else k - FAR
            target = (source + NZ - 1) % NZ if k < FAR else source + 1
            return remote(
                buf.at[(source, *part(j))], buf.at[(target, *part(j))], ssem, rsem.at[k, j], s,
                ahead if k < FAR else behind,
            )

        return copy

    def gather_step(ring, k, chunks, meanwhile=()):
        for j in range(chunks):
            ring(k, j).wait_recv()
            if k + 1 < FAR:
                ring(k + 1, j).start()
            if k < NEAR:
                ring(FAR + k, j).wait_recv()
                if k + 1 < NEAR:
                    ring(FAR + k + 1, j).start()
            if j < len(meanwhile):
                meanwhile[j]()

    def slots_of(r):
        group_row = jnp.broadcast_to(clus_s[r, 0:1, 0:ROWS], (ROWS, ROWS))
        diagonal = iota((ROWS, ROWS), 0) == iota((ROWS, ROWS), 1)
        group_column = jnp.sum(jnp.where(diagonal, group_row, 0.0), axis=1, keepdims=True)
        same = jnp.where(group_row == group_column, 1.0, 0.0)
        earlier_row = iota((ROWS, ROWS), 0) < iota((ROWS, ROWS), 1)
        rank_row = jnp.sum(jnp.where(earlier_row, same, 0.0), axis=0, keepdims=True)
        earlier_column = iota((ROWS, ROWS), 1) < iota((ROWS, ROWS), 0)
        rank_column = jnp.sum(jnp.where(earlier_column, same, 0.0), axis=1, keepdims=True)
        slot_row = group_row[0:1, :] * CAP + rank_row
        slot_column = group_column * CAP + rank_column
        place_s[r] = jnp.where(
            iota((SLOTS, ROWS), 0).astype(F32) == slot_row, 1.0, 0.0
        ).astype(BF16)
        unplace_s[r] = jnp.where(
            iota((ROWS, SLOTS), 1).astype(F32) == slot_column, 1.0, 0.0
        ).astype(BF16)

    groups = gather(clus_s, lambda j: (), cls, clr)
    groups(0, 0).start()
    groups(FAR, 0).start()
    for step in range(FAR):
        if step:
            gather_step(groups, step - 1, 1)
        for j in range(DCH):
            send_d(step, j, step == 0)
            if step < NEAR:
                send_d(FAR + step, j, step == 0)
        if step == 0:
            shared[4].start()
            pl.semaphore_wait(plane_sem, NX - 1)
            pl.semaphore_signal(pair_sem, inc=1, device_id=(s, sibling), device_id_type=MESH)
            slots_of(0)
        else:
            slots_of(NZ - step)
            slots_of(step)
    gather_step(groups, FAR - 1, 1)
    slots_of(FAR)
    mixed = p_s[pl.ds(pl.multiple_of(z * ROWS, ROWS), ROWS), :]
    for k in (FAR + NEAR - 1, FAR - 1):
        for j in range(DCH):
            ring_d(k, j).wait_recv()
        mixed = mixed + drecv[k].astype(F32)

    h_mid = (skip_ref[...].astype(F32) + rms(mixed, post_ref[...])).astype(BF16).astype(F32)
    hmid_s[...] = h_mid
    nz_s[0] = rms(h_mid, pre_ref[...]).astype(BF16)

    lines3 = conv_s.reshape(SLOTS, PITCH, 128)
    own = pl.ds(s * CAP, CAP)

    def slots_for(k):
        return pl.ds(k * CAP, CAP)

    def to_lines(value):
        for i in range(LINES):
            conv_s[pl.ds(i, SLOTS, stride=PITCH), :] = value[:, i * 128 : i * 128 + 128]
        return lines3[:, 0:LINES, :].astype(BF16)

    def from_lines(value, at):
        lines3[:, 0:LINES, :] = value.astype(F32)
        for i in range(LINES):
            x_s[at : at + SLOTS, i * 128 : i * 128 + 128] = conv_s[
                pl.ds(i, SLOTS, stride=PITCH), :
            ].astype(BF16)

    def at_offset(dy, dx):
        return lax.rem(y + dy, NY) * NX + lax.rem(x + dx, NX)

    def all_but_own(src, dst, r, ssem, rsem):
        most = pl.ds(0, SLOTS - CAP)
        return remote(src.at[r, most], dst.at[r, most], ssem, rsem, lax.rem(s + 1, NS), t)

    def scatter(src, dst, r, ssem, rsem):
        for dy, dx in reversed(OFFSETS[1:]):
            there = at_offset(dy, dx)
            remote(src.at[r, slots_for(there)], dst.at[r, own], ssem, rsem, there, t).start()
        dst[r, own] = src[r, own]

    def near_slots(p):
        return pl.ds(p * CAP, CAP)

    def scatter_in(src, dst):
        for dy, dx in reversed(OFFSETS[1:]):
            there = at_offset(dy, dx)
            p = OFFSETS.index(((-dy) % NY, (-dx) % NX))
            remote(
                src.at[0, slots_for(there)], dst.at[0, near_slots(p)], zos, xir.at[p // (NS // ACH)],
                there, t,
            ).start()
        dst[0, 0:CAP] = src[0, own]

    def scattered_in(src, dst, q):
        first = 1 if q == 0 else q * (NS // ACH)
        part = pl.ds(first * CAP, ((q + 1) * (NS // ACH) - first) * CAP)
        return remote(src.at[0, part], dst.at[0, part], zos, xir.at[q], lax.rem(s + 1, NS), t)

    def scatter_back(src, dst, r, ssem, rsem):
        for p in range(NS - 1, -1, -1):
            there = at_offset(*OFFSETS[p])
            remote(src.at[r, near_slots(p)], dst.at[r, own], ssem, rsem, there, sibling).start()

    def given_back(r):
        remote(fin_rt.at[r], rets_rt.at[r], zis, rrs.at[r], s, sibling).wait_recv()
        at = PLACE[r] * SLOTS
        from_lines(rets_rt[r], at)
        qz_s[r] = dot(unp_s[r], x_s[at : at + SLOTS, :])

    def returned(r, rsem):
        all_but_own(fin_rt, ret_rt, r, zis, rsem).wait_recv()
        at = PLACE[r] * SLOTS
        from_lines(ret_rt[r], at)
        return dot(unplace_s[r], x_s[at : at + SLOTS, :])

    for copy in own_weights[2:]:
        copy.wait()
    router = router_ref[...].astype(F32)
    router_rows = iota((16, D), 0)
    router = jnp.where(
        router_rows == 0, router[0:1], jnp.where(router_rows == 1, router[1:2], 0.0)
    ).astype(BF16)
    member = z // (NZ // 2)

    def part_of(r):
        return part_s[PLACE[r] * SLOTS : PLACE[r] * SLOTS + SLOTS, :]

    def hidden_of(places):
        for place in places:
            from_lines(x_rt[place], PLACE[place] * SLOTS)
        at = PLACE[places[0]] * SLOTS
        rows = x_s[at : at + SLOTS * len(places), :]
        scores = sigmoid(dot_nt(rows, router))
        first, second = scores[:, 0:1], scores[:, 1:2]
        weight = jnp.where(member == 0, first, second) / (first + second)
        hidden = []
        for u in range(2):
            gate = dot(rows, swv[u])
            hidden.append((gate * sigmoid(gate) * dot(rows, exv[u])).astype(BF16))
        return places, weight, hidden

    def contract(found):
        places, weight, hidden = found
        at = PLACE[places[0]] * SLOTS
        total = dot(hidden[0], cov[0]) + dot(hidden[1], cov[1])
        part_s[at : at + SLOTS * len(places), :] = total * weight

    def compute(places):
        contract(hidden_of(places))

    def part_z(j):
        first, columns = piece_d(j)
        return pl.ds(first, PIECE), pl.ds(columns.start, D // 2)

    def part_g(j):
        return pl.ds(j * PIECE, PIECE), pl.ds(0, D)

    def reduce(values, part, sent, received, ssem, rsem, to=(ahead, behind)):
        def copy(k, j):
            return remote(
                sent.at[(k, *part(j))], received.at[(k, *part(j))], ssem, rsem.at[k, j], s,
                to[0] if k < FAR else to[1],
            )

        def send(k, j, first):
            place = FAR - k if k < FAR else NZ - (NEAR - (k - FAR))
            rows, columns = (slice(d.start, d.start + d.size) for d in part(j))
            value = values(place, rows, columns)
            if not first:
                copy(k - 1, j).wait_recv()
                value = value + received[k - 1, rows, columns].astype(F32)
            sent[k, rows, columns] = value.astype(BF16)
            copy(k, j).start()

        return copy, send

    def reduce_step(send, chunks, step):
        for j in range(chunks):
            send(step, j, False)
            if step < NEAR:
                send(FAR + step, j, False)

    def reduce_end(copy, received, chunks, total):
        for k in (FAR + NEAR - 1, FAR - 1):
            for j in range(chunks):
                copy(k, j).wait_recv()
            total = total + received[k].astype(F32)
        return total

    sides = [(NZ - 1 - k, k + 1) if k < NEAR else (NZ - 1 - k,) for k in range(FAR)]

    pl.semaphore_wait(pair_sem, 1)

    @pl.when(c == 0)
    def _():
        slots_copy = remote(unplace_s, unp_s, us, ur, s, sibling)
        slots_copy.start()
        ring = gather(x_rt, lambda j: (pl.ds(j * (SLOTS // ACH), SLOTS // ACH),), ags, agr)
        out_rt[0] = to_lines(dot(place_s[0], nz_s[0]))
        scatter_in(out_rt, x_rt)
        for copy in shared[2:]:
            copy.wait_recv()
        for j in range(ACH):
            scattered_in(out_rt, x_rt, j).wait_recv()
            ring(0, j).start()
            ring(FAR, j).start()

        def back(places):
            for r in places:
                fin_rt[r] = to_lines(part_of(r))
                scatter_back(fin_rt, rets_rt, r, zis, rrs.at[r])

        compute((0,))
        back((0,))
        gather_step(ring, 0, ACH)
        for k in range(1, FAR):
            found = []
            gather_step(
                ring, k, ACH,
                (
                    lambda: found.append(hidden_of(sides[k - 1])),
                    lambda: contract(found[0]),
                    lambda: back(sides[k - 1]),
                ),
            )
        compute(sides[FAR - 1])
        back(sides[FAR - 1])
        remote(routs_s, routr_s, qs, qr, s, sibling).wait_recv()
        routed = routr_s[...].astype(F32)
        out_ref[...] = (hmid_s[...] + rms(routed, postmix_ref[...])).astype(BF16)
        all_but_own(out_rt, x_rt, 0, zos, xir.at[0]).wait_send()
        slots_copy.wait_send()
        remote(fin_rt, rets_rt, zis, rrs.at[0], s, sibling).wait_send()
        around = pl.ds(0, FAR + NEAR)
        remote(x_rt.at[around], x_rt.at[around], ags, agr.at[0, 0], s, ahead).wait_send()

    @pl.when(c == 1)
    def _():
        ring = gather(nz_s, part_z, ags, agr)
        for j in range(ZCH):
            ring(0, j).start()
            ring(FAR, j).start()

        def dispatch(r):
            out_rt[r] = to_lines(dot(place_s[r], nz_s[r]))
            scatter(out_rt, x_rt, r, zos, zor.at[r])

        def work(places):
            for r in places:
                all_but_own(out_rt, x_rt, r, zos, zor.at[r]).wait_recv()
            compute(places)

        dispatch(0)
        for copy in shared[2:]:
            copy.wait_recv()
        for k in range(FAR):
            gather_step(ring, k, ZCH)
            for r in sides[k]:
                dispatch(r)
            if k == 1:
                work((0,))
            elif k == 2:
                work(sides[0])
        copy, send = reduce(
            lambda place, rows, columns: part_s[
                PLACE[place] * SLOTS + rows.start : PLACE[place] * SLOTS + rows.stop, columns
            ],
            part_g, gsend, grecv, gss, drs,
        )
        work(sides[1])
        work(sides[2])
        for j in range(GCH):
            send(FAR, j, True)
        work(sides[3])
        for j in range(GCH):
            send(0, j, True)
        copy_s, send_s = reduce(
            lambda place, rows, columns: qz_s[place, rows, columns], part_z, sends_s, recvs_s,
            oss, agr, (behind, ahead),
        )
        remote(unplace_s, unp_s, us, ur, s, sibling).wait_recv()
        for r in (0, 7, 1):
            given_back(r)
        reduce_step(send, GCH, 1)
        for r in (6, 2):
            given_back(r)
        reduce_step(send, GCH, 2)
        given_back(5)
        for j in range(ZCH):
            send_s(FAR, j, True)
        given_back(3)
        reduce_step(send, GCH, 3)
        given_back(4)
        for j in range(ZCH):
            send_s(0, j, True)
        reduce_step(send_s, ZCH, 1)
        final = reduce_end(copy, grecv, GCH, part_of(0))
        fin_rt[0] = to_lines(final)
        scatter(fin_rt, ret_rt, 0, zis, xir.at[0])
        reduce_step(send_s, ZCH, 2)
        reduce_step(send_s, ZCH, 3)
        routed = returned(0, xir.at[0])
        out_ref[...] = (hmid_s[...] + rms(routed, postmix_ref[...])).astype(BF16)
        routs_s[...] = reduce_end(copy_s, recvs_s, ZCH, qz_s[0]).astype(BF16)
        sums_copy = remote(routs_s, routr_s, qs, qr, s, sibling)
        sums_copy.start()
        most = pl.ds(0, SLOTS - CAP)
        remote(
            out_rt.at[:, most], x_rt.at[:, most], zos, zor.at[0], lax.rem(s + 1, NS), t
        ).wait_send()
        all_but_own(fin_rt, ret_rt, 0, zis, xir.at[0]).wait_send()
        around = pl.ds(0, FAR + NEAR)
        remote(nz_s.at[around], nz_s.at[around], ags, agr.at[0, 0], s, ahead).wait_send()
        remote(gsend, grecv, gss, drs.at[0, 0], s, ahead).wait_send()
        remote(sends_s, recvs_s, oss, agr.at[0, 0], s, ahead).wait_send()
        sums_copy.wait_send()

    remote(
        buf1.at[pl.ds(0, NX - 1)], buf1.at[pl.ds(0, NX - 1)], s1s, s1r.at[0], s, sibling
    ).wait_send()
    for d in range(1, NY):
        @pl.when(y + d < NY)
        def _():
            along_y(d).wait_send()
    around = pl.ds(0, FAR + NEAR)
    remote(clus_s.at[around], clus_s.at[around], cls, clr.at[0, 0], s, ahead).wait_send()
    for copy in shared:
        copy.wait_send()
    swap.wait_send()
    remote(dsend, drecv, dss, drs.at[0, 0], s, ahead).wait_send()


def shards(
    ask_left, keep_left, gap_left, ask_right, keep_right, gap_right, payload, switch_logits,
    keep_bias, lanewise, alpha, beta, skip, post, pre, postmix, router, switch, expansion,
    contraction, cluster,
):
    inputs = (
        keep_left, keep_right, gap_left.reshape(1, -1), gap_right.reshape(1, -1), keep_bias.T,
        cluster.reshape(1, -1), ask_left, ask_right, payload, switch_logits,
        lanewise.reshape(1, -1), skip, post.reshape(1, -1), pre.reshape(1, -1),
        postmix.reshape(1, -1), router.T,
    )
    vmem = pl.BlockSpec(memory_space=pltpu.VMEM)
    hbm = pl.BlockSpec(memory_space=pl.ANY)
    ring = FAR + NEAR
    dma = pltpu.SemaphoreType.DMA
    return pl.pallas_call(
        kernel,
        out_shape=pltpu.VMEM((ROWS, D), BF16),
        in_specs=[hbm] * 21,
        out_specs=vmem,
        scratch_shapes=[
            *(pltpu.VMEM(a.shape, a.dtype) for a in inputs),
            dma((16,)),
            pltpu.VMEM((TOK, KT), F32),
            pltpu.VMEM((TOK, KT), F32),
            pltpu.VMEM((TOK, KT), BF16),
            pltpu.VMEM((TOK, KT), BF16),
            pltpu.VMEM((TOK, KT), BF16),
            pltpu.VMEM((TOK, 128), F32),
            pltpu.VMEM((NX, 72, KT), BF16),
            pltpu.VMEM((NY, 72, KT), BF16),
            pltpu.VMEM((64, KT), F32),
            pltpu.VMEM((2, TOK // 2, 128), BF16),
            pltpu.VMEM((TOK // 2, 128), BF16),
            pltpu.VMEM((2, 128, D), BF16),
            pltpu.VMEM((TOK // 2, D), F32),
            pltpu.VMEM((ring, ROWS, D), BF16),
            pltpu.VMEM((ring, ROWS, D), BF16),
            pltpu.VMEM((ROWS, D), F32),
            pltpu.VMEM((NZ, SLOTS, LINES, 128), BF16),
            pltpu.VMEM((NZ, SLOTS, LINES, 128), BF16),
            pltpu.VMEM((SLOTS * PITCH, 128), F32),
            pltpu.VMEM((NZ * SLOTS, D), BF16),
            pltpu.VMEM((NZ * SLOTS, D), F32),
            pltpu.VMEM((2, D, HID), BF16),
            pltpu.VMEM((2, D, HID), BF16),
            pltpu.VMEM((2, HID, D), BF16),
            pltpu.VMEM((ring, SLOTS, D), BF16),
            pltpu.VMEM((ring, SLOTS, D), BF16),
            pltpu.VMEM((NZ, SLOTS, LINES, 128), BF16),
            pltpu.VMEM((NZ, SLOTS, LINES, 128), BF16),
            pltpu.VMEM((NZ, 8, 128), F32),
            pltpu.VMEM((NZ, SLOTS, ROWS), BF16),
            pltpu.VMEM((NZ, ROWS, SLOTS), BF16),
            pltpu.VMEM((NZ, ROWS, D), BF16),
            pltpu.VMEM((NZ, ROWS, D), F32),
            pltpu.VMEM((NZ, SLOTS, LINES, 128), BF16),
            pltpu.VMEM((ring, ROWS, D), BF16),
            pltpu.VMEM((ring, ROWS, D), BF16),
            pltpu.VMEM((NZ, ROWS, SLOTS), BF16),
            pltpu.VMEM((ROWS, D), BF16),
            pltpu.VMEM((ROWS, D), BF16),
            dma, dma((NZ,)), dma, dma, dma, dma, pltpu.SemaphoreType.REGULAR,
            pltpu.SemaphoreType.REGULAR, dma, dma((ring, 1)),
            dma, dma((NZ,)), dma, dma((ACH,)),
            dma((5,)), dma((5,)), dma((5,)),
            dma, dma((NX,)), dma((NY,)), dma((NY,)),
            dma, dma,
            dma, dma((ring, DCH)),
            dma, dma((ring, max(ACH, ZCH))),
            dma,
        ],
        compiler_params=pltpu.CompilerParams(
            collective_id=0, has_side_effects=True, vmem_limit_bytes=56 * 1024 * 1024
        ),
    )(
        *inputs, alpha, beta, switch, expansion, contraction,
    )


def solution(mesh):
    placed = (
        P("sp", "tp"),
        P("sp", "tp"),
        P("tp"),
        P("sp", "tp"),
        P("sp", "tp"),
        P("tp"),
        P("sp", "tp"),
        P("sp", "tp"),
        P("sp", "tp"),
        P(),
        P("tp", None),
        P("tp", None),
        P(("sp", "tp"), None),
        P(),
        P(),
        P(),
        P(None, "sp"),
        P("sp", None, "tp"),
        P("sp", None, "tp"),
        P("sp", "tp", None),
        P(("sp", "tp")),
    )
    return jax.shard_map(
        shards, mesh=mesh, in_specs=placed, out_specs=P(("sp", "tp"), None), check_vma=False
    )
```

```python
import functools

import jax
import jax.numpy as jnp
from jax import lax
from jax.experimental import pallas as pl
from jax.experimental.pallas import tpu as pltpu
from jax.sharding import PartitionSpec as P

EPSILON = 1e-06
NX, NY, NZ = 4, 4, 8
NS = NX * NY
D = 2048
KT = 384
TOK = 512
ROWS = 32
CAP = 3
SLOTS = NS * CAP
LINES = D // 128
HID = 256
FAR, NEAR = NZ // 2, NZ // 2 - 1
PLACE = {0: 0, 7: 1, 1: 2, 6: 3, 2: 4, 5: 5, 3: 6, 4: 7}
PITCH = 24
OFFSETS = sorted(
    ((dy, dx) for dy in range(NY) for dx in range(NX)),
    key=lambda o: min(o[0], NY - o[0]) + min(o[1], NX - o[1]),
)
PIECE = 8
DCH, GCH, ZCH, ACH = 8, 6, 8, 8
MESH = pl.DeviceIdType.MESH
F32, BF16 = jnp.float32, jnp.bfloat16


def dot(a, b):
    return jnp.dot(a, b, preferred_element_type=F32)


def dot_nt(a, b):
    return lax.dot_general(a, b, (((1,), (1,)), ((), ())), preferred_element_type=F32)


def dot_tn(a, b):
    return lax.dot_general(a, b, (((0,), (0,)), ((), ())), preferred_element_type=F32)


def sigmoid(v):
    return 1.0 / (1.0 + jnp.exp(-v))


def rms(v, gain):
    return v * lax.rsqrt(jnp.mean(v * v, axis=-1, keepdims=True) + EPSILON) * gain


def split3(v):
    high = v.astype(BF16)
    rest = v - high.astype(F32)
    mid = rest.astype(BF16)
    low = (rest - mid.astype(F32)).astype(BF16)
    return high, mid, low


def iota(shape, dim):
    return lax.broadcasted_iota(jnp.int32, shape, dim)


def kernel(
    fa_hbm, fb_hbm, ga_hbm, gb_hbm, bias_hbm, cluster_hbm, qa_hbm, qb_hbm, v_hbm,
    gate_hbm, lane_hbm, skip_hbm, post_hbm, pre_hbm, postmix_hbm, router_hbm,
    alpha_ref, beta_ref, sw_ref, ex_ref, co_ref,
    out_ref,
    fa_ref, fb_ref, ga_ref, gb_ref, bias_ref, cluster_ref, qa_ref, qb_ref, v_ref,
    gate_ref, lane_ref, skip_ref, post_ref, pre_ref, postmix_ref, router_ref, insem,
    key_s, ins_s, qd_s, kg_s, wk_s, intra_s, buf1, buf2, row_s, hd_s, hrecv, wproj, p_s,
    dsend, drecv, hmid_s, out_rt, x_rt, conv_s, x_s, part_s, swv, exv, cov, gsend, grecv, ret_rt, fin_rt,
    clus_s, place_s, unplace_s, nz_s, qz_s,
    rets_rt, sends_s, recvs_s, unp_s, routs_s, routr_s, oss, rrs, us, ur, qs, qr, pair_sem,
    plane_sem, cls, clr, zos, zor, zis, xir,
    wsem, wssem, wrsem, s1s, s1r, s2s, s2r, hs, hr, dss, drs, ags, agr, gss,
):
    s = lax.axis_index("sp")
    t = lax.axis_index("tp")
    y, x = s // NX, lax.rem(s, NX)
    z, c = t // 2, lax.rem(t, 2)
    way = 1 - 2 * c
    ahead = lax.rem(z + way + NZ, NZ) * 2 + c
    behind = lax.rem(z - way + NZ, NZ) * 2 + c
    sibling = z * 2 + 1 - c

    def remote(src, dst, ssem, rsem, sp, tp):
        return pltpu.make_async_remote_copy(
            src_ref=src, dst_ref=dst, send_sem=ssem, recv_sem=rsem,
            device_id=(sp, tp), device_id_type=MESH,
        )

    barrier = pltpu.get_barrier_semaphore()
    row = [(y * NX + lax.rem(x + d, NX), t) for d in range(1, NX)]
    column = [(lax.rem(y + d, NY) * NX + x, t) for d in range(1, NY)]
    near = [*row, *column, (s, ahead), (s, behind), (s, sibling)]
    for peer in near:
        pl.semaphore_signal(barrier, inc=1, device_id=peer, device_id_type=MESH)

    inputs = [
        pltpu.make_async_copy(a, b, insem.at[k])
        for k, (a, b) in enumerate(
            [
                (fa_hbm, fa_ref), (fb_hbm, fb_ref), (ga_hbm, ga_ref), (gb_hbm, gb_ref),
                (bias_hbm, bias_ref), (cluster_hbm, cluster_ref), (qa_hbm, qa_ref),
                (qb_hbm, qb_ref), (v_hbm, v_ref), (gate_hbm, gate_ref), (lane_hbm, lane_ref),
                (skip_hbm, skip_ref), (post_hbm, post_ref), (pre_hbm, pre_ref),
                (postmix_hbm, postmix_ref), (router_hbm, router_ref),
            ]
        )
    ]
    for copy in inputs:
        copy.start()
    own_weights = [
        pltpu.make_async_copy(alpha_ref, wproj.at[0, pl.ds(0, 64)], wsem.at[0]),
        pltpu.make_async_copy(beta_ref, wproj.at[0, pl.ds(64, 64)], wsem.at[1]),
        pltpu.make_async_copy(sw_ref.at[0], swv.at[0], wsem.at[2]),
        pltpu.make_async_copy(ex_ref.at[0], exv.at[0], wsem.at[3]),
        pltpu.make_async_copy(co_ref.at[0], cov.at[0], wsem.at[4]),
    ]
    for copy in own_weights:
        copy.start()

    for copy in inputs[:6]:
        copy.wait()
    gap = jnp.concatenate([ga_ref[...], gb_ref[...]], axis=1)
    lower = jnp.where(iota((128, 128), 0) >= iota((128, 128), 1), 1.0, 0.0).astype(BF16)

    def decays(r, carry):
        rows = slice(r * 128, r * 128 + 128)
        forget = jnp.concatenate([fa_ref[rows, :].astype(F32), fb_ref[rows, :].astype(F32)], axis=1)
        key = gap * sigmoid(-forget)
        left = jnp.broadcast_to(bias_ref[0:1, rows], (128, 128)).T
        right = jnp.broadcast_to(bias_ref[1:2, rows], (128, 128)).T
        logf = jnp.log1p(-key) + jnp.concatenate([left, right, right], axis=1)
        high, mid, _ = split3(logf)
        inside = dot(lower, high) + dot(lower, mid) + carry
        key_s[rows, :] = key
        ins_s[rows, :] = inside
        return inside[127:128, :]

    last = jnp.zeros((1, KT), F32)
    for r in range(TOK // 128):
        last = decays(r, last)

    def weighted(r):
        rows = slice(r * 128, r * 128 + 128)
        wk_s[rows, :] = (key_s[rows, :] * jnp.exp(last - ins_s[rows, :])).astype(BF16)

    def scaled(r):
        rows = slice(r * 128, r * 128 + 128)
        ask = jnp.concatenate([qa_ref[rows, :].astype(F32), qb_ref[rows, :].astype(F32)], axis=1)
        inside = ins_s[rows, :]
        qd_s[rows, :] = (ask * sigmoid(ask) * jnp.exp(inside)).astype(BF16)
        kg_s[rows, :] = (key_s[rows, :] * jnp.exp(-inside)).astype(BF16)

    for r in range(TOK // 128):
        weighted(r)
    inputs[8].wait()
    summed = dot_tn(v_ref[...], wk_s[...])
    state = jnp.concatenate([summed[0:64, 0:128], summed[64:128, 128:KT]], axis=1)

    def packed(buf, place, state, total):
        rows3 = iota((8, KT), 0)
        high, mid, low = (part.astype(F32) for part in split3(total))
        lines = jnp.where(rows3 == 0, high, jnp.where(rows3 == 1, mid, jnp.where(rows3 == 2, low, 0.0)))
        buf[place, 0:64, :] = state.astype(BF16)
        buf[place, 64:72, :] = lines.astype(BF16)

    def unpacked(buf, place):
        lines = buf[place, 64:72, :].astype(F32)
        return buf[place, 0:64, :].astype(F32), lines[0:1] + lines[1:2] + lines[2:3]

    packed(buf1, x, state, last)
    clus_s[0] = jnp.zeros((8, 128), F32)
    clus_s[0, :, 0:ROWS] = jnp.broadcast_to(cluster_ref[...].astype(F32), (8, ROWS))
    pl.semaphore_wait(barrier, len(near))
    for peer in row:
        pl.semaphore_signal(plane_sem, inc=1, device_id=peer, device_id_type=MESH)

    def along_x(d):
        return remote(buf1.at[x], buf1.at[x], s1s, s1r.at[x], y * NX + lax.rem(x + d, NX), t)

    def from_x(d):
        there = lax.rem(x + d, NX)
        return remote(buf1.at[there], buf1.at[there], s1s, s1r.at[there], y * NX + there, t)

    for d in (2, 1, 3):
        along_x(d).start()

    shared = [
        (alpha_ref, wproj.at[1, pl.ds(0, 64)]), (beta_ref, wproj.at[1, pl.ds(64, 64)]),
        (sw_ref.at[0], swv.at[1]), (ex_ref.at[0], exv.at[1]), (co_ref.at[0], cov.at[1]),
    ]
    shared = [remote(a, b, wssem.at[k], wrsem.at[k], s, sibling) for k, (a, b) in enumerate(shared)]
    for copy in shared[:4]:
        copy.start()

    left_half = iota((256, 128), 1) < 64

    def intra(columns, first):
        for block in range(2):
            rows, width = slice(block * 256, block * 256 + 256), 256 * (block + 1)
            scores = dot_nt(qd_s[rows, columns], kg_s[0:width, columns])
            causal = iota((256, width), 0) + 256 * block >= iota((256, width), 1)
            scores = jnp.where(causal, scores, 0.0).astype(BF16)
            found = dot(scores, v_ref[0:width, :])
            intra_s[rows, :] = found if first else jnp.where(left_half, intra_s[rows, :], found)

    for copy in inputs[6:8] + inputs[9:]:
        copy.wait()
    for r in range(TOK // 128):
        scaled(r)
    intra(slice(0, 128), True)

    for d in range(1, NX):
        from_x(d).wait_recv()
    sofar, gone = jnp.zeros((64, KT), F32), jnp.zeros((1, KT), F32)
    before, before_gone = sofar, gone
    for k in range(NX):
        before = jnp.where(x == k, sofar, before)
        before_gone = jnp.where(x == k, gone, before_gone)
        piece, total = unpacked(buf1, k)
        sofar = jnp.exp(total) * sofar + piece
        gone = gone + total
    packed(buf2, y, sofar, gone)
    row_s[...] = jnp.zeros_like(row_s)

    def along_y(d):
        return remote(buf2.at[y], buf2.at[y], s2s.at[d], s2r.at[y], (y + d) * NX + x, t)

    def from_y(k):
        return remote(buf2.at[k], buf2.at[k], s2s.at[0], s2r.at[k], k * NX + x, t)

    for d in (2, 3, 1):
        @pl.when(y + d < NY)
        def _():
            along_y(d).start()

    intra(slice(128, KT), False)

    for k in range(NY - 1):
        @pl.when(k < y)
        def _():
            from_y(k).wait_recv()
            piece, total = unpacked(buf2, k)
            row_s[...] = jnp.exp(total) * row_s[...] + piece

    carried = jnp.exp(before_gone) * row_s[...] + before
    is_left = iota((64, KT), 1) < 128
    carried = jnp.concatenate(
        [jnp.where(is_left, carried, 0.0), jnp.where(is_left, 0.0, carried)], axis=0
    ).astype(BF16)
    lane_gain = jnp.concatenate([lane_ref[...], lane_ref[...]], axis=1)
    left = iota((128, 128), 1) < 64
    for r in range(TOK // 128):
        rows = slice(r * 128, r * 128 + 128)
        raw = intra_s[rows, :] + dot_nt(qd_s[rows, :], carried)
        squares = raw * raw
        mean_a = jnp.sum(jnp.where(left, squares, 0.0), axis=1, keepdims=True) * (1.0 / 64)
        mean_b = jnp.sum(jnp.where(left, 0.0, squares), axis=1, keepdims=True) * (1.0 / 64)
        mean = jnp.where(left, mean_a, mean_b)
        head = raw * lax.rsqrt(mean + EPSILON) * lane_gain * sigmoid(gate_ref[rows, :].astype(F32))
        head = head.astype(BF16)
        for q in range(4):
            at = (2 * r + q // 2) * 32
            hd_s[q % 2, at : at + 32, :] = head[q * 32 : q * 32 + 32, :]

    swap = remote(hd_s.at[1 - c], hrecv, hs, hr, s, sibling)
    swap.start()
    for copy in own_weights[:2]:
        copy.wait()
    p_s[...] = dot(hd_s[c], wproj[0])
    for copy in shared[:2]:
        copy.wait_recv()
    swap.wait_recv()
    p_s[...] = p_s[...] + dot(hrecv[...], wproj[1])

    def piece_d(j):
        return j // 2 * PIECE, slice(j % 2 * (D // 2), (j % 2 + 1) * (D // 2))

    def ring_d(k, j):
        first, columns = piece_d(j)
        part = (k, pl.ds(first, PIECE), pl.ds(columns.start, D // 2))
        return remote(
            dsend.at[part], drecv.at[part], dss, drs.at[k, j], s,
            ahead if k < FAR else behind,
        )

    def send_d(k, j, starts):
        place = FAR - k if k < FAR else -(NEAR - (k - FAR))
        target = lax.rem(z + way * place + NZ, NZ)
        first, columns = piece_d(j)
        rows = pl.ds(pl.multiple_of(target * ROWS + first, PIECE), PIECE)
        value = p_s[rows, columns]
        if not starts:
            ring_d(k - 1, j).wait_recv()
            value = value + drecv[k - 1, first : first + PIECE, columns].astype(F32)
        dsend[k, first : first + PIECE, columns] = value.astype(BF16)
        ring_d(k, j).start()

    def gather(buf, part, ssem, rsem):
        def copy(k, j):
            source = (NZ - k) % NZ if k < FAR else k - FAR
            target = (source + NZ - 1) % NZ if k < FAR else source + 1
            return remote(
                buf.at[(source, *part(j))], buf.at[(target, *part(j))], ssem, rsem.at[k, j], s,
                ahead if k < FAR else behind,
            )

        return copy

    def gather_step(ring, k, chunks, meanwhile=()):
        for j in range(chunks):
            ring(k, j).wait_recv()
            if k + 1 < FAR:
                ring(k + 1, j).start()
            if k < NEAR:
                ring(FAR + k, j).wait_recv()
                if k + 1 < NEAR:
                    ring(FAR + k + 1, j).start()
            if j < len(meanwhile):
                meanwhile[j]()

    def slots_of(r):
        group_row = jnp.broadcast_to(clus_s[r, 0:1, 0:ROWS], (ROWS, ROWS))
        diagonal = iota((ROWS, ROWS), 0) == iota((ROWS, ROWS), 1)
        group_column = jnp.sum(jnp.where(diagonal, group_row, 0.0), axis=1, keepdims=True)
        same = jnp.where(group_row == group_column, 1.0, 0.0)
        earlier_row = iota((ROWS, ROWS), 0) < iota((ROWS, ROWS), 1)
        rank_row = jnp.sum(jnp.where(earlier_row, same, 0.0), axis=0, keepdims=True)
        earlier_column = iota((ROWS, ROWS), 1) < iota((ROWS, ROWS), 0)
        rank_column = jnp.sum(jnp.where(earlier_column, same, 0.0), axis=1, keepdims=True)
        slot_row = group_row[0:1, :] * CAP + rank_row
        slot_column = group_column * CAP + rank_column
        place_s[r] = jnp.where(
            iota((SLOTS, ROWS), 0).astype(F32) == slot_row, 1.0, 0.0
        ).astype(BF16)
        unplace_s[r] = jnp.where(
            iota((ROWS, SLOTS), 1).astype(F32) == slot_column, 1.0, 0.0
        ).astype(BF16)

    groups = gather(clus_s, lambda j: (), cls, clr)
    groups(0, 0).start()
    groups(FAR, 0).start()
    for step in range(FAR):
        if step:
            gather_step(groups, step - 1, 1)
        for j in range(DCH):
            send_d(step, j, step == 0)
            if step < NEAR:
                send_d(FAR + step, j, step == 0)
        if step == 0:
            shared[4].start()
            pl.semaphore_wait(plane_sem, NX - 1)
            pl.semaphore_signal(pair_sem, inc=1, device_id=(s, sibling), device_id_type=MESH)
            slots_of(0)
        else:
            slots_of(NZ - step)
            slots_of(step)
    gather_step(groups, FAR - 1, 1)
    slots_of(FAR)
    mixed = p_s[pl.ds(pl.multiple_of(z * ROWS, ROWS), ROWS), :]
    for k in (FAR + NEAR - 1, FAR - 1):
        for j in range(DCH):
            ring_d(k, j).wait_recv()
        mixed = mixed + drecv[k].astype(F32)

    h_mid = (skip_ref[...].astype(F32) + rms(mixed, post_ref[...])).astype(BF16).astype(F32)
    hmid_s[...] = h_mid
    nz_s[0] = rms(h_mid, pre_ref[...]).astype(BF16)

    lines3 = conv_s.reshape(SLOTS, PITCH, 128)
    own = pl.ds(s * CAP, CAP)

    def slots_for(k):
        return pl.ds(k * CAP, CAP)

    def to_lines(value):
        for i in range(LINES):
            conv_s[pl.ds(i, SLOTS, stride=PITCH), :] = value[:, i * 128 : i * 128 + 128]
        return lines3[:, 0:LINES, :].astype(BF16)

    def from_lines(value, at):
        lines3[:, 0:LINES, :] = value.astype(F32)
        for i in range(LINES):
            x_s[at : at + SLOTS, i * 128 : i * 128 + 128] = conv_s[
                pl.ds(i, SLOTS, stride=PITCH), :
            ].astype(BF16)

    def at_offset(dy, dx):
        return lax.rem(y + dy, NY) * NX + lax.rem(x + dx, NX)

    def all_but_own(src, dst, r, ssem, rsem):
        most = pl.ds(0, SLOTS - CAP)
        return remote(src.at[r, most], dst.at[r, most], ssem, rsem, lax.rem(s + 1, NS), t)

    def scatter(src, dst, r, ssem, rsem):
        for dy, dx in reversed(OFFSETS[1:]):
            there = at_offset(dy, dx)
            remote(src.at[r, slots_for(there)], dst.at[r, own], ssem, rsem, there, t).start()
        dst[r, own] = src[r, own]

    def near_slots(p):
        return pl.ds(p * CAP, CAP)

    def scatter_in(src, dst):
        for dy, dx in reversed(OFFSETS[1:]):
            there = at_offset(dy, dx)
            p = OFFSETS.index(((-dy) % NY, (-dx) % NX))
            remote(
                src.at[0, slots_for(there)], dst.at[0, near_slots(p)], zos, xir.at[p // (NS // ACH)],
                there, t,
            ).start()
        dst[0, 0:CAP] = src[0, own]

    def scattered_in(src, dst, q):
        first = 1 if q == 0 else q * (NS // ACH)
        part = pl.ds(first * CAP, ((q + 1) * (NS // ACH) - first) * CAP)
        return remote(src.at[0, part], dst.at[0, part], zos, xir.at[q], lax.rem(s + 1, NS), t)

    def scatter_back(src, dst, r, ssem, rsem):
        for p in range(NS - 1, -1, -1):
            there = at_offset(*OFFSETS[p])
            remote(src.at[r, near_slots(p)], dst.at[r, own], ssem, rsem, there, sibling).start()

    def given_back(r):
        remote(fin_rt.at[r], rets_rt.at[r], zis, rrs.at[r], s, sibling).wait_recv()
        at = PLACE[r] * SLOTS
        from_lines(rets_rt[r], at)
        qz_s[r] = dot(unp_s[r], x_s[at : at + SLOTS, :])

    def returned(r, rsem):
        all_but_own(fin_rt, ret_rt, r, zis, rsem).wait_recv()
        at = PLACE[r] * SLOTS
        from_lines(ret_rt[r], at)
        return dot(unplace_s[r], x_s[at : at + SLOTS, :])

    for copy in own_weights[2:]:
        copy.wait()
    router = router_ref[...].astype(F32)
    router_rows = iota((16, D), 0)
    router = jnp.where(
        router_rows == 0, router[0:1], jnp.where(router_rows == 1, router[1:2], 0.0)
    ).astype(BF16)
    member = z // (NZ // 2)

    def part_of(r):
        return part_s[PLACE[r] * SLOTS : PLACE[r] * SLOTS + SLOTS, :]

    def hidden_of(places):
        for place in places:
            from_lines(x_rt[place], PLACE[place] * SLOTS)
        at = PLACE[places[0]] * SLOTS
        rows = x_s[at : at + SLOTS * len(places), :]
        scores = sigmoid(dot_nt(rows, router))
        first, second = scores[:, 0:1], scores[:, 1:2]
        weight = jnp.where(member == 0, first, second) / (first + second)
        hidden = []
        for u in range(2):
            gate = dot(rows, swv[u])
            hidden.append((gate * sigmoid(gate) * dot(rows, exv[u])).astype(BF16))
        return places, weight, hidden

    def contract(found):
        places, weight, hidden = found
        at = PLACE[places[0]] * SLOTS
        total = dot(hidden[0], cov[0]) + dot(hidden[1], cov[1])
        part_s[at : at + SLOTS * len(places), :] = total * weight

    def compute(places):
        contract(hidden_of(places))

    def part_z(j):
        first, columns = piece_d(j)
        return pl.ds(first, PIECE), pl.ds(columns.start, D // 2)

    def part_g(j):
        return pl.ds(j * PIECE, PIECE), pl.ds(0, D)

    def reduce(values, part, sent, received, ssem, rsem, to=(ahead, behind)):
        def copy(k, j):
            return remote(
                sent.at[(k, *part(j))], received.at[(k, *part(j))], ssem, rsem.at[k, j], s,
                to[0] if k < FAR else to[1],
            )

        def send(k, j, first):
            place = FAR - k if k < FAR else NZ - (NEAR - (k - FAR))
            rows, columns = (slice(d.start, d.start + d.size) for d in part(j))
            value = values(place, rows, columns)
            if not first:
                copy(k - 1, j).wait_recv()
                value = value + received[k - 1, rows, columns].astype(F32)
            sent[k, rows, columns] = value.astype(BF16)
            copy(k, j).start()

        return copy, send

    def reduce_step(send, chunks, step):
        for j in range(chunks):
            send(step, j, False)
            if step < NEAR:
                send(FAR + step, j, False)

    def reduce_end(copy, received, chunks, total):
        for k in (FAR + NEAR - 1, FAR - 1):
            for j in range(chunks):
                copy(k, j).wait_recv()
            total = total + received[k].astype(F32)
        return total

    def summed_rows(h):
        rows = pl.ds(h * (ROWS // 2), ROWS // 2)
        return remote(routs_s.at[rows], routr_s.at[rows], qs, qr.at[h], s, sibling)

    sides = [(NZ - 1 - k, k + 1) if k < NEAR else (NZ - 1 - k,) for k in range(FAR)]

    pl.semaphore_wait(pair_sem, 1)

    @pl.when(c == 0)
    def _():
        slots_copy = remote(unplace_s, unp_s, us, ur, s, sibling)
        slots_copy.start()
        ring = gather(x_rt, lambda j: (pl.ds(j * (SLOTS // ACH), SLOTS // ACH),), ags, agr)
        out_rt[0] = to_lines(dot(place_s[0], nz_s[0]))
        scatter_in(out_rt, x_rt)
        for copy in shared[2:]:
            copy.wait_recv()
        for j in range(ACH):
            scattered_in(out_rt, x_rt, j).wait_recv()
            ring(0, j).start()
            ring(FAR, j).start()

        def back(places):
            for r in places:
                fin_rt[r] = to_lines(part_of(r))
                scatter_back(fin_rt, rets_rt, r, zis, rrs.at[r])

        compute((0,))
        back((0,))
        gather_step(ring, 0, ACH)
        for k in range(1, FAR):
            found = []
            gather_step(
                ring, k, ACH,
                (
                    lambda: found.append(hidden_of(sides[k - 1])),
                    lambda: contract(found[0]),
                    lambda: back(sides[k - 1]),
                ),
            )
        compute(sides[FAR - 1])
        back(sides[FAR - 1])
        for h in range(2):
            summed_rows(h).wait_recv()
        routed = routr_s[...].astype(F32)
        out_ref[...] = (hmid_s[...] + rms(routed, postmix_ref[...])).astype(BF16)
        all_but_own(out_rt, x_rt, 0, zos, xir.at[0]).wait_send()
        slots_copy.wait_send()
        remote(fin_rt, rets_rt, zis, rrs.at[0], s, sibling).wait_send()
        around = pl.ds(0, FAR + NEAR)
        remote(x_rt.at[around], x_rt.at[around], ags, agr.at[0, 0], s, ahead).wait_send()

    @pl.when(c == 1)
    def _():
        ring = gather(nz_s, part_z, ags, agr)
        for j in range(ZCH):
            ring(0, j).start()
            ring(FAR, j).start()

        def dispatch(r):
            out_rt[r] = to_lines(dot(place_s[r], nz_s[r]))
            scatter(out_rt, x_rt, r, zos, zor.at[r])

        def work(places):
            for r in places:
                all_but_own(out_rt, x_rt, r, zos, zor.at[r]).wait_recv()
            compute(places)

        dispatch(0)
        for copy in shared[2:]:
            copy.wait_recv()
        for k in range(FAR):
            gather_step(ring, k, ZCH)
            for r in sides[k]:
                dispatch(r)
            if k == 1:
                work((0,))
            elif k == 2:
                work(sides[0])
        copy, send = reduce(
            lambda place, rows, columns: part_s[
                PLACE[place] * SLOTS + rows.start : PLACE[place] * SLOTS + rows.stop, columns
            ],
            part_g, gsend, grecv, gss, drs,
        )
        work(sides[1])
        work(sides[2])
        for j in range(GCH):
            send(FAR, j, True)
        work(sides[3])
        for j in range(GCH):
            send(0, j, True)
        copy_s, send_s = reduce(
            lambda place, rows, columns: qz_s[place, rows, columns], part_z, sends_s, recvs_s,
            oss, agr, (behind, ahead),
        )
        remote(unplace_s, unp_s, us, ur, s, sibling).wait_recv()
        for r in (0, 7, 1):
            given_back(r)
        reduce_step(send, GCH, 1)
        for r in (6, 2):
            given_back(r)
        reduce_step(send, GCH, 2)
        given_back(5)
        for j in range(ZCH):
            send_s(FAR, j, True)
        given_back(3)
        reduce_step(send, GCH, 3)
        given_back(4)
        for j in range(ZCH):
            send_s(0, j, True)
        reduce_step(send_s, ZCH, 1)
        final = reduce_end(copy, grecv, GCH, part_of(0))
        fin_rt[0] = to_lines(final)
        scatter(fin_rt, ret_rt, 0, zis, xir.at[0])
        reduce_step(send_s, ZCH, 2)
        reduce_step(send_s, ZCH, 3)
        routed = returned(0, xir.at[0])
        out_ref[...] = (hmid_s[...] + rms(routed, postmix_ref[...])).astype(BF16)
        for h in range(2):
            rows = slice(h * (ROWS // 2), (h + 1) * (ROWS // 2))
            for k in (FAR + NEAR - 1, FAR - 1):
                for j in range(h * (ZCH // 2), (h + 1) * (ZCH // 2)):
                    copy_s(k, j).wait_recv()
            total = qz_s[0, rows, :] + recvs_s[FAR + NEAR - 1, rows, :].astype(F32)
            routs_s[rows, :] = (total + recvs_s[FAR - 1, rows, :].astype(F32)).astype(BF16)
            summed_rows(h).start()
        most = pl.ds(0, SLOTS - CAP)
        remote(
            out_rt.at[:, most], x_rt.at[:, most], zos, zor.at[0], lax.rem(s + 1, NS), t
        ).wait_send()
        all_but_own(fin_rt, ret_rt, 0, zis, xir.at[0]).wait_send()
        around = pl.ds(0, FAR + NEAR)
        remote(nz_s.at[around], nz_s.at[around], ags, agr.at[0, 0], s, ahead).wait_send()
        remote(gsend, grecv, gss, drs.at[0, 0], s, ahead).wait_send()
        remote(sends_s, recvs_s, oss, agr.at[0, 0], s, ahead).wait_send()
        remote(routs_s, routr_s, qs, qr.at[0], s, sibling).wait_send()

    remote(
        buf1.at[pl.ds(0, NX - 1)], buf1.at[pl.ds(0, NX - 1)], s1s, s1r.at[0], s, sibling
    ).wait_send()
    for d in range(1, NY):
        @pl.when(y + d < NY)
        def _():
            along_y(d).wait_send()
    around = pl.ds(0, FAR + NEAR)
    remote(clus_s.at[around], clus_s.at[around], cls, clr.at[0, 0], s, ahead).wait_send()
    for copy in shared:
        copy.wait_send()
    swap.wait_send()
    remote(dsend, drecv, dss, drs.at[0, 0], s, ahead).wait_send()


def shards(
    ask_left, keep_left, gap_left, ask_right, keep_right, gap_right, payload, switch_logits,
    keep_bias, lanewise, alpha, beta, skip, post, pre, postmix, router, switch, expansion,
    contraction, cluster,
):
    inputs = (
        keep_left, keep_right, gap_left.reshape(1, -1), gap_right.reshape(1, -1), keep_bias.T,
        cluster.reshape(1, -1), ask_left, ask_right, payload, switch_logits,
        lanewise.reshape(1, -1), skip, post.reshape(1, -1), pre.reshape(1, -1),
        postmix.reshape(1, -1), router.T,
    )
    vmem = pl.BlockSpec(memory_space=pltpu.VMEM)
    hbm = pl.BlockSpec(memory_space=pl.ANY)
    ring = FAR + NEAR
    dma = pltpu.SemaphoreType.DMA
    return pl.pallas_call(
        kernel,
        out_shape=pltpu.VMEM((ROWS, D), BF16),
        in_specs=[hbm] * 21,
        out_specs=vmem,
        scratch_shapes=[
            *(pltpu.VMEM(a.shape, a.dtype) for a in inputs),
            dma((16,)),
            pltpu.VMEM((TOK, KT), F32),
            pltpu.VMEM((TOK, KT), F32),
            pltpu.VMEM((TOK, KT), BF16),
            pltpu.VMEM((TOK, KT), BF16),
            pltpu.VMEM((TOK, KT), BF16),
            pltpu.VMEM((TOK, 128), F32),
            pltpu.VMEM((NX, 72, KT), BF16),
            pltpu.VMEM((NY, 72, KT), BF16),
            pltpu.VMEM((64, KT), F32),
            pltpu.VMEM((2, TOK // 2, 128), BF16),
            pltpu.VMEM((TOK // 2, 128), BF16),
            pltpu.VMEM((2, 128, D), BF16),
            pltpu.VMEM((TOK // 2, D), F32),
            pltpu.VMEM((ring, ROWS, D), BF16),
            pltpu.VMEM((ring, ROWS, D), BF16),
            pltpu.VMEM((ROWS, D), F32),
            pltpu.VMEM((NZ, SLOTS, LINES, 128), BF16),
            pltpu.VMEM((NZ, SLOTS, LINES, 128), BF16),
            pltpu.VMEM((SLOTS * PITCH, 128), F32),
            pltpu.VMEM((NZ * SLOTS, D), BF16),
            pltpu.VMEM((NZ * SLOTS, D), F32),
            pltpu.VMEM((2, D, HID), BF16),
            pltpu.VMEM((2, D, HID), BF16),
            pltpu.VMEM((2, HID, D), BF16),
            pltpu.VMEM((ring, SLOTS, D), BF16),
            pltpu.VMEM((ring, SLOTS, D), BF16),
            pltpu.VMEM((NZ, SLOTS, LINES, 128), BF16),
            pltpu.VMEM((NZ, SLOTS, LINES, 128), BF16),
            pltpu.VMEM((NZ, 8, 128), F32),
            pltpu.VMEM((NZ, SLOTS, ROWS), BF16),
            pltpu.VMEM((NZ, ROWS, SLOTS), BF16),
            pltpu.VMEM((NZ, ROWS, D), BF16),
            pltpu.VMEM((NZ, ROWS, D), F32),
            pltpu.VMEM((NZ, SLOTS, LINES, 128), BF16),
            pltpu.VMEM((ring, ROWS, D), BF16),
            pltpu.VMEM((ring, ROWS, D), BF16),
            pltpu.VMEM((NZ, ROWS, SLOTS), BF16),
            pltpu.VMEM((ROWS, D), BF16),
            pltpu.VMEM((ROWS, D), BF16),
            dma, dma((NZ,)), dma, dma, dma, dma((2,)), pltpu.SemaphoreType.REGULAR,
            pltpu.SemaphoreType.REGULAR, dma, dma((ring, 1)),
            dma, dma((NZ,)), dma, dma((ACH,)),
            dma((5,)), dma((5,)), dma((5,)),
            dma, dma((NX,)), dma((NY,)), dma((NY,)),
            dma, dma,
            dma, dma((ring, DCH)),
            dma, dma((ring, max(ACH, ZCH))),
            dma,
        ],
        compiler_params=pltpu.CompilerParams(
            collective_id=0, has_side_effects=True, vmem_limit_bytes=56 * 1024 * 1024
        ),
    )(
        *inputs, alpha, beta, switch, expansion, contraction,
    )


def solution(mesh):
    placed = (
        P("sp", "tp"),
        P("sp", "tp"),
        P("tp"),
        P("sp", "tp"),
        P("sp", "tp"),
        P("tp"),
        P("sp", "tp"),
        P("sp", "tp"),
        P("sp", "tp"),
        P(),
        P("tp", None),
        P("tp", None),
        P(("sp", "tp"), None),
        P(),
        P(),
        P(),
        P(None, "sp"),
        P("sp", None, "tp"),
        P("sp", None, "tp"),
        P("sp", "tp", None),
        P(("sp", "tp")),
    )
    return jax.shard_map(
        shards, mesh=mesh, in_specs=placed, out_specs=P(("sp", "tp"), None), check_vma=False
    )
```
